256 devices in a mesh: row: 32 (over z, x), col: 8 (over y, core).
Axes of the slice: x: 4, y: 4, z: 8, core: 2. Of those that a mesh axis runs over, the one named last changes fastest.
Arguments:
- tokens: bfloat16 [8192, 2048], P('row'), may hold values from -6 to 6
- norm_gain: float32 [2048], replicated, may hold values from 0.5 to 1.5
- first_gate: bfloat16 [2048, 1024], P(None, 'col'), may hold values from -0.125 to 0.125
- second_gate: bfloat16 [2048, 1024], P(None, 'col'), may hold values from -0.125 to 0.125
- value_weight: bfloat16 [2048, 1024], P(None, 'col'), may hold values from -0.125 to 0.125
- short_weight: bfloat16 [3, 3, 1024], P(None, None, 'col'), may hold values from -3.5 to 3.5
- short_bias: float32 [3, 1024], P(None, 'col'), may hold values from -2 to 2
- embed_weight: float32 [33, 64], replicated, may hold values from -1 to 1
- embed_bias: float32 [64], replicated, may hold values from -3 to 3
- inner_weight: float32 [64, 64], replicated, may hold values from -0.75 to 0.75
- inner_bias: float32 [64], replicated, may hold values from -3 to 3
- filter_freq: float32 [64], replicated, may hold values from 0.5 to 1.5
- filter_weight: float32 [2, 2, 64, 1024], P(None, None, None, ('col', 'row')), may hold values from -0.0234375 to 0.0234375
- filter_skip: float32 [2, 1024], P(None, ('col', 'row')), may hold values from -3 to 3
- output_gain: float32 [1024], P('col'), may hold values from 0.5 to 1.5
- output_weight: bfloat16 [1024, 2048], replicated, may hold values from -0.1875 to 0.1875
Outputs:
- mixed_output: bfloat16 [8192, 2048], P(('row', 'col'))
The draws below stay inside these ranges and needn't reach their ends.
All inputs are finite; a program needn't handle non-finite values.
Results may differ from the reference program's by a relative error of at most 0.01.
Values may be sent and summed in bfloat16 or wider, within the bound.
No kernel may reach another device: no remote copies, remote signals or barrier semaphores. Data moves between devices by JAX's collectives and lax.ppermute only.
A program may use at most 64 MiB of HBM per device.

```python
import math
import jax
import jax.numpy as jnp
from jax import lax

MODEL_WIDTH = 2048
CHANNELS = 1024
GROUPS = 8
SHORT = 3
FREQ_BANDS = 16
FEATURES = 33
FILTER_HIDDEN = 64
SEQ_LEN = 8192


def shard_levels(key, dims, cuts, smallest, top_value):
    loudness = 1.0
    for dim, blocks in cuts:
        draws = jax.random.uniform(jax.random.fold_in(jax.random.fold_in(key, 6), dim), (blocks,), jnp.float32, smallest / len(cuts), top_value / len(cuts))
        loudness = loudness * jnp.repeat(jnp.exp(draws), dims[dim] // blocks).reshape((-1,) + (1,) * (len(dims) - 1 - dim))
    return loudness


def scatter_about(stream_key, shape, deviation, limit, cuts=(), held_as=jnp.bfloat16):
    array = deviation * jax.random.normal(stream_key, shape, jnp.float32)
    if cuts:
        array = array * shard_levels(stream_key, shape, cuts, -0.22, 0.18)
    return jnp.clip(array, -limit, limit).astype(held_as)


def setup_inputs(seed: int = 0) -> dict:
    key_of = jax.random.split(jax.random.key(seed), 17)
    return {
        "tokens": scatter_about(key_of[0], (SEQ_LEN, MODEL_WIDTH), 1.0, 6.0, ((0, 32),)),
        "norm_gain": jnp.clip(1.0 + 0.1 * jax.random.normal(key_of[1], (MODEL_WIDTH,), jnp.float32), 0.5, 1.5),
        "first_gate": scatter_about(key_of[2], (MODEL_WIDTH, CHANNELS), MODEL_WIDTH ** -0.5, 0.125, ((1, 8),)),
        "second_gate": scatter_about(key_of[3], (MODEL_WIDTH, CHANNELS), MODEL_WIDTH ** -0.5, 0.125, ((1, 8),)),
        "value_weight": scatter_about(key_of[4], (MODEL_WIDTH, CHANNELS), MODEL_WIDTH ** -0.5, 0.125, ((1, 8),)),
        "short_weight": scatter_about(key_of[5], (3, SHORT, CHANNELS), SHORT ** -0.5, 3.5, ((2, 8),)),
        "short_bias": scatter_about(key_of[6], (3, CHANNELS), 0.3, 2.0, ((1, 8),), jnp.float32),
        "embed_weight": scatter_about(key_of[7], (FEATURES, FILTER_HIDDEN), FEATURES ** -0.5, 1.0, (), jnp.float32),
        "embed_bias": scatter_about(key_of[8], (FILTER_HIDDEN,), 0.5, 3.0, (), jnp.float32),
        "inner_weight": scatter_about(key_of[9], (FILTER_HIDDEN, FILTER_HIDDEN), FILTER_HIDDEN ** -0.5, 0.75, (), jnp.float32),
        "inner_bias": scatter_about(key_of[10], (FILTER_HIDDEN,), 0.5, 3.0, (), jnp.float32),
        "filter_freq": jnp.clip(1.0 + 0.1 * jax.random.normal(key_of[11], (FILTER_HIDDEN,), jnp.float32), 0.5, 1.5),
        "filter_weight": scatter_about(key_of[12], (2, 2, FILTER_HIDDEN, CHANNELS), (FILTER_HIDDEN * SEQ_LEN // 8) ** -0.5, 0.0234375, ((3, 256),), jnp.float32),
        "filter_skip": scatter_about(key_of[13], (2, CHANNELS), 0.5, 3.0, ((1, 256),), jnp.float32),
        "output_gain": jnp.clip(1.0 + 0.1 * jax.random.normal(key_of[14], (CHANNELS,), jnp.float32), 0.5, 1.5),
        "output_weight": scatter_about(key_of[15], (CHANNELS, MODEL_WIDTH), CHANNELS ** -0.5, 0.1875),
    }


HIGHEST = lax.Precision.HIGHEST
NORM_EPS = 1e-06
DECAY_TARGET = 0.01
FAST_SPAN = 0.3
SLOW_SPAN = 1.5

def position_features(length):
    position_ramp = jnp.linspace(0.0, 1.0, length, dtype=jnp.float32)[:, None]
    angles = 2.0 * math.pi * jnp.arange(length, dtype=jnp.float32)[:, None] / length
    band_freqs = jnp.linspace(0.0001, FREQ_BANDS - 1, FREQ_BANDS, dtype=jnp.float32)[None, :]
    features = jnp.concatenate([position_ramp, jnp.cos(band_freqs * angles), -jnp.sin(band_freqs * angles)], axis=1)
    return (position_ramp, features)

def filter_hidden(length, embed_weight, embed_bias, inner_weight, inner_bias, filter_freq):
    position_ramp, features = position_features(length)
    hidden = jnp.sin(filter_freq * (jnp.dot(features, embed_weight, precision=HIGHEST) + embed_bias))
    hidden = jnp.sin(filter_freq * (jnp.dot(hidden, inner_weight, precision=HIGHEST) + inner_bias))
    return (position_ramp, hidden)

def decay_rates():
    fastest = math.log(DECAY_TARGET) / FAST_SPAN
    slowest = math.log(DECAY_TARGET) / SLOW_SPAN
    return jnp.abs(jnp.linspace(slowest, fastest, CHANNELS, dtype=jnp.float32))

def short_filter(padded, weights, bias_row, length):
    result = bias_row.astype(jnp.float32)
    for tap_index in range(weights.shape[0]):
        result = result + padded[tap_index:tap_index + length].astype(jnp.float32) * weights[tap_index].astype(jnp.float32)
    return result

def two_sided(signal, forward, backward, skip_gain):
    length = signal.shape[0]
    circular_taps = jnp.concatenate([forward, jnp.zeros_like(forward[:1]), backward[:0:-1]], axis=0)
    spectrum = jnp.fft.rfft(signal, n=2 * length, axis=0) * jnp.fft.rfft(circular_taps, axis=0)
    return jnp.fft.irfft(spectrum, n=2 * length, axis=0)[:length] + signal * skip_gain

def reference(tokens, norm_gain, first_gate, second_gate, value_weight, short_weight, short_bias, embed_weight, embed_bias, inner_weight, inner_bias, filter_freq, filter_weight, filter_skip, output_gain, output_weight):
    widened = tokens.astype(jnp.float32)
    normed = (widened * lax.rsqrt(lax.optimization_barrier(jnp.mean(widened * widened, axis=1, keepdims=True)) + NORM_EPS) * norm_gain).astype(jnp.bfloat16)
    gate_first = jnp.dot(normed, first_gate, preferred_element_type=jnp.float32).astype(jnp.bfloat16)
    gate_second = jnp.dot(normed, second_gate, preferred_element_type=jnp.float32).astype(jnp.bfloat16)
    gate_value = jnp.dot(normed, value_weight, preferred_element_type=jnp.float32).astype(jnp.bfloat16)
    length = tokens.shape[0]
    position_ramp, hidden = filter_hidden(length, embed_weight, embed_bias, inner_weight, inner_bias, filter_freq)
    group_width = CHANNELS // GROUPS
    half_width = SHORT // 2

    def blocks(matrix):
        split = matrix.reshape(matrix.shape[:-1] + (GROUPS, group_width))
        return jnp.moveaxis(split, -2, 0)

    def one_block(pieces):
        first_block, second_block, value_block, weight_block, bias_block, filter_block, skip_block, decay_block, gain_block = pieces
        window = jnp.exp(-position_ramp * decay_block[None, :])
        smoothed = []
        for branch, source in enumerate((first_block, second_block, value_block)):
            padded = jnp.pad(source.astype(jnp.float32), ((half_width, SHORT - 1 - half_width), (0, 0)))
            smoothed.append(short_filter(padded, weight_block[branch], bias_block[branch], length))
        signal = smoothed[2]
        for order_index in range(2):
            forward = jnp.dot(hidden, filter_block[order_index, 0], precision=HIGHEST) * window
            backward = jnp.dot(hidden, filter_block[order_index, 1], precision=HIGHEST) * window
            signal = smoothed[order_index] * two_sided(signal, forward, backward, skip_block[order_index])
        scaled = signal * lax.rsqrt(lax.optimization_barrier(jnp.mean(signal * signal, axis=1, keepdims=True)) + NORM_EPS)
        return (scaled * gain_block).astype(jnp.bfloat16)
    normed_blocks = lax.map(one_block, (blocks(gate_first), blocks(gate_second), blocks(gate_value), blocks(short_weight), blocks(short_bias), blocks(filter_weight), blocks(filter_skip), blocks(decay_rates()), blocks(output_gain)))
    mixed = jnp.moveaxis(normed_blocks, 0, 1).reshape(length, CHANNELS)
    return jnp.dot(mixed, output_weight, preferred_element_type=jnp.float32).astype(jnp.bfloat16)
```

```python
import functools
import math

import jax
import jax.numpy as jnp
from jax import lax
from jax.experimental import pallas as pl
from jax.experimental.pallas import tpu as pltpu
from jax.sharding import PartitionSpec as P

CHANNELS = 1024
FREQ_BANDS = 16
NORM_EPS = 1e-06
DECAY_SLOW = math.log(0.01) / 1.5
DECAY_FAST = math.log(0.01) / 0.3

F32 = jnp.float32
BF16 = jnp.bfloat16

SIN_COEFFS = (
    6.283182818555376,
    -41.34142139902321,
    81.59618388026023,
    -76.58010058967308,
    41.20539511150987,
    -12.271262699024827,
)


def sin_turns(turns):
    r = turns - jnp.floor(turns + 0.5)
    s = r * r
    acc = jnp.full_like(s, SIN_COEFFS[-1])
    for coeff in SIN_COEFFS[-2::-1]:
        acc = acc * s + coeff
    return acc * r


def split(value):
    high = value.astype(BF16)
    low = (value - high.astype(F32)).astype(BF16)
    return high, low


def iota(shape, dim):
    return lax.broadcasted_iota(jnp.int32, shape, dim)


def to_turns(index, period):
    return (index & (period - 1)).astype(F32) * (1.0 / period)


def row_dft_table():
    shape = (128, 192)
    k1, n1 = iota(shape, 0) & 63, iota(shape, 1) & 63
    turns = to_turns((2 * k1 + 1) * n1, 256)
    value = sin_turns(turns + jnp.where(iota(shape, 0) < 64, 0.25, 0.5))
    high = value.astype(BF16).astype(F32)
    return jnp.where(iota(shape, 1) < 128, high, value - high).astype(BF16)


def row_inverse_table(scale):
    shape = (64, 384)
    n1, k1 = iota(shape, 0), iota(shape, 1) & 63
    turns = to_turns((2 * k1 + 1) * n1, 256)
    value = sin_turns(turns + jnp.where((iota(shape, 1) & 64) == 0, 0.25, 0.5)) * scale
    high = value.astype(BF16).astype(F32)
    return jnp.where(iota(shape, 1) < 256, high, value - high).astype(BF16)


def twiddles():
    shape = (64, 128)
    turns = to_turns((2 * iota(shape, 0) + 1) * iota(shape, 1), 32768)
    return sin_turns(turns + 0.25), sin_turns(turns)


def lane_dft():
    shape = (128, 128)
    turns = to_turns(iota(shape, 0) * iota(shape, 1), 128)
    return split(sin_turns(turns + 0.25)), split(sin_turns(turns))


def dot(left, right):
    return jnp.dot(left, right, preferred_element_type=F32)


def stack3(value):
    high, low = split(value)
    return jnp.concatenate([high, low, high], axis=0)


def lanes3(value):
    high, low = split(value)
    return jnp.concatenate([high, low, high], axis=1)


def project_kernel(tokens, gain, w0, w1, w2, out, scratch):
    wide = tokens[...].astype(F32)
    scale = lax.rsqrt(jnp.mean(wide * wide, axis=1, keepdims=True) + NORM_EPS)
    normed = (wide * scale * gain[...]).astype(BF16)
    weights = jnp.concatenate([w0[...], w1[...], w2[...]], axis=1)
    gates = dot(normed, weights)
    for half in range(2):
        for branch in range(3):
            block = gates[half * 128 : half * 128 + 128, branch * 128 : branch * 128 + 128].T
            for peer in range(32):
                start = peer * 24 + half * 12 + branch * 4
                scratch[start : start + 4, :] = block[peer * 4 : peer * 4 + 4, :]
    out[...] = scratch[...].astype(BF16)


def filter_kernel(decay, ew, eb, iw, ib, freq, fw, hre, him, build, lhs1, lhs2, taps):
    length = 8192
    turns_of = freq[...] * (1.0 / (2.0 * math.pi))

    def high_of(value):
        return value.astype(BF16).astype(F32)

    embed = ew[...] * turns_of
    embed_bias = eb[...] * turns_of
    build[...] = jnp.zeros_like(build)
    build[0:33, 0:64] = high_of(embed)
    build[33:34, 0:64] = high_of(embed_bias)
    build[48:81, 0:64] = high_of(embed)
    build[96:129, 0:64] = embed - high_of(embed)
    build[129:130, 0:64] = embed_bias - high_of(embed_bias)
    lhs1[...] = build[...].T[0:64, :].astype(BF16)
    inner = iw[...] * turns_of
    inner_bias = ib[...] * turns_of
    build[...] = jnp.zeros_like(build)
    build[0:64, 0:64] = high_of(inner)
    build[64:128, 0:64] = high_of(inner)
    build[128:192, 0:64] = inner - high_of(inner)
    build[192:193, 0:64] = high_of(inner_bias)
    build[193:194, 0:64] = inner_bias - high_of(inner_bias)
    lhs2[...] = build[...].T[0:64, :].astype(BF16)
    left1 = lhs1[:, 0:144]
    left2 = lhs2[:, 0:208]
    parts = []
    for order in range(2):
        parts.append(fw[order, 0] + fw[order, 1])
        parts.append(fw[order, 0] - fw[order, 1])
    fweights = jnp.concatenate(parts, axis=0)
    fhigh, flow = split(fweights)
    left3 = jnp.concatenate([fhigh, fhigh, flow], axis=1)

    chunk = 1024
    row = iota((48, chunk), 0)
    band_index = jnp.where(row < 17, row - 1, row - 17).astype(F32)
    band_step = (FREQ_BANDS - 1 - 0.0001) / (FREQ_BANDS - 1)
    band = (0.0001 + band_index * band_step) * (1.0 / length)
    phase = jnp.where(row < 17, 0.25, 0.5)
    ones16 = jnp.ones((16, chunk), BF16)
    crow = iota((8, chunk), 0) & 3
    rate = jnp.where(
        crow < 2,
        jnp.where(crow == 0, decay[0], decay[1]),
        jnp.where(crow == 2, decay[2], decay[3]),
    )
    for step in range(length // chunk):
        position = (iota((1, chunk), 1) + step * chunk).astype(F32)
        ramp = position * (1.0 / (length - 1))
        feature = sin_turns(band * position + phase)
        feature = jnp.where(row == 0, ramp, jnp.where(row == 33, 1.0, feature))
        hidden = sin_turns(dot(left1, stack3(feature)))
        hidden = sin_turns(dot(left2, jnp.concatenate([stack3(hidden), ones16], axis=0)))
        value = dot(left3, stack3(hidden))
        window = jnp.exp(ramp * -rate)
        value = value * jnp.concatenate([window, window], axis=0)
        for block in range(chunk // 128):
            piece = value[:, block * 128 : block * 128 + 128]
            n1 = step * (chunk // 128) + block
            if n1 == 0:
                swapped = jnp.concatenate([piece[4:8], piece[0:4], piece[12:16], piece[8:12]], axis=0)
                piece = jnp.where(iota((16, 128), 1) == 0, 0.5 * (piece + swapped), piece)
            taps[n1 * 16 : n1 * 16 + 16, :] = piece

    spread = jnp.concatenate([taps[pl.ds(r, 64, stride=16), :] for r in range(16)], axis=1)
    stage = dot(row_dft_table(), stack3(spread))
    tw_cos, tw_sin = twiddles()
    (cos_high, cos_low), (sin_high, sin_low) = lane_dft()
    real_table = jnp.concatenate([cos_high, sin_high, cos_high, sin_high, cos_low, sin_low], axis=0)
    imag_table = jnp.concatenate([-sin_high, cos_high, -sin_high, cos_high, -sin_low, cos_low], axis=0)
    for kind, table, out in ((0, real_table, hre), (1, imag_table, him)):
        reals, imags = [], []
        for order in range(2):
            for channel in range(4):
                lane = (order * 8 + kind * 4 + channel) * 128
                real, imag = stage[0:64, lane : lane + 128], stage[64:128, lane : lane + 128]
                reals.append(real * tw_cos + imag * tw_sin)
                imags.append(imag * tw_cos - real * tw_sin)
        left = jnp.concatenate([jnp.concatenate(reals, axis=0), jnp.concatenate(imags, axis=0)], axis=1)
        out[...] = dot(lanes3(left), table)


def shifted(value, amount):
    size = 128
    lane, row = iota(value.shape, 1), iota(value.shape, 0)
    rolled = pltpu.roll(value, amount % size, 1)
    carried = pltpu.roll(rolled, amount % 64, 0)
    edge_lane = 0 if amount == 1 else size - 1
    edge_row = 0 if amount == 1 else 63
    carried = jnp.where(row == edge_row, 0.0, carried)
    return jnp.where(lane == edge_lane, carried, rolled)


def conv_kernel(scalars, moved, hre, him, out, wide, result):
    wide[...] = moved[...].astype(F32)
    smoothed = []
    for branch in range(3):
        rows = []
        for channel in range(4):
            value = wide[pl.ds(branch * 4 + channel, 64, stride=12), :]
            base = (branch * 4 + channel) * 4
            total = scalars[base] + shifted(value, 1) * scalars[base + 1]
            total = total + value * scalars[base + 2]
            total = total + shifted(value, -1) * scalars[base + 3]
            rows.append(total)
        smoothed.append(rows)
    forward_rows = row_dft_table()
    inverse_rows = row_inverse_table(1.0 / 8192)
    tw_cos, tw_sin = twiddles()
    (cos_high, cos_low), (sin_high, sin_low) = lane_dft()

    def table(sign):
        def part(cos, sin):
            top = jnp.concatenate([cos, -sin if sign > 0 else sin], axis=1)
            bottom = jnp.concatenate([sin if sign > 0 else -sin, cos], axis=1)
            return jnp.concatenate([top, bottom], axis=0)

        high, low = part(cos_high, sin_high), part(cos_low, sin_low)
        return jnp.concatenate([high, high, low], axis=0)

    forward_lanes, inverse_lanes = table(1), table(-1)
    signal = smoothed[2]
    for order in range(2):
        stage = dot(forward_rows, stack3(jnp.concatenate(signal, axis=1)))
        reals, imags = [], []
        for channel in range(4):
            real = stage[0:64, channel * 128 : channel * 128 + 128]
            imag = stage[64:128, channel * 128 : channel * 128 + 128]
            reals.append(real * tw_cos + imag * tw_sin)
            imags.append(imag * tw_cos - real * tw_sin)
        left = jnp.concatenate([jnp.concatenate(reals, axis=0), jnp.concatenate(imags, axis=0)], axis=1)
        spectrum = dot(lanes3(left), forward_lanes)
        real, imag = spectrum[:, 0:128], spectrum[:, 128:256]
        tap_real = hre[order * 256 : order * 256 + 256, :]
        tap_imag = him[order * 256 : order * 256 + 256, :]
        left = jnp.concatenate(
            [real * tap_real - imag * tap_imag, real * tap_imag + imag * tap_real], axis=1
        )
        back = dot(lanes3(left), inverse_lanes)
        columns = []
        for channel in range(4):
            real = back[channel * 64 : channel * 64 + 64, 0:128]
            imag = back[channel * 64 : channel * 64 + 64, 128:256]
            columns.append(
                jnp.concatenate([real * tw_cos - imag * tw_sin, real * tw_sin + imag * tw_cos], axis=0)
            )
        values = dot(inverse_rows, stack3(jnp.concatenate(columns, axis=1)))
        following = []
        for channel in range(4):
            skip = scalars[48 + order * 4 + channel]
            conv = values[:, channel * 128 : channel * 128 + 128] + signal[channel] * skip
            following.append(smoothed[order][channel] * conv)
        signal = following
    for channel in range(4):
        result[pl.ds(channel, 64, stride=4), :] = signal[channel]
    out[...] = result[...].astype(BF16)


def norm_kernel(moved, gain, out, wide, ordered):
    wide[...] = moved[...].astype(F32)
    for half in range(2):
        for channel in range(4):
            ordered[pl.ds(half * 128 + channel, 32, stride=4), :] = wide[
                pl.ds(half * 4 + channel, 32, stride=8), :
            ]
    for half in range(2):
        value = ordered[half * 128 : half * 128 + 128, :]
        scale = lax.rsqrt(jnp.mean(value * value, axis=0, keepdims=True) + NORM_EPS)
        out[half * 128 : half * 128 + 128, :] = ((value * scale).T * gain[...]).astype(BF16)


def output_kernel(mixed, weight, out):
    left = jnp.concatenate([mixed[c * 32 : c * 32 + 32, :] for c in range(8)], axis=1)
    out[...] = dot(left, weight[...]).astype(BF16)


VMEM = pl.BlockSpec(memory_space=pltpu.VMEM)
SMEM = pl.BlockSpec(memory_space=pltpu.SMEM)


def run(kernel, out_shape, in_specs, scratch, name, interpret=False):
    multi = isinstance(out_shape, (tuple, list))
    return pl.pallas_call(
        kernel,
        out_shape=out_shape,
        in_specs=in_specs,
        out_specs=tuple(VMEM for _ in out_shape) if multi else VMEM,
        scratch_shapes=scratch,
        name=name,
        interpret=interpret,
    )


def shape_of(shape, dtype):
    return jax.ShapeDtypeStruct(shape, dtype)


def local(
    tokens,
    norm_gain,
    first_gate,
    second_gate,
    value_weight,
    short_weight,
    short_bias,
    embed_weight,
    embed_bias,
    inner_weight,
    inner_bias,
    filter_freq,
    filter_weight,
    filter_skip,
    output_gain,
    output_weight,
):
    row_index = lax.axis_index("row")
    col_index = lax.axis_index("col")
    sent = run(
        project_kernel, shape_of((768, 128), BF16), [VMEM] * 5, [pltpu.VMEM((768, 128), F32)], "project"
    )(tokens, norm_gain.reshape(1, -1), first_gate, second_gate, value_weight)
    moved = lax.all_to_all(
        sent.reshape(32, 24, 128), "row", split_axis=0, concat_axis=0, tiled=True
    ).reshape(768, 128)

    channel = ((col_index * 32 + row_index) * 4 + jnp.arange(4)).astype(F32)
    decay = -(DECAY_SLOW + (DECAY_FAST - DECAY_SLOW) * (channel * (1.0 / (CHANNELS - 1))))
    hre, him = run(
        filter_kernel,
        (shape_of((512, 128), F32), shape_of((512, 128), F32)),
        [SMEM] + [VMEM] * 6,
        [
            pltpu.VMEM((256, 128), F32),
            pltpu.VMEM((64, 256), BF16),
            pltpu.VMEM((64, 256), BF16),
            pltpu.VMEM((1024, 128), F32),
        ],
        "filters",
    )(
        decay,
        embed_weight,
        embed_bias.reshape(1, -1),
        inner_weight,
        inner_bias.reshape(1, -1),
        filter_freq.reshape(1, -1),
        filter_weight.transpose(0, 1, 3, 2),
    )
    weights_own = lax.dynamic_slice_in_dim(short_weight, row_index * 4, 4, 2).astype(F32)
    bias_own = lax.dynamic_slice_in_dim(short_bias, row_index * 4, 4, 1)
    taps_own = jnp.concatenate([bias_own[:, None, :], weights_own], axis=1)
    scalars = jnp.concatenate([taps_own.transpose(0, 2, 1).reshape(-1), filter_skip.reshape(-1)])
    mixed = run(
        conv_kernel,
        shape_of((256, 128), BF16),
        [SMEM] + [VMEM] * 3,
        [pltpu.VMEM((768, 128), F32), pltpu.VMEM((256, 128), F32)],
        "convolve",
    )(scalars, moved, hre, him)
    result = lax.all_to_all(
        mixed.reshape(32, 8, 128), "row", split_axis=0, concat_axis=0, tiled=True
    ).reshape(256, 128)
    normed = run(
        norm_kernel,
        shape_of((256, 128), BF16),
        [VMEM] * 2,
        [pltpu.VMEM((256, 128), F32), pltpu.VMEM((256, 128), F32)],
        "groupnorm",
    )(result, output_gain.reshape(1, -1))
    gathered = lax.all_to_all(
        normed.reshape(8, 32, 128), "col", split_axis=0, concat_axis=0, tiled=True
    ).reshape(256, 128)
    return run(output_kernel, shape_of((32, 2048), BF16), [VMEM] * 2, [], "output")(
        gathered, output_weight
    )


def solution(mesh):
    in_specs = (
        P("row", None),
        P(),
        P(None, "col"),
        P(None, "col"),
        P(None, "col"),
        P(None, None, "col"),
        P(None, "col"),
        P(),
        P(),
        P(),
        P(),
        P(),
        P(None, None, None, ("col", "row")),
        P(None, ("col", "row")),
        P("col"),
        P(),
    )
    out_specs = P(("row", "col"), None)
    return jax.shard_map(local, mesh=mesh, in_specs=in_specs, out_specs=out_specs, check_vma=False)
```

```python
import functools
import math

import jax
import jax.numpy as jnp
from jax import lax
from jax.experimental import pallas as pl
from jax.experimental.pallas import tpu as pltpu
from jax.sharding import PartitionSpec as P

CHANNELS = 1024
FREQ_BANDS = 16
NORM_EPS = 1e-06
DECAY_SLOW = math.log(0.01) / 1.5
DECAY_FAST = math.log(0.01) / 0.3

F32 = jnp.float32
BF16 = jnp.bfloat16

SIN_COEFFS = (
    6.283182818555376,
    -41.34142139902321,
    81.59618388026023,
    -76.58010058967308,
    41.20539511150987,
    -12.271262699024827,
)


def sin_turns(turns):
    r = turns - jnp.floor(turns + 0.5)
    s = r * r
    acc = jnp.full_like(s, SIN_COEFFS[-1])
    for coeff in SIN_COEFFS[-2::-1]:
        acc = acc * s + coeff
    return acc * r


def split(value):
    high = value.astype(BF16)
    low = (value - high.astype(F32)).astype(BF16)
    return high, low


def iota(shape, dim):
    return lax.broadcasted_iota(jnp.int32, shape, dim)


def to_turns(index, period):
    return (index & (period - 1)).astype(F32) * (1.0 / period)


def row_dft_table():
    shape = (128, 192)
    k1, n1 = iota(shape, 0) & 63, iota(shape, 1) & 63
    turns = to_turns((2 * k1 + 1) * n1, 256)
    value = sin_turns(turns + jnp.where(iota(shape, 0) < 64, 0.25, 0.5))
    high = value.astype(BF16).astype(F32)
    return jnp.where(iota(shape, 1) < 128, high, value - high).astype(BF16)


def row_inverse_table(scale):
    shape = (64, 384)
    n1, k1 = iota(shape, 0), iota(shape, 1) & 63
    turns = to_turns((2 * k1 + 1) * n1, 256)
    value = sin_turns(turns + jnp.where((iota(shape, 1) & 64) == 0, 0.25, 0.5)) * scale
    high = value.astype(BF16).astype(F32)
    return jnp.where(iota(shape, 1) < 256, high, value - high).astype(BF16)


def twiddles():
    shape = (64, 128)
    turns = to_turns((2 * iota(shape, 0) + 1) * iota(shape, 1), 32768)
    return sin_turns(turns + 0.25), sin_turns(turns)


def lane_dft():
    shape = (128, 128)
    turns = to_turns(iota(shape, 0) * iota(shape, 1), 128)
    return split(sin_turns(turns + 0.25)), split(sin_turns(turns))


def dot(left, right):
    return jnp.dot(left, right, preferred_element_type=F32)


def stack3(value):
    high, low = split(value)
    return jnp.concatenate([high, low, high], axis=0)


def lanes3(value):
    high, low = split(value)
    return jnp.concatenate([high, low, high], axis=1)


def project_kernel(tokens, gain, w0, w1, w2, out, scratch):
    wide = tokens[...].astype(F32)
    scale = lax.rsqrt(jnp.mean(wide * wide, axis=1, keepdims=True) + NORM_EPS)
    normed = (wide * scale * gain[...]).astype(BF16)
    weights = jnp.concatenate([w0[...], w1[...], w2[...]], axis=1)
    gates = dot(normed, weights)
    for half in range(2):
        for branch in range(3):
            block = gates[half * 128 : half * 128 + 128, branch * 128 : branch * 128 + 128].T
            for peer in range(32):
                start = peer * 24 + half * 12 + branch * 4
                scratch[start : start + 4, :] = block[peer * 4 : peer * 4 + 4, :]
    out[...] = scratch[...].astype(BF16).reshape(32, 24, 128)


def lane_table(sign, cos, sin):
    def part(c, s):
        top = jnp.concatenate([c, -s if sign > 0 else s], axis=1)
        bottom = jnp.concatenate([s if sign > 0 else -s, c], axis=1)
        return jnp.concatenate([top, bottom], axis=0)

    high, low = part(cos[0], sin[0]), part(cos[1], sin[1])
    return jnp.concatenate([high, high, low], axis=0)


def filter_kernel(
    ew, eb, iw, ib, freq, fw, sw, sb, skip,
    hre, him, frows, irows, flanes, ilanes, twiddle, scalars,
    build, lhs1, lhs2, taps,
):
    length = 8192
    own = lax.axis_index("row") * 4
    first_channel = lax.axis_index("col") * 128 + own

    lines = []
    for branch in range(3):
        lines.append(sb[branch : branch + 1, :])
        lines.append(sw[branch].astype(F32))
    lines.append(jnp.zeros((4, 128), F32))
    lines = pltpu.roll(jnp.concatenate(lines, axis=0), (128 - own) % 128, 1)
    for channel in range(4):
        scalars[channel * 16 : channel * 16 + 16, :] = jnp.broadcast_to(
            lines[:, channel : channel + 1], (16, 128)
        )
        scalars[channel * 16 + 12 : channel * 16 + 14, :] = jnp.broadcast_to(
            skip[:, channel : channel + 1], (2, 128)
        )

    frows[...] = row_dft_table()
    irows[...] = row_inverse_table(1.0 / 8192)
    tw_cos, tw_sin = twiddles()
    twiddle[0:64, :] = tw_cos
    twiddle[64:128, :] = tw_sin
    cos, sin = lane_dft()
    flanes[...] = lane_table(1, cos, sin)
    ilanes[...] = lane_table(-1, cos, sin)

    def high_of(value):
        return value.astype(BF16).astype(F32)

    turns_of = freq[...] * (1.0 / (2.0 * math.pi))
    build[...] = jnp.zeros_like(build)
    embed = ew[...] * turns_of
    bias = eb[...] * turns_of
    rows = jnp.concatenate([embed[1:33], embed[0:1], bias], axis=0)
    build[0:34, 0:64] = high_of(rows)
    build[48:82, 0:64] = high_of(rows)
    build[96:130, 0:64] = rows - high_of(rows)
    lhs1[...] = build[...].T[0:64, :].astype(BF16)
    inner = iw[...] * turns_of
    bias = ib[...] * turns_of
    build[...] = jnp.zeros_like(build)
    build[0:64, 0:64] = high_of(inner)
    build[64:128, 0:64] = high_of(inner)
    build[128:192, 0:64] = inner - high_of(inner)
    build[192:193, 0:64] = high_of(bias)
    build[193:194, 0:64] = bias - high_of(bias)
    lhs2[...] = build[...].T[0:64, :].astype(BF16)
    left1 = lhs1[:, 0:144]
    left2 = lhs2[:, 0:208]
    parts = []
    for order in range(2):
        parts.append(fw[order, 0] + fw[order, 1])
        parts.append(fw[order, 0] - fw[order, 1])
    fhigh, flow = split(jnp.concatenate(parts, axis=0))
    left3 = jnp.concatenate([fhigh, fhigh, flow], axis=1)

    band_step = (FREQ_BANDS - 1 - 0.0001) / (FREQ_BANDS - 1)
    band = 0.0001 + iota((16, 128), 0).astype(F32) * band_step
    lane = iota((16, 128), 1).astype(F32)
    coarse = band * (lane * (128.0 / length))
    fine = band * (lane * (1.0 / length))
    coarse_cos, coarse_sin = sin_turns(coarse + 0.25), sin_turns(coarse)
    fine_cos, fine_sin = sin_turns(fine + 0.25), sin_turns(fine)
    row = iota((16, 128), 0)
    extra = jnp.where(row == 0, lane * (1.0 / (length - 1)), jnp.where(row == 1, 1.0, 0.0))
    extra_step = jnp.where(row == 0, 128.0 / (length - 1), 0.0)

    rate_step = (DECAY_SLOW - DECAY_FAST) / (CHANNELS - 1)
    channel_row = (iota((8, 128), 0) & 3) + first_channel
    rate = -DECAY_SLOW + channel_row.astype(F32) * rate_step
    ramp = iota((8, 128), 1).astype(F32) * (1.0 / (length - 1))

    chunk = 1024
    blocks = chunk // 128
    ones16 = jnp.ones((16, chunk), BF16)
    for step in range(length // chunk):
        feature = []
        for block in range(blocks):
            n1 = step * blocks + block
            ca = jnp.broadcast_to(coarse_cos[:, n1 : n1 + 1], (16, 128))
            sa = jnp.broadcast_to(coarse_sin[:, n1 : n1 + 1], (16, 128))
            feature.append(
                jnp.concatenate(
                    [
                        ca * fine_cos - sa * fine_sin,
                        -(sa * fine_cos + ca * fine_sin),
                        extra + extra_step * float(n1),
                    ],
                    axis=0,
                )
            )
        hidden = sin_turns(dot(left1, stack3(jnp.concatenate(feature, axis=1))))
        hidden = sin_turns(dot(left2, jnp.concatenate([stack3(hidden), ones16], axis=0)))
        value = dot(left3, stack3(hidden))
        for block in range(blocks):
            n1 = step * blocks + block
            window = jnp.exp((ramp + n1 * 128.0 / (length - 1)) * -rate)
            piece = value[:, block * 128 : block * 128 + 128] * jnp.concatenate([window, window], axis=0)
            if n1 == 0:
                swapped = jnp.concatenate([piece[4:8], piece[0:4], piece[12:16], piece[8:12]], axis=0)
                piece = jnp.where(iota((16, 128), 1) == 0, 0.5 * (piece + swapped), piece)
            taps[n1 * 16 : n1 * 16 + 16, :] = piece

    spread = jnp.concatenate([taps[pl.ds(r, 64, stride=16), :] for r in range(16)], axis=1)
    stage = dot(frows[...], stack3(spread))
    (cos_high, cos_low), (sin_high, sin_low) = cos, sin
    real_table = jnp.concatenate([cos_high, sin_high, cos_high, sin_high, cos_low, sin_low], axis=0)
    imag_table = jnp.concatenate([-sin_high, cos_high, -sin_high, cos_high, -sin_low, cos_low], axis=0)
    for kind, table, out in ((0, real_table, hre), (1, imag_table, him)):
        reals, imags = [], []
        for order in range(2):
            for channel in range(4):
                at = (order * 8 + kind * 4 + channel) * 128
                real, imag = stage[0:64, at : at + 128], stage[64:128, at : at + 128]
                reals.append(real * tw_cos + imag * tw_sin)
                imags.append(imag * tw_cos - real * tw_sin)
        left = jnp.concatenate([jnp.concatenate(reals, axis=0), jnp.concatenate(imags, axis=0)], axis=1)
        out[...] = dot(lanes3(left), table)


def shifted(value, amount):
    size = 128
    lane, row = iota(value.shape, 1), iota(value.shape, 0)
    rolled = pltpu.roll(value, amount % size, 1)
    carried = pltpu.roll(rolled, amount % 64, 0)
    edge_lane = 0 if amount == 1 else size - 1
    edge_row = 0 if amount == 1 else 63
    carried = jnp.where(row == edge_row, 0.0, carried)
    return jnp.where(lane == edge_lane, carried, rolled)


def conv_kernel(
    moved, hre, him, frows, irows, flanes, ilanes, twiddle, scalars, weight, out, kept, wide, result, arrived
):
    fetch = pltpu.make_async_copy(weight, kept, arrived)
    fetch.start()
    wide[...] = moved[...].astype(F32).reshape(768, 128)
    smoothed = []
    for branch in range(3):
        rows = []
        for channel in range(4):
            value = wide[pl.ds(branch * 4 + channel, 64, stride=12), :]
            base = channel * 16 + branch * 4
            total = scalars[base : base + 1, :] + shifted(value, 1) * scalars[base + 1 : base + 2, :]
            total = total + value * scalars[base + 2 : base + 3, :]
            total = total + shifted(value, -1) * scalars[base + 3 : base + 4, :]
            rows.append(total)
        smoothed.append(rows)
    forward_rows, inverse_rows = frows[...], irows[...]
    forward_lanes, inverse_lanes = flanes[...], ilanes[...]
    tw_cos, tw_sin = twiddle[0:64, :], twiddle[64:128, :]
    signal = smoothed[2]
    for order in range(2):
        stage = dot(forward_rows, stack3(jnp.concatenate(signal, axis=1)))
        reals, imags = [], []
        for channel in range(4):
            real = stage[0:64, channel * 128 : channel * 128 + 128]
            imag = stage[64:128, channel * 128 : channel * 128 + 128]
            reals.append(real * tw_cos + imag * tw_sin)
            imags.append(imag * tw_cos - real * tw_sin)
        left = jnp.concatenate([jnp.concatenate(reals, axis=0), jnp.concatenate(imags, axis=0)], axis=1)
        spectrum = dot(lanes3(left), forward_lanes)
        real, imag = spectrum[:, 0:128], spectrum[:, 128:256]
        tap_real = hre[order * 256 : order * 256 + 256, :]
        tap_imag = him[order * 256 : order * 256 + 256, :]
        left = jnp.concatenate(
            [real * tap_real - imag * tap_imag, real * tap_imag + imag * tap_real], axis=1
        )
        back = dot(lanes3(left), inverse_lanes)
        columns = []
        for channel in range(4):
            real = back[channel * 64 : channel * 64 + 64, 0:128]
            imag = back[channel * 64 : channel * 64 + 64, 128:256]
            columns.append(
                jnp.concatenate([real * tw_cos - imag * tw_sin, real * tw_sin + imag * tw_cos], axis=0)
            )
        values = dot(inverse_rows, stack3(jnp.concatenate(columns, axis=1)))
        following = []
        for channel in range(4):
            at = channel * 16 + 12 + order
            skip = scalars[at : at + 1, :]
            conv = values[:, channel * 128 : channel * 128 + 128] + signal[channel] * skip
            following.append(smoothed[order][channel] * conv)
        signal = following
    for channel in range(4):
        result[pl.ds(channel, 64, stride=4), :] = signal[channel]
    out[...] = result[...].astype(BF16).reshape(32, 8, 128)
    fetch.wait()


def norm_kernel(moved, gain, out, wide, ordered):
    wide[...] = moved[...].astype(F32).reshape(256, 128)
    for half in range(2):
        for channel in range(4):
            ordered[pl.ds(half * 128 + channel, 32, stride=4), :] = wide[
                pl.ds(half * 4 + channel, 32, stride=8), :
            ]
    for half in range(2):
        value = ordered[half * 128 : half * 128 + 128, :]
        scale = lax.rsqrt(jnp.mean(value * value, axis=0, keepdims=True) + NORM_EPS)
        normed = ((value * scale).T * gain[...]).astype(BF16)
        out[half * 4 : half * 4 + 4] = normed.reshape(4, 32, 128)


def output_kernel(mixed, weight, out):
    left = jnp.concatenate([mixed[c] for c in range(8)], axis=1)
    out[...] = dot(left, weight[...]).astype(BF16)


VMEM = pl.BlockSpec(memory_space=pltpu.VMEM)
HBM = pl.BlockSpec(memory_space=pltpu.HBM)


def run(kernel, out_shape, inputs, scratch, name, unread=0):
    multi = isinstance(out_shape, (tuple, list))
    return pl.pallas_call(
        kernel,
        out_shape=out_shape,
        in_specs=[VMEM] * (len(inputs) - unread) + [HBM] * unread,
        out_specs=tuple(VMEM for _ in out_shape) if multi else VMEM,
        scratch_shapes=scratch,
        name=name,
        compiler_params=pltpu.CompilerParams(vmem_limit_bytes=24 * 1024 * 1024),
    )(*inputs)


def near(value):
    return pltpu.with_memory_space_constraint(value, pltpu.VMEM)


def far(*values):
    return tuple(pltpu.with_memory_space_constraint(value, pltpu.HBM) for value in values)


def local(
    tokens,
    norm_gain,
    first_gate,
    second_gate,
    value_weight,
    short_weight,
    short_bias,
    embed_weight,
    embed_bias,
    inner_weight,
    inner_bias,
    filter_freq,
    filter_weight,
    filter_skip,
    output_gain,
    output_weight,
):
    sent = run(
        project_kernel,
        pltpu.VMEM((32, 24, 128), BF16),
        far(tokens, norm_gain.reshape(1, -1), first_gate, second_gate, value_weight),
        [pltpu.VMEM((768, 128), F32)],
        "project",
    )
    moved = lax.all_to_all(sent, "row", split_axis=0, concat_axis=0, tiled=True)
    prepared = run(
        filter_kernel,
        (
            pltpu.VMEM((512, 128), F32),
            pltpu.VMEM((512, 128), F32),
            pltpu.VMEM((128, 192), BF16),
            pltpu.VMEM((64, 384), BF16),
            pltpu.VMEM((768, 256), BF16),
            pltpu.VMEM((768, 256), BF16),
            pltpu.VMEM((128, 128), F32),
            pltpu.VMEM((64, 128), F32),
        ),
        far(
            embed_weight,
            embed_bias.reshape(1, -1),
            inner_weight,
            inner_bias.reshape(1, -1),
            filter_freq.reshape(1, -1),
            filter_weight.transpose(0, 1, 3, 2),
            short_weight,
            short_bias,
            filter_skip,
        ),
        [
            pltpu.VMEM((256, 128), F32),
            pltpu.VMEM((64, 256), BF16),
            pltpu.VMEM((64, 256), BF16),
            pltpu.VMEM((1024, 128), F32),
        ],
        "filters",
    )
    mixed, kept = run(
        conv_kernel,
        (pltpu.VMEM((32, 8, 128), BF16), pltpu.VMEM((1024, 2048), BF16)),
        (*(near(value) for value in (moved, *prepared)), *far(output_weight)),
        [pltpu.VMEM((768, 128), F32), pltpu.VMEM((256, 128), F32), pltpu.SemaphoreType.DMA],
        "convolve",
        1,
    )
    result = lax.all_to_all(mixed, "row", split_axis=0, concat_axis=0, tiled=True)
    normed = run(
        norm_kernel,
        pltpu.VMEM((8, 32, 128), BF16),
        (near(result), *far(output_gain.reshape(1, -1))),
        [pltpu.VMEM((256, 128), F32), pltpu.VMEM((256, 128), F32)],
        "groupnorm",
    )
    gathered = lax.all_to_all(normed, "col", split_axis=0, concat_axis=0, tiled=True)
    return run(
        output_kernel,
        jax.ShapeDtypeStruct((32, 2048), BF16),
        (near(gathered), near(kept)),
        [],
        "output",
    )


def solution(mesh):
    in_specs = (
        P("row", None),
        P(),
        P(None, "col"),
        P(None, "col"),
        P(None, "col"),
        P(None, None, "col"),
        P(None, "col"),
        P(),
        P(),
        P(),
        P(),
        P(),
        P(None, None, None, ("col", "row")),
        P(None, ("col", "row")),
        P("col"),
        P(),
    )
    out_specs = P(("row", "col"), None)
    return jax.shard_map(local, mesh=mesh, in_specs=in_specs, out_specs=out_specs, check_vma=False)
```

```python
import functools
import math

import jax
import jax.numpy as jnp
from jax import lax
from jax.experimental import pallas as pl
from jax.experimental.pallas import tpu as pltpu
from jax.sharding import PartitionSpec as P

CHANNELS = 1024
FREQ_BANDS = 16
NORM_EPS = 1e-06
DECAY_SLOW = math.log(0.01) / 1.5
DECAY_FAST = math.log(0.01) / 0.3

F32 = jnp.float32
BF16 = jnp.bfloat16

SIN_COEFFS = (
    6.283182818555376,
    -41.34142139902321,
    81.59618388026023,
    -76.58010058967308,
    41.20539511150987,
    -12.271262699024827,
)


def sin_turns(turns):
    r = turns - jnp.floor(turns + 0.5)
    s = r * r
    acc = jnp.full_like(s, SIN_COEFFS[-1])
    for coeff in SIN_COEFFS[-2::-1]:
        acc = acc * s + coeff
    return acc * r


def split(value):
    high = value.astype(BF16)
    low = (value - high.astype(F32)).astype(BF16)
    return high, low


def iota(shape, dim):
    return lax.broadcasted_iota(jnp.int32, shape, dim)


def to_turns(index, period):
    return (index & (period - 1)).astype(F32) * (1.0 / period)


def row_dft_table():
    shape = (128, 192)
    k1, n1 = iota(shape, 0) & 63, iota(shape, 1) & 63
    turns = to_turns((2 * k1 + 1) * n1, 256)
    value = sin_turns(turns + jnp.where(iota(shape, 0) < 64, 0.25, 0.5))
    high = value.astype(BF16).astype(F32)
    return jnp.where(iota(shape, 1) < 128, high, value - high).astype(BF16)


def row_inverse_table(scale):
    shape = (64, 384)
    n1, k1 = iota(shape, 0), iota(shape, 1) & 63
    turns = to_turns((2 * k1 + 1) * n1, 256)
    value = sin_turns(turns + jnp.where((iota(shape, 1) & 64) == 0, 0.25, 0.5)) * scale
    high = value.astype(BF16).astype(F32)
    return jnp.where(iota(shape, 1) < 256, high, value - high).astype(BF16)


def twiddles():
    shape = (64, 128)
    turns = to_turns((2 * iota(shape, 0) + 1) * iota(shape, 1), 32768)
    return sin_turns(turns + 0.25), sin_turns(turns)


def lane_dft():
    shape = (128, 128)
    turns = to_turns(iota(shape, 0) * iota(shape, 1), 128)
    return split(sin_turns(turns + 0.25)), split(sin_turns(turns))


def dot(left, right):
    return jnp.dot(left, right, preferred_element_type=F32)


def stack3(value):
    high, low = split(value)
    return jnp.concatenate([high, low, high], axis=0)


def lanes3(value):
    high, low = split(value)
    return jnp.concatenate([high, low, high], axis=1)


def project_kernel(*refs):
    count = len(refs) - 15
    tokens, gain, w0, w1, w2 = refs[0:5]
    small = refs[5 : 5 + count // 2]
    out = refs[5 + count // 2]
    carried = refs[6 + count // 2 : 6 + count]
    near_tokens, near_gain, n0, n1, n2, normed, scratch, arrived, carry = refs[6 + count :]
    rows = 64
    copies = [pltpu.make_async_copy(gain, near_gain, arrived.at[0])]
    for part in range(4):
        where = pl.ds(part * rows, rows)
        copies.append(pltpu.make_async_copy(tokens.at[where], near_tokens.at[where], arrived.at[part + 1]))
    for index, (source, target) in enumerate(((w0, n0), (w1, n1), (w2, n2))):
        copies.append(pltpu.make_async_copy(source, target, arrived.at[index + 5]))
    carries = [
        pltpu.make_async_copy(source, target, carry.at[index])
        for index, (source, target) in enumerate(zip(small, carried))
    ]
    for copy in copies + carries:
        copy.start()
    copies[0].wait()
    for part in range(4):
        copies[part + 1].wait()
        wide = near_tokens[part * rows : part * rows + rows, :].astype(F32)
        scale = lax.rsqrt(jnp.mean(wide * wide, axis=1, keepdims=True) + NORM_EPS)
        normed[part * rows : part * rows + rows, :] = (wide * scale * near_gain[...]).astype(BF16)
    for copy in copies[5:]:
        copy.wait()
    weights = jnp.concatenate([n0[...], n1[...], n2[...]], axis=1)
    for half in range(2):
        gates = dot(normed[half * 128 : half * 128 + 128, :], weights)
        for branch in range(3):
            block = gates[:, branch * 128 : branch * 128 + 128].T
            for peer in range(32):
                start = peer * 24 + half * 12 + branch * 4
                scratch[start : start + 4, :] = block[peer * 4 : peer * 4 + 4, :]
    out[...] = scratch[...].astype(BF16).reshape(32, 24, 128)
    for copy in carries:
        copy.wait()


def lane_table(sign, cos, sin):
    def part(c, s):
        top = jnp.concatenate([c, -s if sign > 0 else s], axis=1)
        bottom = jnp.concatenate([s if sign > 0 else -s, c], axis=1)
        return jnp.concatenate([top, bottom], axis=0)

    high, low = part(cos[0], sin[0]), part(cos[1], sin[1])
    return jnp.concatenate([high, high, low], axis=0)


def filter_kernel(
    ew, eb, iw, ib, freq, fw, sw, sb, skip,
    hre, him, frows, irows, flanes, ilanes, twiddle, scalars,
    build, lhs1, lhs2, taps,
):
    length = 8192
    own = lax.axis_index("row") * 4
    first_channel = lax.axis_index("col") * 128 + own

    lines = []
    for branch in range(3):
        lines.append(sb[branch : branch + 1, :])
        lines.append(sw[branch].astype(F32))
    lines.append(jnp.zeros((4, 128), F32))
    lines = pltpu.roll(jnp.concatenate(lines, axis=0), (128 - own) % 128, 1)
    for channel in range(4):
        scalars[channel * 16 : channel * 16 + 16, :] = jnp.broadcast_to(
            lines[:, channel : channel + 1], (16, 128)
        )
        scalars[channel * 16 + 12 : channel * 16 + 14, :] = jnp.broadcast_to(
            skip[:, channel : channel + 1], (2, 128)
        )

    frows[...] = row_dft_table()
    irows[...] = row_inverse_table(1.0 / 8192)
    tw_cos, tw_sin = twiddles()
    twiddle[0:64, :] = tw_cos
    twiddle[64:128, :] = tw_sin
    cos, sin = lane_dft()
    flanes[...] = lane_table(1, cos, sin)
    ilanes[...] = lane_table(-1, cos, sin)

    def high_of(value):
        return value.astype(BF16).astype(F32)

    turns_of = freq[...] * (1.0 / (2.0 * math.pi))
    build[...] = jnp.zeros_like(build)
    embed = ew[...] * turns_of
    bias = eb[...] * turns_of
    rows = jnp.concatenate([embed[1:33], embed[0:1], bias], axis=0)
    build[0:34, 0:64] = high_of(rows)
    build[48:82, 0:64] = high_of(rows)
    build[96:130, 0:64] = rows - high_of(rows)
    lhs1[...] = build[...].T[0:64, :].astype(BF16)
    inner = iw[...] * turns_of
    bias = ib[...] * turns_of
    build[...] = jnp.zeros_like(build)
    build[0:64, 0:64] = high_of(inner)
    build[64:128, 0:64] = high_of(inner)
    build[128:192, 0:64] = inner - high_of(inner)
    build[192:193, 0:64] = high_of(bias)
    build[193:194, 0:64] = bias - high_of(bias)
    lhs2[...] = build[...].T[0:64, :].astype(BF16)
    left1 = lhs1[:, 0:144]
    left2 = lhs2[:, 0:208]
    parts = []
    for order in range(2):
        parts.append(fw[order, 0] + fw[order, 1])
        parts.append(fw[order, 0] - fw[order, 1])
    fhigh, flow = split(jnp.concatenate(parts, axis=0))
    left3 = jnp.concatenate([fhigh, flow], axis=1)

    band_step = (FREQ_BANDS - 1 - 0.0001) / (FREQ_BANDS - 1)
    band = 0.0001 + iota((16, 128), 0).astype(F32) * band_step
    lane = iota((16, 128), 1).astype(F32)
    coarse = band * (lane * (128.0 / length))
    fine = band * (lane * (1.0 / length))
    coarse_cos, coarse_sin = sin_turns(coarse + 0.25), sin_turns(coarse)
    fine_cos, fine_sin = sin_turns(fine + 0.25), sin_turns(fine)
    row = iota((16, 128), 0)
    extra = jnp.where(row == 0, lane * (1.0 / (length - 1)), jnp.where(row == 1, 1.0, 0.0))
    extra_step = jnp.where(row == 0, 128.0 / (length - 1), 0.0)

    rate_step = (DECAY_SLOW - DECAY_FAST) / (CHANNELS - 1)
    channel_row = (iota((8, 128), 0) & 3) + first_channel
    rate = -DECAY_SLOW + channel_row.astype(F32) * rate_step
    ramp = iota((8, 128), 1).astype(F32) * (1.0 / (length - 1))

    chunk = 1024
    blocks = chunk // 128
    ones16 = jnp.ones((16, chunk), BF16)
    for step in range(length // chunk):
        feature = []
        for block in range(blocks):
            n1 = step * blocks + block
            ca = jnp.broadcast_to(coarse_cos[:, n1 : n1 + 1], (16, 128))
            sa = jnp.broadcast_to(coarse_sin[:, n1 : n1 + 1], (16, 128))
            feature.append(
                jnp.concatenate(
                    [
                        ca * fine_cos - sa * fine_sin,
                        -(sa * fine_cos + ca * fine_sin),
                        extra + extra_step * float(n1),
                    ],
                    axis=0,
                )
            )
        hidden = sin_turns(dot(left1, stack3(jnp.concatenate(feature, axis=1))))
        hidden = sin_turns(dot(left2, jnp.concatenate([stack3(hidden), ones16], axis=0)))
        high = hidden.astype(BF16)
        value = dot(left3, jnp.concatenate([high, high], axis=0))
        for block in range(blocks):
            n1 = step * blocks + block
            window = jnp.exp((ramp + n1 * 128.0 / (length - 1)) * -rate)
            piece = value[:, block * 128 : block * 128 + 128] * jnp.concatenate([window, window], axis=0)
            if n1 == 0:
                swapped = jnp.concatenate([piece[4:8], piece[0:4], piece[12:16], piece[8:12]], axis=0)
                piece = jnp.where(iota((16, 128), 1) == 0, 0.5 * (piece + swapped), piece)
            taps[n1 * 16 : n1 * 16 + 16, :] = piece

    spread = jnp.concatenate([taps[pl.ds(r, 64, stride=16), :] for r in range(16)], axis=1)
    stage = dot(frows[...], stack3(spread))
    (cos_high, cos_low), (sin_high, sin_low) = cos, sin
    real_table = jnp.concatenate([cos_high, sin_high, cos_low, sin_low], axis=0)
    imag_table = jnp.concatenate([-sin_high, cos_high, -sin_low, cos_low], axis=0)
    for kind, table, out in ((0, real_table, hre), (1, imag_table, him)):
        reals, imags = [], []
        for order in range(2):
            for channel in range(4):
                at = (order * 8 + kind * 4 + channel) * 128
                real, imag = stage[0:64, at : at + 128], stage[64:128, at : at + 128]
                reals.append(real * tw_cos + imag * tw_sin)
                imags.append(imag * tw_cos - real * tw_sin)
        left = jnp.concatenate([jnp.concatenate(reals, axis=0), jnp.concatenate(imags, axis=0)], axis=1)
        left = left.astype(BF16)
        out[...] = dot(jnp.concatenate([left, left], axis=1), table)


def shifted(value, amount):
    size = 128
    lane, row = iota(value.shape, 1), iota(value.shape, 0)
    rolled = pltpu.roll(value, amount % size, 1)
    carried = pltpu.roll(rolled, amount % 64, 0)
    edge_lane = 0 if amount == 1 else size - 1
    edge_row = 0 if amount == 1 else 63
    carried = jnp.where(row == edge_row, 0.0, carried)
    return jnp.where(lane == edge_lane, carried, rolled)


def conv_kernel(
    moved, hre, him, frows, irows, flanes, ilanes, twiddle, scalars, weight, out, kept, wide, result, arrived
):
    fetch = pltpu.make_async_copy(weight, kept, arrived)
    fetch.start()
    wide[...] = moved[...].astype(F32).reshape(768, 128)
    smoothed = []
    for branch in range(3):
        rows = []
        for channel in range(4):
            value = wide[pl.ds(branch * 4 + channel, 64, stride=12), :]
            base = channel * 16 + branch * 4
            total = scalars[base : base + 1, :] + shifted(value, 1) * scalars[base + 1 : base + 2, :]
            total = total + value * scalars[base + 2 : base + 3, :]
            total = total + shifted(value, -1) * scalars[base + 3 : base + 4, :]
            rows.append(total)
        smoothed.append(rows)
    forward_rows, inverse_rows = frows[...], irows[...]
    forward_lanes, inverse_lanes = flanes[...], ilanes[...]
    tw_cos, tw_sin = twiddle[0:64, :], twiddle[64:128, :]
    signal = smoothed[2]
    for order in range(2):
        following = []
        for pair in ((0, 1), (2, 3)):
            stage = dot(forward_rows, stack3(jnp.concatenate([signal[c] for c in pair], axis=1)))
            reals, imags = [], []
            for place in range(2):
                real = stage[0:64, place * 128 : place * 128 + 128]
                imag = stage[64:128, place * 128 : place * 128 + 128]
                reals.append(real * tw_cos + imag * tw_sin)
                imags.append(imag * tw_cos - real * tw_sin)
            left = jnp.concatenate([jnp.concatenate(reals, axis=0), jnp.concatenate(imags, axis=0)], axis=1)
            spectrum = dot(lanes3(left), forward_lanes)
            real, imag = spectrum[:, 0:128], spectrum[:, 128:256]
            at = order * 256 + pair[0] * 64
            tap_real, tap_imag = hre[at : at + 128, :], him[at : at + 128, :]
            left = jnp.concatenate(
                [real * tap_real - imag * tap_imag, real * tap_imag + imag * tap_real], axis=1
            )
            back = dot(lanes3(left), inverse_lanes)
            columns = []
            for place in range(2):
                real = back[place * 64 : place * 64 + 64, 0:128]
                imag = back[place * 64 : place * 64 + 64, 128:256]
                columns.append(
                    jnp.concatenate([real * tw_cos - imag * tw_sin, real * tw_sin + imag * tw_cos], axis=0)
                )
            values = dot(inverse_rows, stack3(jnp.concatenate(columns, axis=1)))
            for place, channel in enumerate(pair):
                at = channel * 16 + 12 + order
                conv = values[:, place * 128 : place * 128 + 128] + signal[channel] * scalars[at : at + 1, :]
                following.append(smoothed[order][channel] * conv)
        signal = following
    for channel in range(4):
        result[pl.ds(channel, 64, stride=4), :] = signal[channel]
    out[...] = result[...].astype(BF16).reshape(32, 8, 128)
    fetch.wait()


def norm_kernel(moved, gain, out, wide, ordered):
    wide[...] = moved[...].astype(F32).reshape(256, 128)
    for half in range(2):
        for channel in range(4):
            ordered[pl.ds(half * 128 + channel, 32, stride=4), :] = wide[
                pl.ds(half * 4 + channel, 32, stride=8), :
            ]
    for half in range(2):
        value = ordered[half * 128 : half * 128 + 128, :]
        scale = lax.rsqrt(jnp.mean(value * value, axis=0, keepdims=True) + NORM_EPS)
        normed = ((value * scale).T * gain[...]).astype(BF16)
        out[half * 4 : half * 4 + 4] = normed.reshape(4, 32, 128)


def output_kernel(mixed, weight, out):
    left = jnp.concatenate([mixed[c] for c in range(8)], axis=1)
    out[...] = dot(left, weight[...]).astype(BF16)


VMEM = pl.BlockSpec(memory_space=pltpu.VMEM)
HBM = pl.BlockSpec(memory_space=pltpu.HBM)


def run(kernel, out_shape, inputs, scratch, name, unread=0):
    multi = isinstance(out_shape, (tuple, list))
    return pl.pallas_call(
        kernel,
        out_shape=out_shape,
        in_specs=[VMEM] * (len(inputs) - unread) + [HBM] * unread,
        out_specs=tuple(VMEM for _ in out_shape) if multi else VMEM,
        scratch_shapes=scratch,
        name=name,
        compiler_params=pltpu.CompilerParams(vmem_limit_bytes=24 * 1024 * 1024),
    )(*inputs)


def near(value):
    return pltpu.with_memory_space_constraint(value, pltpu.VMEM)


def far(*values):
    return tuple(pltpu.with_memory_space_constraint(value, pltpu.HBM) for value in values)


def local(
    tokens,
    norm_gain,
    first_gate,
    second_gate,
    value_weight,
    short_weight,
    short_bias,
    embed_weight,
    embed_bias,
    inner_weight,
    inner_bias,
    filter_freq,
    filter_weight,
    filter_skip,
    output_gain,
    output_weight,
):
    small = (
        embed_weight,
        embed_bias.reshape(1, -1),
        inner_weight,
        inner_bias.reshape(1, -1),
        filter_freq.reshape(1, -1),
        filter_weight.transpose(0, 1, 3, 2),
        short_weight,
        short_bias,
        filter_skip,
        output_gain.reshape(1, -1),
    )
    sent, *small = run(
        project_kernel,
        (pltpu.VMEM((32, 24, 128), BF16), *(pltpu.VMEM(value.shape, value.dtype) for value in small)),
        far(tokens, norm_gain.reshape(1, -1), first_gate, second_gate, value_weight, *small),
        [
            pltpu.VMEM((256, 2048), BF16),
            pltpu.VMEM((1, 2048), F32),
            pltpu.VMEM((2048, 128), BF16),
            pltpu.VMEM((2048, 128), BF16),
            pltpu.VMEM((2048, 128), BF16),
            pltpu.VMEM((256, 2048), BF16),
            pltpu.VMEM((768, 128), F32),
            pltpu.SemaphoreType.DMA((8,)),
            pltpu.SemaphoreType.DMA((len(small),)),
        ],
        "project",
        5 + len(small),
    )
    moved = lax.all_to_all(sent, "row", split_axis=0, concat_axis=0, tiled=True)
    prepared = run(
        filter_kernel,
        (
            pltpu.VMEM((512, 128), F32),
            pltpu.VMEM((512, 128), F32),
            pltpu.VMEM((128, 192), BF16),
            pltpu.VMEM((64, 384), BF16),
            pltpu.VMEM((768, 256), BF16),
            pltpu.VMEM((768, 256), BF16),
            pltpu.VMEM((128, 128), F32),
            pltpu.VMEM((64, 128), F32),
        ),
        tuple(near(value) for value in small[:9]),
        [
            pltpu.VMEM((256, 128), F32),
            pltpu.VMEM((64, 256), BF16),
            pltpu.VMEM((64, 256), BF16),
            pltpu.VMEM((1024, 128), F32),
        ],
        "filters",
    )
    mixed, kept = run(
        conv_kernel,
        (pltpu.VMEM((32, 8, 128), BF16), pltpu.VMEM((1024, 2048), BF16)),
        (*(near(value) for value in (moved, *prepared)), *far(output_weight)),
        [pltpu.VMEM((768, 128), F32), pltpu.VMEM((256, 128), F32), pltpu.SemaphoreType.DMA],
        "convolve",
        1,
    )
    result = lax.all_to_all(mixed, "row", split_axis=0, concat_axis=0, tiled=True)
    normed = run(
        norm_kernel,
        pltpu.VMEM((8, 32, 128), BF16),
        (near(result), near(small[9])),
        [pltpu.VMEM((256, 128), F32), pltpu.VMEM((256, 128), F32)],
        "groupnorm",
    )
    gathered = lax.all_to_all(normed, "col", split_axis=0, concat_axis=0, tiled=True)
    return run(
        output_kernel,
        jax.ShapeDtypeStruct((32, 2048), BF16),
        (near(gathered), near(kept)),
        [],
        "output",
    )


def solution(mesh):
    in_specs = (
        P("row", None),
        P(),
        P(None, "col"),
        P(None, "col"),
        P(None, "col"),
        P(None, None, "col"),
        P(None, "col"),
        P(),
        P(),
        P(),
        P(),
        P(),
        P(None, None, None, ("col", "row")),
        P(None, ("col", "row")),
        P("col"),
        P(),
    )
    out_specs = P(("row", "col"), None)
    return jax.shard_map(local, mesh=mesh, in_specs=in_specs, out_specs=out_specs, check_vma=False)
```

```python
import functools
import math

import jax
import jax.numpy as jnp
from jax import lax
from jax.experimental import pallas as pl
from jax.experimental.pallas import tpu as pltpu
from jax.sharding import PartitionSpec as P

CHANNELS = 1024
FREQ_BANDS = 16
EARLY = 384
NORM_EPS = 1e-06
DECAY_SLOW = math.log(0.01) / 1.5
DECAY_FAST = math.log(0.01) / 0.3

F32 = jnp.float32
BF16 = jnp.bfloat16

LONG_COEFFS = (
    6.283185160089469,
    -41.34165503141532,
    81.60100407320796,
    -76.54978229245017,
    39.5367060575916,
)
SHORT_COEFFS = (6.283164044302229, -41.33714237106961, 81.3407688866883, -70.99343326314641)


def cos_turns(turns, coeffs=LONG_COEFFS):
    r = 0.25 - jnp.abs(turns - jnp.round(turns))
    s = r * r
    acc = s * coeffs[-1] + coeffs[-2]
    for coeff in coeffs[-3::-1]:
        acc = acc * s + coeff
    return acc * r


def sin_turns(turns):
    return cos_turns(turns - 0.25)


def split(value):
    high = value.astype(BF16)
    low = (value - high.astype(F32)).astype(BF16)
    return high, low


def iota(shape, dim):
    return lax.broadcasted_iota(jnp.int32, shape, dim)


def to_turns(index, period):
    return (index & (period - 1)).astype(F32) * (1.0 / period)


def row_dft_table():
    shape = (128, 192)
    k1, n1 = iota(shape, 0) & 63, iota(shape, 1) & 63
    turns = to_turns((2 * k1 + 1) * n1, 256)
    value = cos_turns(turns + jnp.where(iota(shape, 0) < 64, 0.0, 0.25))
    high = value.astype(BF16).astype(F32)
    return jnp.where(iota(shape, 1) < 128, high, value - high).astype(BF16)


def row_inverse_table(scale):
    shape = (64, 384)
    n1, k1 = iota(shape, 0), iota(shape, 1) & 63
    turns = to_turns((2 * k1 + 1) * n1, 256)
    value = cos_turns(turns + jnp.where((iota(shape, 1) & 64) == 0, 0.0, 0.25)) * scale
    high = value.astype(BF16).astype(F32)
    return jnp.where(iota(shape, 1) < 256, high, value - high).astype(BF16)


def twiddles():
    shape = (64, 128)
    turns = to_turns((2 * iota(shape, 0) + 1) * iota(shape, 1), 32768)
    return cos_turns(turns), sin_turns(turns)


def lane_dft():
    shape = (128, 128)
    turns = to_turns(iota(shape, 0) * iota(shape, 1), 128)
    return split(cos_turns(turns)), split(sin_turns(turns))


def dot(left, right):
    return jnp.dot(left, right, preferred_element_type=F32)


def stack3(value):
    high, low = split(value)
    return jnp.concatenate([high, low, high], axis=0)


def lanes3(value):
    high, low = split(value)
    return jnp.concatenate([high, low, high], axis=1)


def project_kernel(*refs):
    count = len(refs) - 15
    tokens, gain, w0, w1, w2 = refs[0:5]
    small = refs[5 : 5 + count // 2]
    out = refs[5 + count // 2]
    carried = refs[6 + count // 2 : 6 + count]
    near_tokens, near_gain, n0, n1, n2, normed, scratch, arrived, carry = refs[6 + count :]
    rows = 64
    copies = [pltpu.make_async_copy(gain, near_gain, arrived.at[0])]
    for part in range(4):
        where = pl.ds(part * rows, rows)
        copies.append(pltpu.make_async_copy(tokens.at[where], near_tokens.at[where], arrived.at[part + 1]))
    for index, (source, target) in enumerate(((w0, n0), (w1, n1), (w2, n2))):
        copies.append(pltpu.make_async_copy(source, target, arrived.at[index + 5]))
    carries = [
        pltpu.make_async_copy(source, target, carry.at[index])
        for index, (source, target) in enumerate(zip(small, carried))
    ]
    for copy in copies + carries:
        copy.start()
    copies[0].wait()
    for part in range(4):
        copies[part + 1].wait()
        wide = near_tokens[part * rows : part * rows + rows, :].astype(F32)
        scale = lax.rsqrt(jnp.mean(wide * wide, axis=1, keepdims=True) + NORM_EPS)
        normed[part * rows : part * rows + rows, :] = (wide * scale * near_gain[...]).astype(BF16)
    for copy in copies[5:]:
        copy.wait()
    weights = jnp.concatenate([n0[...], n1[...], n2[...]], axis=1)
    for half in range(2):
        gates = dot(normed[half * 128 : half * 128 + 128, :], weights)
        for branch in range(3):
            block = gates[:, branch * 128 : branch * 128 + 128].T
            for peer in range(32):
                start = peer * 24 + half * 12 + branch * 4
                scratch[start : start + 4, :] = block[peer * 4 : peer * 4 + 4, :]
    out[...] = scratch[...].astype(BF16).reshape(32, 24, 128)
    for copy in carries:
        copy.wait()


def lane_table(sign, cos, sin):
    def part(c, s):
        top = jnp.concatenate([c, -s if sign > 0 else s], axis=1)
        bottom = jnp.concatenate([s if sign > 0 else -s, c], axis=1)
        return jnp.concatenate([top, bottom], axis=0)

    high, low = part(cos[0], sin[0]), part(cos[1], sin[1])
    return jnp.concatenate([high, high, low], axis=0)


def filter_kernel(
    ew, eb, iw, ib, freq, fw, sw, sb, skip, weight,
    hre, him, frows, irows, flanes, ilanes, twiddle, scalars, kept,
    build, lhs1, lhs2, taps, arrived,
):
    length = 8192
    fetch = pltpu.make_async_copy(weight.at[0:EARLY], kept, arrived)
    fetch.start()
    own = lax.axis_index("row") * 4
    first_channel = lax.axis_index("col") * 128 + own

    lines = []
    for branch in range(3):
        lines.append(sb[branch : branch + 1, :])
        lines.append(sw[branch].astype(F32))
    lines.append(jnp.zeros((4, 128), F32))
    lines = pltpu.roll(jnp.concatenate(lines, axis=0), (128 - own) % 128, 1)
    for channel in range(4):
        scalars[channel * 16 : channel * 16 + 16, :] = jnp.broadcast_to(
            lines[:, channel : channel + 1], (16, 128)
        )
        scalars[channel * 16 + 12 : channel * 16 + 14, :] = jnp.broadcast_to(
            skip[:, channel : channel + 1], (2, 128)
        )

    frows[...] = row_dft_table()
    irows[...] = row_inverse_table(1.0 / 8192)
    tw_cos, tw_sin = twiddles()
    twiddle[0:64, :] = tw_cos
    twiddle[64:128, :] = tw_sin
    cos, sin = lane_dft()
    flanes[...] = lane_table(1, cos, sin)
    ilanes[...] = lane_table(-1, cos, sin)

    def high_of(value):
        return value.astype(BF16).astype(F32)

    turns_of = freq[...] * (1.0 / (2.0 * math.pi))
    build[...] = jnp.zeros_like(build)
    embed = ew[...] * turns_of
    bias = eb[...] * turns_of - 0.25
    rows = jnp.concatenate([embed[1:33], embed[0:1], bias], axis=0)
    build[0:34, 0:64] = high_of(rows)
    build[48:82, 0:64] = high_of(rows)
    build[96:130, 0:64] = rows - high_of(rows)
    lhs1[...] = build[...].T[0:64, :].astype(BF16)
    inner = iw[...] * turns_of
    bias = ib[...] * turns_of - 0.25
    build[...] = jnp.zeros_like(build)
    build[0:64, 0:64] = high_of(inner)
    build[64:128, 0:64] = high_of(inner)
    build[128:192, 0:64] = inner - high_of(inner)
    build[192:193, 0:64] = high_of(bias)
    build[193:194, 0:64] = bias - high_of(bias)
    lhs2[...] = build[...].T[0:64, :].astype(BF16)
    left1 = lhs1[:, 0:144]
    left2 = lhs2[:, 0:208]
    parts = []
    for order in range(2):
        parts.append(fw[order, 0] + fw[order, 1])
        parts.append(fw[order, 0] - fw[order, 1])
    fhigh, flow = split(jnp.concatenate(parts, axis=0))
    left3 = jnp.concatenate([fhigh, flow], axis=1)

    band_step = (FREQ_BANDS - 1 - 0.0001) / (FREQ_BANDS - 1)
    band = 0.0001 + iota((16, 128), 0).astype(F32) * band_step
    lane = iota((16, 128), 1).astype(F32)
    coarse = band * (lane * (128.0 / length))
    fine = band * (lane * (1.0 / length))
    coarse_cos, coarse_sin = cos_turns(coarse), sin_turns(coarse)
    fine_cos, fine_sin = cos_turns(fine), sin_turns(fine)
    row = iota((16, 128), 0)
    extra = jnp.where(row == 0, lane * (1.0 / (length - 1)), jnp.where(row == 1, 1.0, 0.0))
    extra_step = jnp.where(row == 0, 128.0 / (length - 1), 0.0)

    rate_step = (DECAY_SLOW - DECAY_FAST) / (CHANNELS - 1)
    channel_row = (iota((8, 128), 0) & 3) + first_channel
    rate = -DECAY_SLOW + channel_row.astype(F32) * rate_step
    ramp = iota((8, 128), 1).astype(F32) * (1.0 / (length - 1))

    chunk = 4096
    blocks = chunk // 128
    ones16 = jnp.ones((16, chunk), BF16)
    for step in range(length // chunk):
        feature = []
        for block in range(blocks):
            n1 = step * blocks + block
            ca = jnp.broadcast_to(coarse_cos[:, n1 : n1 + 1], (16, 128))
            sa = jnp.broadcast_to(coarse_sin[:, n1 : n1 + 1], (16, 128))
            feature.append(
                jnp.concatenate(
                    [
                        ca * fine_cos - sa * fine_sin,
                        -(sa * fine_cos + ca * fine_sin),
                        extra + extra_step * float(n1),
                    ],
                    axis=0,
                )
            )
        hidden = cos_turns(dot(left1, stack3(jnp.concatenate(feature, axis=1))), SHORT_COEFFS)
        hidden = cos_turns(dot(left2, jnp.concatenate([stack3(hidden), ones16], axis=0)), SHORT_COEFFS)
        high = hidden.astype(BF16)
        value = dot(left3, jnp.concatenate([high, high], axis=0))
        for block in range(blocks):
            n1 = step * blocks + block
            window = jnp.exp((ramp + n1 * 128.0 / (length - 1)) * -rate)
            piece = value[:, block * 128 : block * 128 + 128] * jnp.concatenate([window, window], axis=0)
            if n1 == 0:
                swapped = jnp.concatenate([piece[4:8], piece[0:4], piece[12:16], piece[8:12]], axis=0)
                piece = jnp.where(iota((16, 128), 1) == 0, 0.5 * (piece + swapped), piece)
            taps[n1 * 16 : n1 * 16 + 16, :] = piece

    spread = jnp.concatenate([taps[pl.ds(r, 64, stride=16), :] for r in range(16)], axis=1)
    stage = dot(frows[...], stack3(spread))
    (cos_high, cos_low), (sin_high, sin_low) = cos, sin
    real_table = jnp.concatenate([cos_high, sin_high, cos_low, sin_low], axis=0)
    imag_table = jnp.concatenate([-sin_high, cos_high, -sin_low, cos_low], axis=0)
    for kind, table, out in ((0, real_table, hre), (1, imag_table, him)):
        reals, imags = [], []
        for order in range(2):
            for channel in range(4):
                at = (order * 8 + kind * 4 + channel) * 128
                real, imag = stage[0:64, at : at + 128], stage[64:128, at : at + 128]
                reals.append(real * tw_cos + imag * tw_sin)
                imags.append(imag * tw_cos - real * tw_sin)
        left = jnp.concatenate([jnp.concatenate(reals, axis=0), jnp.concatenate(imags, axis=0)], axis=1)
        left = left.astype(BF16)
        out[...] = dot(jnp.concatenate([left, left], axis=1), table)
    fetch.wait()


def shifted(value, amount):
    size = 128
    lane, row = iota(value.shape, 1), iota(value.shape, 0)
    rolled = pltpu.roll(value, amount % size, 1)
    carried = pltpu.roll(rolled, amount % 64, 0)
    edge_lane = 0 if amount == 1 else size - 1
    edge_row = 0 if amount == 1 else 63
    carried = jnp.where(row == edge_row, 0.0, carried)
    return jnp.where(lane == edge_lane, carried, rolled)


def conv_kernel(
    moved, hre, him, frows, irows, flanes, ilanes, twiddle, scalars, weight, out, kept, wide, result, arrived
):
    fetch = pltpu.make_async_copy(weight.at[EARLY:1024], kept, arrived)
    fetch.start()
    wide[...] = moved[...].astype(F32).reshape(768, 128)
    smoothed = []
    for branch in range(3):
        rows = []
        for channel in range(4):
            value = wide[pl.ds(branch * 4 + channel, 64, stride=12), :]
            base = channel * 16 + branch * 4
            total = scalars[base : base + 1, :] + shifted(value, 1) * scalars[base + 1 : base + 2, :]
            total = total + value * scalars[base + 2 : base + 3, :]
            total = total + shifted(value, -1) * scalars[base + 3 : base + 4, :]
            rows.append(total)
        smoothed.append(rows)
    forward_rows, inverse_rows = frows[...], irows[...]
    forward_lanes, inverse_lanes = flanes[...], ilanes[...]
    tw_cos, tw_sin = twiddle[0:64, :], twiddle[64:128, :]
    signal = smoothed[2]
    for order in range(2):
        following = []
        for pair in ((0, 1, 2, 3),):
            stage = dot(forward_rows, stack3(jnp.concatenate([signal[c] for c in pair], axis=1)))
            reals, imags = [], []
            for place in range(4):
                real = stage[0:64, place * 128 : place * 128 + 128]
                imag = stage[64:128, place * 128 : place * 128 + 128]
                reals.append(real * tw_cos + imag * tw_sin)
                imags.append(imag * tw_cos - real * tw_sin)
            left = jnp.concatenate([jnp.concatenate(reals, axis=0), jnp.concatenate(imags, axis=0)], axis=1)
            spectrum = dot(lanes3(left), forward_lanes)
            real, imag = spectrum[:, 0:128], spectrum[:, 128:256]
            at = order * 256 + pair[0] * 64
            tap_real, tap_imag = hre[at : at + 256, :], him[at : at + 256, :]
            left = jnp.concatenate(
                [real * tap_real - imag * tap_imag, real * tap_imag + imag * tap_real], axis=1
            )
            back = dot(lanes3(left), inverse_lanes)
            columns = []
            for place in range(4):
                real = back[place * 64 : place * 64 + 64, 0:128]
                imag = back[place * 64 : place * 64 + 64, 128:256]
                columns.append(
                    jnp.concatenate([real * tw_cos - imag * tw_sin, real * tw_sin + imag * tw_cos], axis=0)
                )
            values = dot(inverse_rows, stack3(jnp.concatenate(columns, axis=1)))
            for place, channel in enumerate(pair):
                at = channel * 16 + 12 + order
                conv = values[:, place * 128 : place * 128 + 128] + signal[channel] * scalars[at : at + 1, :]
                following.append(smoothed[order][channel] * conv)
        signal = following
    for channel in range(4):
        result[pl.ds(channel, 64, stride=4), :] = signal[channel]
    out[...] = result[...].astype(BF16).reshape(32, 8, 128)
    fetch.wait()


def norm_kernel(moved, gain, out, wide, ordered):
    wide[...] = moved[...].astype(F32).reshape(256, 128)
    for half in range(2):
        for channel in range(4):
            ordered[pl.ds(half * 128 + channel, 32, stride=4), :] = wide[
                pl.ds(half * 4 + channel, 32, stride=8), :
            ]
    for half in range(2):
        value = ordered[half * 128 : half * 128 + 128, :]
        scale = lax.rsqrt(jnp.mean(value * value, axis=0, keepdims=True) + NORM_EPS)
        normed = ((value * scale).T * gain[...]).astype(BF16)
        out[half * 4 : half * 4 + 4] = normed.reshape(4, 32, 128)


def output_kernel(mixed, early, late, out):
    left = jnp.concatenate([mixed[c] for c in range(8)], axis=1)
    out[...] = (dot(left[:, 0:EARLY], early[...]) + dot(left[:, EARLY:1024], late[...])).astype(BF16)


VMEM = pl.BlockSpec(memory_space=pltpu.VMEM)
HBM = pl.BlockSpec(memory_space=pltpu.HBM)


def run(kernel, out_shape, inputs, scratch, name, unread=0):
    multi = isinstance(out_shape, (tuple, list))
    return pl.pallas_call(
        kernel,
        out_shape=out_shape,
        in_specs=[VMEM] * (len(inputs) - unread) + [HBM] * unread,
        out_specs=tuple(VMEM for _ in out_shape) if multi else VMEM,
        scratch_shapes=scratch,
        name=name,
        compiler_params=pltpu.CompilerParams(vmem_limit_bytes=24 * 1024 * 1024),
    )(*inputs)


def near(value):
    return pltpu.with_memory_space_constraint(value, pltpu.VMEM)


def far(*values):
    return tuple(pltpu.with_memory_space_constraint(value, pltpu.HBM) for value in values)


def local(
    tokens,
    norm_gain,
    first_gate,
    second_gate,
    value_weight,
    short_weight,
    short_bias,
    embed_weight,
    embed_bias,
    inner_weight,
    inner_bias,
    filter_freq,
    filter_weight,
    filter_skip,
    output_gain,
    output_weight,
):
    small = (
        embed_weight,
        embed_bias.reshape(1, -1),
        inner_weight,
        inner_bias.reshape(1, -1),
        filter_freq.reshape(1, -1),
        filter_weight.transpose(0, 1, 3, 2),
        short_weight,
        short_bias,
        filter_skip,
        output_gain.reshape(1, -1),
    )
    sent, *small = run(
        project_kernel,
        (pltpu.VMEM((32, 24, 128), BF16), *(pltpu.VMEM(value.shape, value.dtype) for value in small)),
        far(tokens, norm_gain.reshape(1, -1), first_gate, second_gate, value_weight, *small),
        [
            pltpu.VMEM((256, 2048), BF16),
            pltpu.VMEM((1, 2048), F32),
            pltpu.VMEM((2048, 128), BF16),
            pltpu.VMEM((2048, 128), BF16),
            pltpu.VMEM((2048, 128), BF16),
            pltpu.VMEM((256, 2048), BF16),
            pltpu.VMEM((768, 128), F32),
            pltpu.SemaphoreType.DMA((8,)),
            pltpu.SemaphoreType.DMA((len(small),)),
        ],
        "project",
        5 + len(small),
    )
    moved = lax.all_to_all(sent, "row", split_axis=0, concat_axis=0, tiled=True)
    *prepared, kept_early = run(
        filter_kernel,
        (
            pltpu.VMEM((512, 128), F32),
            pltpu.VMEM((512, 128), F32),
            pltpu.VMEM((128, 192), BF16),
            pltpu.VMEM((64, 384), BF16),
            pltpu.VMEM((768, 256), BF16),
            pltpu.VMEM((768, 256), BF16),
            pltpu.VMEM((128, 128), F32),
            pltpu.VMEM((64, 128), F32),
            pltpu.VMEM((EARLY, 2048), BF16),
        ),
        (*(near(value) for value in small[:9]), *far(output_weight)),
        [
            pltpu.VMEM((256, 128), F32),
            pltpu.VMEM((64, 256), BF16),
            pltpu.VMEM((64, 256), BF16),
            pltpu.VMEM((1024, 128), F32),
            pltpu.SemaphoreType.DMA,
        ],
        "filters",
        1,
    )
    mixed, kept = run(
        conv_kernel,
        (pltpu.VMEM((32, 8, 128), BF16), pltpu.VMEM((1024 - EARLY, 2048), BF16)),
        (*(near(value) for value in (moved, *prepared)), *far(output_weight)),
        [pltpu.VMEM((768, 128), F32), pltpu.VMEM((256, 128), F32), pltpu.SemaphoreType.DMA],
        "convolve",
        1,
    )
    result = lax.all_to_all(mixed, "row", split_axis=0, concat_axis=0, tiled=True)
    normed = run(
        norm_kernel,
        pltpu.VMEM((8, 32, 128), BF16),
        (near(result), near(small[9])),
        [pltpu.VMEM((256, 128), F32), pltpu.VMEM((256, 128), F32)],
        "groupnorm",
    )
    gathered = lax.all_to_all(normed, "col", split_axis=0, concat_axis=0, tiled=True)
    return run(
        output_kernel,
        jax.ShapeDtypeStruct((32, 2048), BF16),
        (near(gathered), near(kept_early), near(kept)),
        [],
        "output",
    )


def solution(mesh):
    in_specs = (
        P("row", None),
        P(),
        P(None, "col"),
        P(None, "col"),
        P(None, "col"),
        P(None, None, "col"),
        P(None, "col"),
        P(),
        P(),
        P(),
        P(),
        P(),
        P(None, None, None, ("col", "row")),
        P(None, ("col", "row")),
        P("col"),
        P(),
    )
    out_specs = P(("row", "col"), None)
    return jax.shard_map(local, mesh=mesh, in_specs=in_specs, out_specs=out_specs, check_vma=False)
```

```python
import functools
import math

import jax
import jax.numpy as jnp
from jax import lax
from jax.experimental import pallas as pl
from jax.experimental.pallas import tpu as pltpu
from jax.sharding import PartitionSpec as P

CHANNELS = 1024
FREQ_BANDS = 16
NORM_EPS = 1e-06
DECAY_SLOW = math.log(0.01) / 1.5
DECAY_FAST = math.log(0.01) / 0.3

F32 = jnp.float32
BF16 = jnp.bfloat16

LONG_COEFFS = (
    6.283185160089469,
    -41.34165503141532,
    81.60100407320796,
    -76.54978229245017,
    39.5367060575916,
)
SHORT_COEFFS = (6.283164044302229, -41.33714237106961, 81.3407688866883, -70.99343326314641)


def cos_turns(turns, coeffs=LONG_COEFFS):
    r = 0.25 - jnp.abs(turns - jnp.round(turns))
    s = r * r
    acc = s * coeffs[-1] + coeffs[-2]
    for coeff in coeffs[-3::-1]:
        acc = acc * s + coeff
    return acc * r


def sin_turns(turns):
    return cos_turns(turns - 0.25)


def split(value):
    high = value.astype(BF16)
    low = (value - high.astype(F32)).astype(BF16)
    return high, low


def iota(shape, dim):
    return lax.broadcasted_iota(jnp.int32, shape, dim)


def to_turns(index, period):
    return (index & (period - 1)).astype(F32) * (1.0 / period)


def row_dft_table():
    shape = (128, 192)
    k1, n1 = iota(shape, 0) & 63, iota(shape, 1) & 63
    turns = to_turns((2 * k1 + 1) * n1, 256)
    value = cos_turns(turns + jnp.where(iota(shape, 0) < 64, 0.0, 0.25))
    high = value.astype(BF16).astype(F32)
    return jnp.where(iota(shape, 1) < 128, high, value - high).astype(BF16)


def row_inverse_table(scale):
    shape = (64, 384)
    n1, k1 = iota(shape, 0), iota(shape, 1) & 63
    turns = to_turns((2 * k1 + 1) * n1, 256)
    value = cos_turns(turns + jnp.where((iota(shape, 1) & 64) == 0, 0.0, 0.25)) * scale
    high = value.astype(BF16).astype(F32)
    return jnp.where(iota(shape, 1) < 256, high, value - high).astype(BF16)


def twiddles():
    shape = (64, 128)
    turns = to_turns((2 * iota(shape, 0) + 1) * iota(shape, 1), 32768)
    return cos_turns(turns), sin_turns(turns)


def lane_dft():
    shape = (128, 128)
    turns = to_turns(iota(shape, 0) * iota(shape, 1), 128)
    return split(cos_turns(turns)), split(sin_turns(turns))


def dot(left, right):
    return jnp.dot(left, right, preferred_element_type=F32)


def stack3(value):
    high, low = split(value)
    return jnp.concatenate([high, low, high], axis=0)


def lanes3(value):
    high, low = split(value)
    return jnp.concatenate([high, low, high], axis=1)


def project_kernel(*refs):
    extra = (len(refs) - 15) // 2
    tokens, gain, w0, w1, w2 = refs[0:5]
    small = refs[5 : 5 + extra]
    out, normed, n1 = refs[5 + extra : 8 + extra]
    carried = refs[8 + extra : 8 + 2 * extra]
    near_tokens, near_gain, n0, n2, scratch, arrived, carry = refs[8 + 2 * extra :]
    rows = 64
    copies = [pltpu.make_async_copy(gain, near_gain, arrived.at[0])]
    for part in range(4):
        where = pl.ds(part * rows, rows)
        copies.append(pltpu.make_async_copy(tokens.at[where], near_tokens.at[where], arrived.at[part + 1]))
    for index, (source, target) in enumerate(((w0, n0), (w2, n2), (w1, n1))):
        copies.append(pltpu.make_async_copy(source, target, arrived.at[index + 5]))
    carries = [
        pltpu.make_async_copy(source, target, carry.at[index])
        for index, (source, target) in enumerate(zip(small, carried))
    ]
    for copy in copies + carries:
        copy.start()
    copies[0].wait()
    for part in range(4):
        copies[part + 1].wait()
        wide = near_tokens[part * rows : part * rows + rows, :].astype(F32)
        scale = lax.rsqrt(jnp.mean(wide * wide, axis=1, keepdims=True) + NORM_EPS)
        normed[part * rows : part * rows + rows, :] = (wide * scale * near_gain[...]).astype(BF16)
    copies[5].wait()
    copies[6].wait()
    weights = jnp.concatenate([n0[...], n2[...]], axis=1)
    for half in range(2):
        gates = dot(normed[half * 128 : half * 128 + 128, :], weights)
        for branch in range(2):
            block = gates[:, branch * 128 : branch * 128 + 128].T
            for peer in range(32):
                start = peer * 18 + half * 9 + branch * 4
                scratch[start : start + 4, :] = block[peer * 4 : peer * 4 + 4, :]
    copies[7].wait()
    edges = dot(jnp.concatenate([normed[0:16, :], normed[240:256, :]], axis=0), n1[...])
    for peer in range(32):
        scratch[peer * 18 + 8 : peer * 18 + 9, :] = edges[0:1, :]
        scratch[peer * 18 + 17 : peer * 18 + 18, :] = edges[31:32, :]
    out[...] = scratch[...].astype(BF16)
    for copy in carries:
        copy.wait()


def lane_table(sign, cos, sin):
    def part(c, s):
        top = jnp.concatenate([c, -s if sign > 0 else s], axis=1)
        bottom = jnp.concatenate([s if sign > 0 else -s, c], axis=1)
        return jnp.concatenate([top, bottom], axis=0)

    high, low = part(cos[0], sin[0]), part(cos[1], sin[1])
    return jnp.concatenate([high, low], axis=0)


def filter_kernel(
    normed, w1, ew, eb, iw, ib, freq, fw, sw, sb, skip,
    hre, him, frows, irows, flanes, ilanes, twiddle, scalars, gate,
    build, lhs1, lhs2, taps, turned,
):
    length = 8192
    own = lax.axis_index("row") * 4
    first_channel = lax.axis_index("col") * 128 + own

    source = dot(normed[...], w1[...]).astype(BF16).astype(F32)
    zero = jnp.zeros((1, 128), F32)
    before = jnp.concatenate([zero, source[0:255]], axis=0)
    after = jnp.concatenate([source[1:256], zero], axis=0)
    second = sw[1].astype(F32)
    total = sb[1:2, :] + before * second[0:1]
    total = total + source * second[1:2]
    gate[...] = total + after * second[2:3]

    lines = []
    for branch in range(3):
        lines.append(sb[branch : branch + 1, :])
        lines.append(sw[branch].astype(F32))
    lines.append(jnp.zeros((4, 128), F32))
    lines = pltpu.roll(jnp.concatenate(lines, axis=0), (128 - own) % 128, 1)
    for channel in range(4):
        scalars[channel * 16 : channel * 16 + 16, :] = jnp.broadcast_to(
            lines[:, channel : channel + 1], (16, 128)
        )
        scalars[channel * 16 + 12 : channel * 16 + 14, :] = jnp.broadcast_to(
            skip[:, channel : channel + 1], (2, 128)
        )

    frows[...] = row_dft_table()
    irows[...] = row_inverse_table(1.0 / 8192)
    tw_cos, tw_sin = twiddles()
    twiddle[0:64, :] = tw_cos
    twiddle[64:128, :] = tw_sin
    cos, sin = lane_dft()
    flanes[...] = lane_table(1, cos, sin)
    ilanes[...] = lane_table(-1, cos, sin)

    def high_of(value):
        return value.astype(BF16).astype(F32)

    turns_of = freq[...] * (1.0 / (2.0 * math.pi))
    build[...] = jnp.zeros_like(build)
    embed = ew[...] * turns_of
    bias = eb[...] * turns_of - 0.25
    rows = jnp.concatenate([embed[1:33], embed[0:1], bias], axis=0)
    build[0:34, 0:64] = high_of(rows)
    build[48:82, 0:64] = high_of(rows)
    build[96:130, 0:64] = rows - high_of(rows)
    lhs1[...] = build[...].T[0:64, :].astype(BF16)
    inner = iw[...] * turns_of
    bias = ib[...] * turns_of - 0.25
    build[...] = jnp.zeros_like(build)
    build[0:64, 0:64] = high_of(inner)
    build[64:128, 0:64] = high_of(inner)
    build[128:192, 0:64] = inner - high_of(inner)
    build[192:193, 0:64] = high_of(bias)
    build[193:194, 0:64] = bias - high_of(bias)
    lhs2[...] = build[...].T[0:64, :].astype(BF16)
    left1 = lhs1[:, 0:144]
    left2 = lhs2[:, 0:208]
    parts = []
    for order in range(2):
        parts.append(fw[order, 0] + fw[order, 1])
        parts.append(fw[order, 0] - fw[order, 1])
    fhigh, flow = split(jnp.concatenate(parts, axis=0))
    left3 = jnp.concatenate([fhigh, flow], axis=1)

    band_step = (FREQ_BANDS - 1 - 0.0001) / (FREQ_BANDS - 1)
    band = 0.0001 + iota((16, 128), 0).astype(F32) * band_step
    lane = iota((16, 128), 1).astype(F32)
    coarse = band * (lane * (128.0 / length))
    fine = band * (lane * (1.0 / length))
    coarse_cos, coarse_sin = cos_turns(coarse), sin_turns(coarse)
    fine_cos, fine_sin = cos_turns(fine), sin_turns(fine)
    row = iota((16, 128), 0)
    extra = jnp.where(row == 0, lane * (1.0 / (length - 1)), jnp.where(row == 1, 1.0, 0.0))
    extra_step = jnp.where(row == 0, 128.0 / (length - 1), 0.0)

    rate_step = (DECAY_SLOW - DECAY_FAST) / (CHANNELS - 1)
    channel_row = (iota((8, 128), 0) & 3) + first_channel
    rate = -DECAY_SLOW + channel_row.astype(F32) * rate_step
    ramp = iota((8, 128), 1).astype(F32) * (1.0 / (length - 1))

    chunk = 4096
    blocks = chunk // 128
    ones16 = jnp.ones((16, chunk), BF16)
    turned[0:16, :] = coarse_cos
    turned[16:32, :] = coarse_sin

    def one_chunk(step, carry):
        first = step * blocks
        column = pltpu.roll(turned[...], (128 - first) % 128, 1)
        start = first.astype(F32)
        feature = []
        for block in range(blocks):
            ca = jnp.broadcast_to(column[0:16, block : block + 1], (16, 128))
            sa = jnp.broadcast_to(column[16:32, block : block + 1], (16, 128))
            feature.append(
                jnp.concatenate(
                    [
                        ca * fine_cos - sa * fine_sin,
                        -(sa * fine_cos + ca * fine_sin),
                        extra + extra_step * (start + float(block)),
                    ],
                    axis=0,
                )
            )
        hidden = cos_turns(dot(left1, stack3(jnp.concatenate(feature, axis=1))), SHORT_COEFFS)
        hidden = cos_turns(
            dot(left2, jnp.concatenate([stack3(hidden), ones16], axis=0)), SHORT_COEFFS
        )
        high = hidden.astype(BF16)
        value = dot(left3, jnp.concatenate([high, high], axis=0))
        for block in range(blocks):
            here = ramp + (start + float(block)) * (128.0 / (length - 1))
            window = jnp.exp(here * -rate)
            piece = value[:, block * 128 : block * 128 + 128] * jnp.concatenate([window, window], axis=0)
            at = pl.multiple_of((first + block) * 16, 16)
            taps[pl.ds(at, 16), :] = piece
        return carry

    lax.fori_loop(0, length // chunk, one_chunk, 0)
    piece = taps[0:16, :]
    swapped = jnp.concatenate([piece[4:8], piece[0:4], piece[12:16], piece[8:12]], axis=0)
    taps[0:16, :] = jnp.where(iota((16, 128), 1) == 0, 0.5 * (piece + swapped), piece)

    spread = jnp.concatenate([taps[pl.ds(r, 64, stride=16), :] for r in range(16)], axis=1)
    stage = dot(frows[...], stack3(spread))
    (cos_high, cos_low), (sin_high, sin_low) = cos, sin
    real_table = jnp.concatenate([cos_high, sin_high, cos_low, sin_low], axis=0)
    imag_table = jnp.concatenate([-sin_high, cos_high, -sin_low, cos_low], axis=0)
    for kind, table, out in ((0, real_table, hre), (1, imag_table, him)):
        reals, imags = [], []
        for order in range(2):
            for channel in range(4):
                at = (order * 8 + kind * 4 + channel) * 128
                real, imag = stage[0:64, at : at + 128], stage[64:128, at : at + 128]
                reals.append(real * tw_cos + imag * tw_sin)
                imags.append(imag * tw_cos - real * tw_sin)
        left = jnp.concatenate([jnp.concatenate(reals, axis=0), jnp.concatenate(imags, axis=0)], axis=1)
        left = left.astype(BF16)
        out[...] = dot(jnp.concatenate([left, left], axis=1), table)


def shifted(value, amount):
    size = 128
    lane, row = iota(value.shape, 1), iota(value.shape, 0)
    rolled = pltpu.roll(value, amount % size, 1)
    carried = pltpu.roll(rolled, amount % 64, 0)
    edge_lane = 0 if amount == 1 else size - 1
    edge_row = 0 if amount == 1 else 63
    carried = jnp.where(row == edge_row, 0.0, carried)
    return jnp.where(lane == edge_lane, carried, rolled)


def repeat_high(table):
    return jnp.concatenate([table[0:256, :], table[0:256, :], table[256:512, :]], axis=0)


def conv_kernel(
    moved, hre, him, frows, irows, flanes, ilanes, twiddle, scalars, sw, weight,
    out, edges, kept, wide, result, state, factors, arrived,
):
    fetch = pltpu.make_async_copy(weight, kept, arrived)
    fetch.start()
    wide[...] = moved[...].astype(F32)
    own = lax.axis_index("row")
    before = wide[pl.ds(jnp.maximum(own - 1, 0) * 18 + 17, 1), :]
    after = wide[pl.ds(jnp.minimum(own + 1, 31) * 18 + 8, 1), :]
    second = sw[1].astype(F32)
    edges[0:1, :] = jnp.where(own > 0, before, 0.0) * second[0:1]
    edges[1:2, :] = jnp.where(own < 31, after, 0.0) * second[2:3]
    smoothed = []
    for branch in range(2):
        rows = []
        for channel in range(4):
            value = wide[pl.ds(branch * 4 + channel, 64, stride=9), :]
            base = channel * 16 + branch * 8
            total = scalars[base : base + 1, :] + shifted(value, 1) * scalars[base + 1 : base + 2, :]
            total = total + value * scalars[base + 2 : base + 3, :]
            total = total + shifted(value, -1) * scalars[base + 3 : base + 4, :]
            rows.append(total)
        smoothed.append(rows)
    forward_rows, inverse_rows, forward_lanes, inverse_lanes = frows, irows, flanes, ilanes
    tw_cos, tw_sin = twiddle[0:64, :], twiddle[64:128, :]
    for channel in range(4):
        state[channel * 64 : channel * 64 + 64, :] = smoothed[1][channel]
        factors[channel * 64 : channel * 64 + 64, :] = smoothed[0][channel]
    factors[256:512, :] = jnp.ones((256, 128), F32)

    def one_order(order, carry):
        signal = [state[c * 64 : c * 64 + 64, :] for c in range(4)]
        stage = dot(forward_rows[...], stack3(jnp.concatenate(signal, axis=1)))
        reals, imags = [], []
        for place in range(4):
            real = stage[0:64, place * 128 : place * 128 + 128]
            imag = stage[64:128, place * 128 : place * 128 + 128]
            reals.append(real * tw_cos + imag * tw_sin)
            imags.append(imag * tw_cos - real * tw_sin)
        left = jnp.concatenate([jnp.concatenate(reals, axis=0), jnp.concatenate(imags, axis=0)], axis=1)
        spectrum = dot(lanes3(left), repeat_high(forward_lanes))
        real, imag = spectrum[:, 0:128], spectrum[:, 128:256]
        at = pl.multiple_of(order * 256, 256)
        tap_real, tap_imag = hre[pl.ds(at, 256), :], him[pl.ds(at, 256), :]
        left = jnp.concatenate([real * tap_real - imag * tap_imag, real * tap_imag + imag * tap_real], axis=1)
        back = dot(lanes3(left), repeat_high(inverse_lanes))
        columns = []
        for place in range(4):
            real = back[place * 64 : place * 64 + 64, 0:128]
            imag = back[place * 64 : place * 64 + 64, 128:256]
            columns.append(
                jnp.concatenate([real * tw_cos - imag * tw_sin, real * tw_sin + imag * tw_cos], axis=0)
            )
        values = dot(inverse_rows[...], stack3(jnp.concatenate(columns, axis=1)))
        for channel in range(4):
            skip = scalars[pl.ds(channel * 16 + 12 + order, 1), :]
            conv = values[:, channel * 128 : channel * 128 + 128] + signal[channel] * skip
            factor = factors[pl.ds(at + channel * 64, 64), :]
            state[channel * 64 : channel * 64 + 64, :] = conv * factor
        return carry

    lax.fori_loop(0, 2, one_order, 0)
    for channel in range(4):
        result[pl.ds(channel, 64, stride=4), :] = state[channel * 64 : channel * 64 + 64, :]
    out[...] = result[...].astype(BF16).reshape(32, 8, 128)
    fetch.wait()


def norm_kernel(moved, gate, edges, gain, out, wide, ordered):
    wide[...] = moved[...].astype(F32).reshape(256, 128)
    for half in range(2):
        for channel in range(4):
            ordered[pl.ds(half * 128 + channel, 32, stride=4), :] = wide[
                pl.ds(half * 4 + channel, 32, stride=8), :
            ]
    for half in range(2):
        edge_row = 0 if half == 0 else 127
        factor = gate[half * 128 : half * 128 + 128, :]
        factor = factor + jnp.where(iota((128, 128), 0) == edge_row, edges[half : half + 1, :], 0.0)
        value = ordered[half * 128 : half * 128 + 128, :].T * factor
        scale = lax.rsqrt(jnp.mean(value * value, axis=1, keepdims=True) + NORM_EPS)
        out[half * 4 : half * 4 + 4] = (value * scale * gain[...]).astype(BF16).reshape(4, 32, 128)


def output_kernel(mixed, weight, out):
    left = jnp.concatenate([mixed[c] for c in range(8)], axis=1)
    out[...] = dot(left, weight[...]).astype(BF16)


VMEM = pl.BlockSpec(memory_space=pltpu.VMEM)
HBM = pl.BlockSpec(memory_space=pltpu.HBM)


def run(kernel, out_shape, inputs, scratch, name, unread=0):
    multi = isinstance(out_shape, (tuple, list))
    return pl.pallas_call(
        kernel,
        out_shape=out_shape,
        in_specs=[VMEM] * (len(inputs) - unread) + [HBM] * unread,
        out_specs=tuple(VMEM for _ in out_shape) if multi else VMEM,
        scratch_shapes=scratch,
        name=name,
        compiler_params=pltpu.CompilerParams(vmem_limit_bytes=24 * 1024 * 1024),
    )(*inputs)


def near(value):
    return pltpu.with_memory_space_constraint(value, pltpu.VMEM)


def far(*values):
    return tuple(pltpu.with_memory_space_constraint(value, pltpu.HBM) for value in values)


def local(
    tokens,
    norm_gain,
    first_gate,
    second_gate,
    value_weight,
    short_weight,
    short_bias,
    embed_weight,
    embed_bias,
    inner_weight,
    inner_bias,
    filter_freq,
    filter_weight,
    filter_skip,
    output_gain,
    output_weight,
):
    small = (
        embed_weight,
        embed_bias.reshape(1, -1),
        inner_weight,
        inner_bias.reshape(1, -1),
        filter_freq.reshape(1, -1),
        filter_weight.transpose(0, 1, 3, 2),
        short_weight,
        short_bias,
        filter_skip,
        output_gain.reshape(1, -1),
    )
    sent, rows, second, *small = run(
        project_kernel,
        (
            pltpu.VMEM((576, 128), BF16),
            pltpu.VMEM((256, 2048), BF16),
            pltpu.VMEM((2048, 128), BF16),
            *(pltpu.VMEM(value.shape, value.dtype) for value in small),
        ),
        far(tokens, norm_gain.reshape(1, -1), first_gate, second_gate, value_weight, *small),
        [
            pltpu.VMEM((256, 2048), BF16),
            pltpu.VMEM((1, 2048), F32),
            pltpu.VMEM((2048, 128), BF16),
            pltpu.VMEM((2048, 128), BF16),
            pltpu.VMEM((576, 128), F32),
            pltpu.SemaphoreType.DMA((8,)),
            pltpu.SemaphoreType.DMA((len(small),)),
        ],
        "project",
        5 + len(small),
    )
    moved = lax.all_to_all(
        sent.reshape(32, 9, 2, 128), "row", split_axis=0, concat_axis=0, tiled=True
    ).reshape(576, 128)
    *prepared, gate = run(
        filter_kernel,
        (
            pltpu.VMEM((512, 128), F32),
            pltpu.VMEM((512, 128), F32),
            pltpu.VMEM((128, 192), BF16),
            pltpu.VMEM((64, 384), BF16),
            pltpu.VMEM((512, 256), BF16),
            pltpu.VMEM((512, 256), BF16),
            pltpu.VMEM((128, 128), F32),
            pltpu.VMEM((64, 128), F32),
            pltpu.VMEM((256, 128), F32),
        ),
        tuple(near(value) for value in (rows, second, *small[:9])),
        [
            pltpu.VMEM((256, 128), F32),
            pltpu.VMEM((64, 256), BF16),
            pltpu.VMEM((64, 256), BF16),
            pltpu.VMEM((1024, 128), F32),
            pltpu.VMEM((32, 128), F32),
        ],
        "filters",
    )
    mixed, edges, kept = run(
        conv_kernel,
        (pltpu.VMEM((32, 8, 128), BF16), pltpu.VMEM((2, 128), F32), pltpu.VMEM((1024, 2048), BF16)),
        (*(near(value) for value in (moved, *prepared, small[6])), *far(output_weight)),
        [
            pltpu.VMEM((576, 128), F32),
            pltpu.VMEM((256, 128), F32),
            pltpu.VMEM((256, 128), F32),
            pltpu.VMEM((512, 128), F32),
            pltpu.SemaphoreType.DMA,
        ],
        "convolve",
        1,
    )
    result = lax.all_to_all(mixed, "row", split_axis=0, concat_axis=0, tiled=True)
    normed = run(
        norm_kernel,
        pltpu.VMEM((8, 32, 128), BF16),
        tuple(near(value) for value in (result, gate, edges, small[9])),
        [pltpu.VMEM((256, 128), F32), pltpu.VMEM((256, 128), F32)],
        "groupnorm",
    )
    gathered = lax.all_to_all(normed, "col", split_axis=0, concat_axis=0, tiled=True)
    return run(
        output_kernel,
        jax.ShapeDtypeStruct((32, 2048), BF16),
        (near(gathered), near(kept)),
        [],
        "output",
    )


def solution(mesh):
    in_specs = (
        P("row", None),
        P(),
        P(None, "col"),
        P(None, "col"),
        P(None, "col"),
        P(None, None, "col"),
        P(None, "col"),
        P(),
        P(),
        P(),
        P(),
        P(),
        P(None, None, None, ("col", "row")),
        P(None, ("col", "row")),
        P("col"),
        P(),
    )
    out_specs = P(("row", "col"), None)
    return jax.shard_map(local, mesh=mesh, in_specs=in_specs, out_specs=out_specs, check_vma=False)
```

```python
import functools
import math

import jax
import jax.numpy as jnp
from jax import lax
from jax.experimental import pallas as pl
from jax.experimental.pallas import tpu as pltpu
from jax.sharding import PartitionSpec as P

CHANNELS = 1024
FREQ_BANDS = 16
EARLY = 192
NORM_EPS = 1e-06
DECAY_SLOW = math.log(0.01) / 1.5
DECAY_FAST = math.log(0.01) / 0.3

F32 = jnp.float32
BF16 = jnp.bfloat16

LONG_COEFFS = (
    6.283185160089469,
    -41.34165503141532,
    81.60100407320796,
    -76.54978229245017,
    39.5367060575916,
)
SHORT_COEFFS = (6.283164044302229, -41.33714237106961, 81.3407688866883, -70.99343326314641)


def cos_turns(turns, coeffs=LONG_COEFFS):
    r = 0.25 - jnp.abs(turns - jnp.round(turns))
    s = r * r
    acc = s * coeffs[-1] + coeffs[-2]
    for coeff in coeffs[-3::-1]:
        acc = acc * s + coeff
    return acc * r


def sin_turns(turns):
    return cos_turns(turns - 0.25)


def split(value):
    high = value.astype(BF16)
    low = (value - high.astype(F32)).astype(BF16)
    return high, low


def iota(shape, dim):
    return lax.broadcasted_iota(jnp.int32, shape, dim)


def to_turns(index, period):
    return (index & (period - 1)).astype(F32) * (1.0 / period)


def row_dft_table():
    shape = (128, 192)
    k1, n1 = iota(shape, 0) & 63, iota(shape, 1) & 63
    turns = to_turns((2 * k1 + 1) * n1, 256)
    value = cos_turns(turns + jnp.where(iota(shape, 0) < 64, 0.0, 0.25))
    high = value.astype(BF16).astype(F32)
    return jnp.where(iota(shape, 1) < 128, high, value - high).astype(BF16)


def row_inverse_table(scale):
    shape = (64, 384)
    n1, k1 = iota(shape, 0), iota(shape, 1) & 63
    turns = to_turns((2 * k1 + 1) * n1, 256)
    value = cos_turns(turns + jnp.where((iota(shape, 1) & 64) == 0, 0.0, 0.25)) * scale
    high = value.astype(BF16).astype(F32)
    return jnp.where(iota(shape, 1) < 256, high, value - high).astype(BF16)


def twiddles():
    shape = (64, 128)
    turns = to_turns((2 * iota(shape, 0) + 1) * iota(shape, 1), 32768)
    return cos_turns(turns), sin_turns(turns)


def lane_dft():
    shape = (128, 128)
    turns = to_turns(iota(shape, 0) * iota(shape, 1), 128)
    return split(cos_turns(turns)), split(sin_turns(turns))


def dot(left, right):
    return jnp.dot(left, right, preferred_element_type=F32)


def stack3(value):
    high, low = split(value)
    return jnp.concatenate([high, low, high], axis=0)


def lanes3(value):
    high, low = split(value)
    return jnp.concatenate([high, low, high], axis=1)


def project_kernel(*refs):
    extra = (len(refs) - 15) // 2
    tokens, gain, w0, w1, w2 = refs[0:5]
    small = refs[5 : 5 + extra]
    out, normed = refs[5 + extra : 7 + extra]
    carried = refs[7 + extra : 7 + 2 * extra]
    near_tokens, near_gain, n0, n1, n2, scratch, arrived, carry = refs[7 + 2 * extra :]
    rows = 128
    copies = [pltpu.make_async_copy(gain, near_gain, arrived.at[0])]
    for part in range(2):
        where = pl.ds(part * rows, rows)
        copies.append(pltpu.make_async_copy(tokens.at[where], near_tokens.at[where], arrived.at[part + 1]))
    for index, (source, target) in enumerate(((w0, n0), (w2, n2), (w1, n1))):
        copies.append(pltpu.make_async_copy(source, target, arrived.at[index + 3]))
    carries = [
        pltpu.make_async_copy(source, target, carry.at[index])
        for index, (source, target) in enumerate(zip(small, carried))
    ]
    for copy in copies:
        copy.start()
    copies[0].wait()
    for part in range(2):
        copies[part + 1].wait()
        wide = near_tokens[part * rows : part * rows + rows, :].astype(F32)
        scale = lax.rsqrt(jnp.mean(wide * wide, axis=1, keepdims=True) + NORM_EPS)
        normed[part * rows : part * rows + rows, :] = (wide * scale * near_gain[...]).astype(BF16)
    for copy in carries:
        copy.start()
    copies[3].wait()
    copies[4].wait()
    weights = jnp.concatenate([n0[...], n2[...]], axis=1)
    for half in range(2):
        gates = dot(normed[half * 128 : half * 128 + 128, :], weights)
        for branch in range(2):
            block = gates[:, branch * 128 : branch * 128 + 128].T
            for peer in range(32):
                start = peer * 18 + half * 9 + branch * 4
                scratch[start : start + 4, :] = block[peer * 4 : peer * 4 + 4, :]
    copies[5].wait()
    edges = dot(jnp.concatenate([normed[0:16, :], normed[240:256, :]], axis=0), n1[...])
    for peer in range(32):
        scratch[peer * 18 + 8 : peer * 18 + 9, :] = edges[0:1, :]
        scratch[peer * 18 + 17 : peer * 18 + 18, :] = edges[31:32, :]
    out[...] = scratch[...].astype(BF16)
    for copy in carries:
        copy.wait()


def lane_table(sign, cos, sin):
    def part(c, s):
        top = jnp.concatenate([c, -s if sign > 0 else s], axis=1)
        bottom = jnp.concatenate([s if sign > 0 else -s, c], axis=1)
        return jnp.concatenate([top, bottom], axis=0)

    high, low = part(cos[0], sin[0]), part(cos[1], sin[1])
    return jnp.concatenate([high, low], axis=0)


def filter_kernel(
    normed, ew, eb, iw, ib, freq, fw, sw, sb, skip, second_weight, weight,
    hre, him, frows, irows, flanes, ilanes, twiddle, scalars, gate, kept,
    build, lhs1, lhs2, taps, turned, w1, arrived,
):
    length = 8192
    fetch_second = pltpu.make_async_copy(second_weight, w1, arrived.at[1])
    fetch_second.start()
    fetch = pltpu.make_async_copy(weight.at[0:EARLY], kept, arrived.at[0])
    fetch.start()
    own = lax.axis_index("row") * 4
    first_channel = lax.axis_index("col") * 128 + own

    lines = []
    for branch in range(3):
        lines.append(sb[branch : branch + 1, :])
        lines.append(sw[branch].astype(F32))
    lines.append(jnp.zeros((4, 128), F32))
    lines = pltpu.roll(jnp.concatenate(lines, axis=0), (128 - own) % 128, 1)
    for channel in range(4):
        scalars[channel * 16 : channel * 16 + 16, :] = jnp.broadcast_to(
            lines[:, channel : channel + 1], (16, 128)
        )
        scalars[channel * 16 + 12 : channel * 16 + 14, :] = jnp.broadcast_to(
            skip[:, channel : channel + 1], (2, 128)
        )

    frows[...] = row_dft_table()
    irows[...] = row_inverse_table(1.0 / 8192)
    tw_cos, tw_sin = twiddles()
    twiddle[0:64, :] = tw_cos
    twiddle[64:128, :] = tw_sin
    cos, sin = lane_dft()
    flanes[...] = lane_table(1, cos, sin)
    ilanes[...] = lane_table(-1, cos, sin)

    def high_of(value):
        return value.astype(BF16).astype(F32)

    turns_of = freq[...] * (1.0 / (2.0 * math.pi))
    build[...] = jnp.zeros_like(build)
    embed = ew[...] * turns_of
    bias = eb[...] * turns_of - 0.25
    rows = jnp.concatenate([embed[1:33], embed[0:1], bias], axis=0)
    build[0:34, 0:64] = high_of(rows)
    build[48:82, 0:64] = high_of(rows)
    build[96:130, 0:64] = rows - high_of(rows)
    lhs1[...] = build[...].T[0:64, :].astype(BF16)
    inner = iw[...] * turns_of
    bias = ib[...] * turns_of - 0.25
    build[...] = jnp.zeros_like(build)
    build[0:64, 0:64] = high_of(inner)
    build[64:128, 0:64] = high_of(inner)
    build[128:192, 0:64] = inner - high_of(inner)
    build[192:193, 0:64] = high_of(bias)
    build[193:194, 0:64] = bias - high_of(bias)
    lhs2[...] = build[...].T[0:64, :].astype(BF16)
    left1 = lhs1[:, 0:144]
    left2 = lhs2[:, 0:208]
    parts = []
    for order in range(2):
        parts.append(fw[order, 0] + fw[order, 1])
        parts.append(fw[order, 0] - fw[order, 1])
    fhigh, flow = split(jnp.concatenate(parts, axis=0))
    left3 = jnp.concatenate([fhigh, flow], axis=1)

    band_step = (FREQ_BANDS - 1 - 0.0001) / (FREQ_BANDS - 1)
    band = 0.0001 + iota((16, 128), 0).astype(F32) * band_step
    lane = iota((16, 128), 1).astype(F32)
    coarse = band * (lane * (128.0 / length))
    fine = band * (lane * (1.0 / length))
    coarse_cos, coarse_sin = cos_turns(coarse), sin_turns(coarse)
    fine_cos, fine_sin = cos_turns(fine), sin_turns(fine)
    row = iota((16, 128), 0)
    extra = jnp.where(row == 0, lane * (1.0 / (length - 1)), jnp.where(row == 1, 1.0, 0.0))
    extra_step = jnp.where(row == 0, 128.0 / (length - 1), 0.0)

    rate_step = (DECAY_SLOW - DECAY_FAST) / (CHANNELS - 1)
    channel_row = (iota((8, 128), 0) & 3) + first_channel
    rate = -DECAY_SLOW + channel_row.astype(F32) * rate_step
    ramp = iota((8, 128), 1).astype(F32) * (1.0 / (length - 1))

    chunk = 4096
    blocks = chunk // 128
    ones16 = jnp.ones((16, chunk), BF16)
    turned[0:16, :] = coarse_cos
    turned[16:32, :] = coarse_sin

    def one_chunk(step, carry):
        first = step * blocks
        column = pltpu.roll(turned[...], (128 - first) % 128, 1)
        start = first.astype(F32)
        feature = []
        for block in range(blocks):
            ca = jnp.broadcast_to(column[0:16, block : block + 1], (16, 128))
            sa = jnp.broadcast_to(column[16:32, block : block + 1], (16, 128))
            feature.append(
                jnp.concatenate(
                    [
                        ca * fine_cos - sa * fine_sin,
                        -(sa * fine_cos + ca * fine_sin),
                        extra + extra_step * (start + float(block)),
                    ],
                    axis=0,
                )
            )
        hidden = cos_turns(dot(left1, stack3(jnp.concatenate(feature, axis=1))), SHORT_COEFFS)
        hidden = cos_turns(
            dot(left2, jnp.concatenate([stack3(hidden), ones16], axis=0)), SHORT_COEFFS
        )
        high = hidden.astype(BF16)
        value = dot(left3, jnp.concatenate([high, high], axis=0))
        for block in range(blocks):
            here = ramp + (start + float(block)) * (128.0 / (length - 1))
            window = jnp.exp(here * -rate)
            piece = value[:, block * 128 : block * 128 + 128] * jnp.concatenate([window, window], axis=0)
            at = pl.multiple_of((first + block) * 16, 16)
            taps[pl.ds(at, 16), :] = piece
        return carry

    lax.fori_loop(0, length // chunk, one_chunk, 0)
    piece = taps[0:16, :]
    swapped = jnp.concatenate([piece[4:8], piece[0:4], piece[12:16], piece[8:12]], axis=0)
    taps[0:16, :] = jnp.where(iota((16, 128), 1) == 0, 0.5 * (piece + swapped), piece)

    fetch_second.wait()
    source = dot(normed[...], w1[...]).astype(BF16).astype(F32)
    zero = jnp.zeros((1, 128), F32)
    before = jnp.concatenate([zero, source[0:255]], axis=0)
    after = jnp.concatenate([source[1:256], zero], axis=0)
    second = sw[1].astype(F32)
    total = sb[1:2, :] + before * second[0:1]
    total = total + source * second[1:2]
    gate[...] = total + after * second[2:3]

    spread = jnp.concatenate([taps[pl.ds(r, 64, stride=16), :] for r in range(16)], axis=1)
    stage = dot(frows[...], stack3(spread))
    (cos_high, cos_low), (sin_high, sin_low) = cos, sin
    real_table = jnp.concatenate([cos_high, sin_high, cos_low, sin_low], axis=0)
    imag_table = jnp.concatenate([-sin_high, cos_high, -sin_low, cos_low], axis=0)
    for kind, table, out in ((0, real_table, hre), (1, imag_table, him)):
        reals, imags = [], []
        for order in range(2):
            for channel in range(4):
                at = (order * 8 + kind * 4 + channel) * 128
                real, imag = stage[0:64, at : at + 128], stage[64:128, at : at + 128]
                reals.append(real * tw_cos + imag * tw_sin)
                imags.append(imag * tw_cos - real * tw_sin)
        left = jnp.concatenate([jnp.concatenate(reals, axis=0), jnp.concatenate(imags, axis=0)], axis=1)
        left = left.astype(BF16)
        out[...] = dot(jnp.concatenate([left, left], axis=1), table)
    fetch.wait()


def shifted(value, amount):
    size = 128
    lane, row = iota(value.shape, 1), iota(value.shape, 0)
    rolled = pltpu.roll(value, amount % size, 1)
    carried = pltpu.roll(rolled, amount % 64, 0)
    edge_lane = 0 if amount == 1 else size - 1
    edge_row = 0 if amount == 1 else 63
    carried = jnp.where(row == edge_row, 0.0, carried)
    return jnp.where(lane == edge_lane, carried, rolled)


def repeat_high(table):
    return jnp.concatenate([table[0:256, :], table[0:256, :], table[256:512, :]], axis=0)


def conv_kernel(
    moved, hre, him, frows, irows, flanes, ilanes, twiddle, scalars, sw, weight,
    out, edges, kept, wide, result, state, factors, arrived,
):
    fetch = pltpu.make_async_copy(weight.at[EARLY:1024], kept, arrived)
    fetch.start()
    wide[...] = moved[...].astype(F32)
    own = lax.axis_index("row")
    before = wide[pl.ds(jnp.maximum(own - 1, 0) * 18 + 17, 1), :]
    after = wide[pl.ds(jnp.minimum(own + 1, 31) * 18 + 8, 1), :]
    second = sw[1].astype(F32)
    edges[0:1, :] = jnp.where(own > 0, before, 0.0) * second[0:1]
    edges[1:2, :] = jnp.where(own < 31, after, 0.0) * second[2:3]
    smoothed = []
    for branch in range(2):
        rows = []
        for channel in range(4):
            value = wide[pl.ds(branch * 4 + channel, 64, stride=9), :]
            base = channel * 16 + branch * 8
            total = scalars[base : base + 1, :] + shifted(value, 1) * scalars[base + 1 : base + 2, :]
            total = total + value * scalars[base + 2 : base + 3, :]
            total = total + shifted(value, -1) * scalars[base + 3 : base + 4, :]
            rows.append(total)
        smoothed.append(rows)
    forward_rows, inverse_rows, forward_lanes, inverse_lanes = frows, irows, flanes, ilanes
    tw_cos, tw_sin = twiddle[0:64, :], twiddle[64:128, :]
    for channel in range(4):
        state[channel * 64 : channel * 64 + 64, :] = smoothed[1][channel]
        factors[channel * 64 : channel * 64 + 64, :] = smoothed[0][channel]
    factors[256:512, :] = jnp.ones((256, 128), F32)

    def one_order(order, carry):
        signal = [state[c * 64 : c * 64 + 64, :] for c in range(4)]
        stage = dot(forward_rows[...], stack3(jnp.concatenate(signal, axis=1)))
        reals, imags = [], []
        for place in range(4):
            real = stage[0:64, place * 128 : place * 128 + 128]
            imag = stage[64:128, place * 128 : place * 128 + 128]
            reals.append(real * tw_cos + imag * tw_sin)
            imags.append(imag * tw_cos - real * tw_sin)
        left = jnp.concatenate([jnp.concatenate(reals, axis=0), jnp.concatenate(imags, axis=0)], axis=1)
        high = left.astype(BF16)
        spectrum = dot(jnp.concatenate([high, high], axis=1), forward_lanes[...])
        real, imag = spectrum[:, 0:128], spectrum[:, 128:256]
        at = pl.multiple_of(order * 256, 256)
        tap_real, tap_imag = hre[pl.ds(at, 256), :], him[pl.ds(at, 256), :]
        left = jnp.concatenate([real * tap_real - imag * tap_imag, real * tap_imag + imag * tap_real], axis=1)
        high = left.astype(BF16)
        back = dot(jnp.concatenate([high, high], axis=1), inverse_lanes[...])
        columns = []
        for place in range(4):
            real = back[place * 64 : place * 64 + 64, 0:128]
            imag = back[place * 64 : place * 64 + 64, 128:256]
            columns.append(
                jnp.concatenate([real * tw_cos - imag * tw_sin, real * tw_sin + imag * tw_cos], axis=0)
            )
        values = dot(inverse_rows[...], stack3(jnp.concatenate(columns, axis=1)))
        for channel in range(4):
            skip = scalars[pl.ds(channel * 16 + 12 + order, 1), :]
            conv = values[:, channel * 128 : channel * 128 + 128] + signal[channel] * skip
            factor = factors[pl.ds(at + channel * 64, 64), :]
            state[channel * 64 : channel * 64 + 64, :] = conv * factor
        return carry

    lax.fori_loop(0, 2, one_order, 0)
    for channel in range(4):
        result[pl.ds(channel, 64, stride=4), :] = state[channel * 64 : channel * 64 + 64, :]
    out[...] = result[...].astype(BF16).reshape(32, 8, 128)
    fetch.wait()


def norm_kernel(moved, gate, edges, gain, out, wide, ordered):
    wide[...] = moved[...].astype(F32).reshape(256, 128)
    for half in range(2):
        for channel in range(4):
            ordered[pl.ds(half * 128 + channel, 32, stride=4), :] = wide[
                pl.ds(half * 4 + channel, 32, stride=8), :
            ]
    for half in range(2):
        edge_row = 0 if half == 0 else 127
        factor = gate[half * 128 : half * 128 + 128, :]
        factor = factor + jnp.where(iota((128, 128), 0) == edge_row, edges[half : half + 1, :], 0.0)
        value = ordered[half * 128 : half * 128 + 128, :].T * factor
        scale = lax.rsqrt(jnp.mean(value * value, axis=1, keepdims=True) + NORM_EPS)
        out[half * 4 : half * 4 + 4] = (value * scale * gain[...]).astype(BF16).reshape(4, 32, 128)


def output_kernel(mixed, early, late, out):
    left = jnp.concatenate([mixed[c] for c in range(8)], axis=1)
    out[...] = (dot(left[:, 0:EARLY], early[...]) + dot(left[:, EARLY:1024], late[...])).astype(BF16)


VMEM = pl.BlockSpec(memory_space=pltpu.VMEM)
HBM = pl.BlockSpec(memory_space=pltpu.HBM)


def run(kernel, out_shape, inputs, scratch, name, unread=0):
    multi = isinstance(out_shape, (tuple, list))
    return pl.pallas_call(
        kernel,
        out_shape=out_shape,
        in_specs=[VMEM] * (len(inputs) - unread) + [HBM] * unread,
        out_specs=tuple(VMEM for _ in out_shape) if multi else VMEM,
        scratch_shapes=scratch,
        name=name,
        compiler_params=pltpu.CompilerParams(vmem_limit_bytes=24 * 1024 * 1024),
    )(*inputs)


def near(value):
    return pltpu.with_memory_space_constraint(value, pltpu.VMEM)


def far(*values):
    return tuple(pltpu.with_memory_space_constraint(value, pltpu.HBM) for value in values)


def local(
    tokens,
    norm_gain,
    first_gate,
    second_gate,
    value_weight,
    short_weight,
    short_bias,
    embed_weight,
    embed_bias,
    inner_weight,
    inner_bias,
    filter_freq,
    filter_weight,
    filter_skip,
    output_gain,
    output_weight,
):
    small = (
        embed_weight,
        embed_bias.reshape(1, -1),
        inner_weight,
        inner_bias.reshape(1, -1),
        filter_freq.reshape(1, -1),
        filter_weight.transpose(0, 1, 3, 2),
        short_weight,
        short_bias,
        filter_skip,
        output_gain.reshape(1, -1),
    )
    sent, rows, *small = run(
        project_kernel,
        (
            pltpu.VMEM((576, 128), BF16),
            pltpu.VMEM((256, 2048), BF16),
            *(pltpu.VMEM(value.shape, value.dtype) for value in small),
        ),
        far(tokens, norm_gain.reshape(1, -1), first_gate, second_gate, value_weight, *small),
        [
            pltpu.VMEM((256, 2048), BF16),
            pltpu.VMEM((1, 2048), F32),
            pltpu.VMEM((2048, 128), BF16),
            pltpu.VMEM((2048, 128), BF16),
            pltpu.VMEM((2048, 128), BF16),
            pltpu.VMEM((576, 128), F32),
            pltpu.SemaphoreType.DMA((6,)),
            pltpu.SemaphoreType.DMA((len(small),)),
        ],
        "project",
        5 + len(small),
    )
    moved = lax.all_to_all(
        sent.reshape(32, 9, 2, 128), "row", split_axis=0, concat_axis=0, tiled=True
    ).reshape(576, 128)
    *prepared, gate, kept_early = run(
        filter_kernel,
        (
            pltpu.VMEM((512, 128), F32),
            pltpu.VMEM((512, 128), F32),
            pltpu.VMEM((128, 192), BF16),
            pltpu.VMEM((64, 384), BF16),
            pltpu.VMEM((512, 256), BF16),
            pltpu.VMEM((512, 256), BF16),
            pltpu.VMEM((128, 128), F32),
            pltpu.VMEM((64, 128), F32),
            pltpu.VMEM((256, 128), F32),
            pltpu.VMEM((EARLY, 2048), BF16),
        ),
        (*(near(value) for value in (rows, *small[:9])), *far(second_gate, output_weight)),
        [
            pltpu.VMEM((256, 128), F32),
            pltpu.VMEM((64, 256), BF16),
            pltpu.VMEM((64, 256), BF16),
            pltpu.VMEM((1024, 128), F32),
            pltpu.VMEM((32, 128), F32),
            pltpu.VMEM((2048, 128), BF16),
            pltpu.SemaphoreType.DMA((2,)),
        ],
        "filters",
        2,
    )
    mixed, edges, kept = run(
        conv_kernel,
        (pltpu.VMEM((32, 8, 128), BF16), pltpu.VMEM((2, 128), F32), pltpu.VMEM((1024 - EARLY, 2048), BF16)),
        (*(near(value) for value in (moved, *prepared, small[6])), *far(output_weight)),
        [
            pltpu.VMEM((576, 128), F32),
            pltpu.VMEM((256, 128), F32),
            pltpu.VMEM((256, 128), F32),
            pltpu.VMEM((512, 128), F32),
            pltpu.SemaphoreType.DMA,
        ],
        "convolve",
        1,
    )
    result = lax.all_to_all(mixed, "row", split_axis=0, concat_axis=0, tiled=True)
    normed = run(
        norm_kernel,
        pltpu.VMEM((8, 32, 128), BF16),
        tuple(near(value) for value in (result, gate, edges, small[9])),
        [pltpu.VMEM((256, 128), F32), pltpu.VMEM((256, 128), F32)],
        "groupnorm",
    )
    gathered = lax.all_to_all(normed, "col", split_axis=0, concat_axis=0, tiled=True)
    return run(
        output_kernel,
        jax.ShapeDtypeStruct((32, 2048), BF16),
        (near(gathered), near(kept_early), near(kept)),
        [],
        "output",
    )


def solution(mesh):
    in_specs = (
        P("row", None),
        P(),
        P(None, "col"),
        P(None, "col"),
        P(None, "col"),
        P(None, None, "col"),
        P(None, "col"),
        P(),
        P(),
        P(),
        P(),
        P(),
        P(None, None, None, ("col", "row")),
        P(None, ("col", "row")),
        P("col"),
        P(),
    )
    out_specs = P(("row", "col"), None)
    return jax.shard_map(local, mesh=mesh, in_specs=in_specs, out_specs=out_specs, check_vma=False)
```

```python
import functools
import math

import jax
import jax.numpy as jnp
from jax import lax
from jax.experimental import pallas as pl
from jax.experimental.pallas import tpu as pltpu
from jax.sharding import PartitionSpec as P

CHANNELS = 1024
FREQ_BANDS = 16
EARLY = 192
NORM_EPS = 1e-06
DECAY_SLOW = math.log(0.01) / 1.5
DECAY_FAST = math.log(0.01) / 0.3

F32 = jnp.float32
BF16 = jnp.bfloat16

LONG_COEFFS = (
    6.283185160089469,
    -41.34165503141532,
    81.60100407320796,
    -76.54978229245017,
    39.5367060575916,
)
SHORT_COEFFS = (6.283164044302229, -41.33714237106961, 81.3407688866883, -70.99343326314641)


def cos_turns(turns, coeffs=LONG_COEFFS):
    r = 0.25 - jnp.abs(turns - jnp.round(turns))
    s = r * r
    acc = s * coeffs[-1] + coeffs[-2]
    for coeff in coeffs[-3::-1]:
        acc = acc * s + coeff
    return acc * r


def sin_turns(turns):
    return cos_turns(turns - 0.25)


def split(value):
    high = value.astype(BF16)
    low = (value - high.astype(F32)).astype(BF16)
    return high, low


def iota(shape, dim):
    return lax.broadcasted_iota(jnp.int32, shape, dim)


def to_turns(index, period):
    return (index & (period - 1)).astype(F32) * (1.0 / period)


def row_dft_table():
    shape = (128, 192)
    k1, n1 = iota(shape, 0) & 63, iota(shape, 1) & 63
    turns = to_turns((2 * k1 + 1) * n1, 256)
    value = cos_turns(turns + jnp.where(iota(shape, 0) < 64, 0.0, 0.25))
    high = value.astype(BF16).astype(F32)
    return jnp.where(iota(shape, 1) < 128, high, value - high).astype(BF16)


def row_inverse_table(scale):
    shape = (64, 384)
    n1, k1 = iota(shape, 0), iota(shape, 1) & 63
    turns = to_turns((2 * k1 + 1) * n1, 256)
    value = cos_turns(turns + jnp.where((iota(shape, 1) & 64) == 0, 0.0, 0.25)) * scale
    high = value.astype(BF16).astype(F32)
    return jnp.where(iota(shape, 1) < 256, high, value - high).astype(BF16)


def twiddles():
    shape = (64, 128)
    turns = to_turns((2 * iota(shape, 0) + 1) * iota(shape, 1), 32768)
    return cos_turns(turns), sin_turns(turns)


def lane_dft():
    shape = (128, 128)
    turns = to_turns(iota(shape, 0) * iota(shape, 1), 128)
    return split(cos_turns(turns)), split(sin_turns(turns))


def dot(left, right):
    return jnp.dot(left, right, preferred_element_type=F32)


def stack3(value):
    high, low = split(value)
    return jnp.concatenate([high, low, high], axis=0)


def lanes3(value):
    high, low = split(value)
    return jnp.concatenate([high, low, high], axis=1)


def project_kernel(*refs):
    extra = (len(refs) - 15) // 2
    tokens, gain, w0, w1, w2 = refs[0:5]
    small = refs[5 : 5 + extra]
    out, normed = refs[5 + extra : 7 + extra]
    carried = refs[7 + extra : 7 + 2 * extra]
    near_tokens, near_gain, n0, n1, n2, scratch, arrived, carry = refs[7 + 2 * extra :]
    rows = 128
    copies = [pltpu.make_async_copy(gain, near_gain, arrived.at[0])]
    for part in range(2):
        where = pl.ds(part * rows, rows)
        copies.append(pltpu.make_async_copy(tokens.at[where], near_tokens.at[where], arrived.at[part + 1]))
    for index, (source, target) in enumerate(((w0, n0), (w2, n2), (w1, n1))):
        copies.append(pltpu.make_async_copy(source, target, arrived.at[index + 3]))
    carries = [
        pltpu.make_async_copy(source, target, carry.at[index])
        for index, (source, target) in enumerate(zip(small, carried))
    ]
    for copy in copies:
        copy.start()
    copies[0].wait()
    for part in range(2):
        copies[part + 1].wait()
        wide = near_tokens[part * rows : part * rows + rows, :].astype(F32)
        scale = lax.rsqrt(jnp.mean(wide * wide, axis=1, keepdims=True) + NORM_EPS)
        normed[part * rows : part * rows + rows, :] = (wide * scale * near_gain[...]).astype(BF16)
    for copy in carries:
        copy.start()
    copies[3].wait()
    copies[4].wait()
    weights = jnp.concatenate([n0[...], n2[...]], axis=1)
    for half in range(2):
        gates = dot(normed[half * 128 : half * 128 + 128, :], weights)
        for branch in range(2):
            block = gates[:, branch * 128 : branch * 128 + 128].T
            for peer in range(32):
                start = peer * 18 + half * 9 + branch * 4
                scratch[start : start + 4, :] = block[peer * 4 : peer * 4 + 4, :]
    copies[5].wait()
    edges = dot(jnp.concatenate([normed[0:16, :], normed[240:256, :]], axis=0), n1[...])
    for peer in range(32):
        scratch[peer * 18 + 8 : peer * 18 + 9, :] = edges[0:1, :]
        scratch[peer * 18 + 17 : peer * 18 + 18, :] = edges[31:32, :]
    out[...] = scratch[...].astype(BF16)
    for copy in carries:
        copy.wait()


def lane_table(sign, cos, sin):
    def part(c, s):
        top = jnp.concatenate([c, -s if sign > 0 else s], axis=1)
        bottom = jnp.concatenate([s if sign > 0 else -s, c], axis=1)
        return jnp.concatenate([top, bottom], axis=0)

    high, low = part(cos[0], sin[0]), part(cos[1], sin[1])
    return jnp.concatenate([high, low], axis=0)


def filter_kernel(
    normed, ew, eb, iw, ib, freq, fw, sw, sb, skip, second_weight, weight,
    hre, him, frows, irows, flanes, ilanes, twiddle, scalars, gate, kept,
    build, lhs1, lhs2, taps, turned, w1, arrived,
):
    length = 8192
    fetch_second = pltpu.make_async_copy(second_weight, w1, arrived.at[1])
    fetch_second.start()
    fetch = pltpu.make_async_copy(weight.at[0:EARLY], kept, arrived.at[0])
    fetch.start()
    own = lax.axis_index("row") * 4
    first_channel = lax.axis_index("col") * 128 + own

    lines = []
    for branch in range(3):
        lines.append(sb[branch : branch + 1, :])
        lines.append(sw[branch].astype(F32))
    lines.append(jnp.zeros((4, 128), F32))
    lines = pltpu.roll(jnp.concatenate(lines, axis=0), (128 - own) % 128, 1)
    for channel in range(4):
        scalars[channel * 16 : channel * 16 + 16, :] = jnp.broadcast_to(
            lines[:, channel : channel + 1], (16, 128)
        )
        scalars[channel * 16 + 12 : channel * 16 + 14, :] = jnp.broadcast_to(
            skip[:, channel : channel + 1], (2, 128)
        )

    frows[...] = row_dft_table()
    irows[...] = row_inverse_table(1.0 / 8192)
    tw_cos, tw_sin = twiddles()
    twiddle[0:64, :] = tw_cos
    twiddle[64:128, :] = tw_sin
    cos, sin = lane_dft()
    flanes[...] = lane_table(1, cos, sin)
    ilanes[...] = lane_table(-1, cos, sin)

    def high_of(value):
        return value.astype(BF16).astype(F32)

    turns_of = freq[...] * (1.0 / (2.0 * math.pi))
    build[...] = jnp.zeros_like(build)
    embed = ew[...] * turns_of
    bias = eb[...] * turns_of - 0.25
    rows = jnp.concatenate([embed[1:33], embed[0:1], bias], axis=0)
    build[0:34, 0:64] = high_of(rows)
    build[48:82, 0:64] = high_of(rows)
    build[96:130, 0:64] = rows - high_of(rows)
    lhs1[...] = build[...].T[0:64, :].astype(BF16)
    inner = iw[...] * turns_of
    bias = ib[...] * turns_of - 0.25
    build[...] = jnp.zeros_like(build)
    build[0:64, 0:64] = high_of(inner)
    build[64:128, 0:64] = high_of(inner)
    build[128:192, 0:64] = inner - high_of(inner)
    build[192:193, 0:64] = high_of(bias)
    build[193:194, 0:64] = bias - high_of(bias)
    lhs2[...] = build[...].T[0:64, :].astype(BF16)
    left1 = lhs1[:, 0:144]
    left2 = lhs2[:, 0:208]
    parts = []
    for order in range(2):
        parts.append(fw[order, 0] + fw[order, 1])
        parts.append(fw[order, 0] - fw[order, 1])
    fhigh, flow = split(jnp.concatenate(parts, axis=0))
    left3 = jnp.concatenate([fhigh, flow], axis=1)

    band_step = (FREQ_BANDS - 1 - 0.0001) / (FREQ_BANDS - 1)
    band = 0.0001 + iota((16, 128), 0).astype(F32) * band_step
    lane = iota((16, 128), 1).astype(F32)
    coarse = band * (lane * (128.0 / length))
    fine = band * (lane * (1.0 / length))
    coarse_cos, coarse_sin = cos_turns(coarse), sin_turns(coarse)
    fine_cos, fine_sin = cos_turns(fine), sin_turns(fine)
    row = iota((16, 128), 0)
    extra = jnp.where(row == 0, lane * (1.0 / (length - 1)), jnp.where(row == 1, 1.0, 0.0))
    extra_step = jnp.where(row == 0, 128.0 / (length - 1), 0.0)

    rate_step = (DECAY_SLOW - DECAY_FAST) / (CHANNELS - 1)
    channel_row = (iota((8, 128), 0) & 3) + first_channel
    rate = -DECAY_SLOW + channel_row.astype(F32) * rate_step
    ramp = iota((8, 128), 1).astype(F32) * (1.0 / (length - 1))

    chunk = 4096
    blocks = chunk // 128
    ones16 = jnp.ones((16, chunk), BF16)
    turned[0:16, :] = coarse_cos
    turned[16:32, :] = coarse_sin

    def one_chunk(step, carry):
        first = step * blocks
        column = pltpu.roll(turned[...], (128 - first) % 128, 1)
        start = first.astype(F32)
        feature = []
        for block in range(blocks):
            ca = jnp.broadcast_to(column[0:16, block : block + 1], (16, 128))
            sa = jnp.broadcast_to(column[16:32, block : block + 1], (16, 128))
            feature.append(
                jnp.concatenate(
                    [
                        ca * fine_cos - sa * fine_sin,
                        -(sa * fine_cos + ca * fine_sin),
                        extra + extra_step * (start + float(block)),
                    ],
                    axis=0,
                )
            )
        hidden = cos_turns(dot(left1, stack3(jnp.concatenate(feature, axis=1))), SHORT_COEFFS)
        hidden = cos_turns(
            dot(left2, jnp.concatenate([stack3(hidden), ones16], axis=0)), SHORT_COEFFS
        )
        high = hidden.astype(BF16)
        value = dot(left3, jnp.concatenate([high, high], axis=0))
        for block in range(blocks):
            here = ramp + (start + float(block)) * (128.0 / (length - 1))
            window = jnp.exp(here * -rate)
            piece = value[:, block * 128 : block * 128 + 128] * jnp.concatenate([window, window], axis=0)
            at = pl.multiple_of((first + block) * 16, 16)
            taps[pl.ds(at, 16), :] = piece
        return carry

    lax.fori_loop(0, length // chunk, one_chunk, 0)
    piece = taps[0:16, :]
    swapped = jnp.concatenate([piece[4:8], piece[0:4], piece[12:16], piece[8:12]], axis=0)
    taps[0:16, :] = jnp.where(iota((16, 128), 1) == 0, 0.5 * (piece + swapped), piece)

    fetch_second.wait()
    source = dot(normed[...], w1[...]).astype(BF16).astype(F32)
    zero = jnp.zeros((1, 128), F32)
    before = jnp.concatenate([zero, source[0:255]], axis=0)
    after = jnp.concatenate([source[1:256], zero], axis=0)
    second = sw[1].astype(F32)
    total = sb[1:2, :] + before * second[0:1]
    total = total + source * second[1:2]
    gate[...] = total + after * second[2:3]

    spread = jnp.concatenate([taps[pl.ds(r, 64, stride=16), :] for r in range(16)], axis=1)
    stage = dot(frows[...], stack3(spread))
    (cos_high, cos_low), (sin_high, sin_low) = cos, sin
    real_table = jnp.concatenate([cos_high, sin_high, cos_low, sin_low], axis=0)
    imag_table = jnp.concatenate([-sin_high, cos_high, -sin_low, cos_low], axis=0)
    for kind, table, out in ((0, real_table, hre), (1, imag_table, him)):
        reals, imags = [], []
        for order in range(2):
            for channel in range(4):
                at = (order * 8 + kind * 4 + channel) * 128
                real, imag = stage[0:64, at : at + 128], stage[64:128, at : at + 128]
                reals.append(real * tw_cos + imag * tw_sin)
                imags.append(imag * tw_cos - real * tw_sin)
        left = jnp.concatenate([jnp.concatenate(reals, axis=0), jnp.concatenate(imags, axis=0)], axis=1)
        left = left.astype(BF16)
        out[...] = dot(jnp.concatenate([left, left], axis=1), table)
    fetch.wait()


def shifted(value, amount):
    size = 128
    lane, row = iota(value.shape, 1), iota(value.shape, 0)
    rolled = pltpu.roll(value, amount % size, 1)
    carried = pltpu.roll(rolled, amount % 64, 0)
    edge_lane = 0 if amount == 1 else size - 1
    edge_row = 0 if amount == 1 else 63
    carried = jnp.where(row == edge_row, 0.0, carried)
    return jnp.where(lane == edge_lane, carried, rolled)


def repeat_high(table):
    return jnp.concatenate([table[0:256, :], table[0:256, :], table[256:512, :]], axis=0)


def conv_kernel(
    moved, hre, him, frows, irows, flanes, ilanes, twiddle, scalars, sw, weight,
    out, edges, kept, wide, result, state, factors, arrived,
):
    fetch = pltpu.make_async_copy(weight.at[EARLY:1024], kept, arrived)
    fetch.start()
    wide[...] = moved[...].astype(F32)
    own = lax.axis_index("row")
    before = wide[pl.ds(jnp.maximum(own - 1, 0) * 18 + 17, 1), :]
    after = wide[pl.ds(jnp.minimum(own + 1, 31) * 18 + 8, 1), :]
    second = sw[1].astype(F32)
    edges[0:1, :] = jnp.where(own > 0, before, 0.0) * second[0:1]
    edges[1:2, :] = jnp.where(own < 31, after, 0.0) * second[2:3]
    smoothed = []
    for branch in range(2):
        rows = []
        for channel in range(4):
            value = wide[pl.ds(branch * 4 + channel, 64, stride=9), :]
            base = channel * 16 + branch * 8
            total = scalars[base : base + 1, :] + shifted(value, 1) * scalars[base + 1 : base + 2, :]
            total = total + value * scalars[base + 2 : base + 3, :]
            total = total + shifted(value, -1) * scalars[base + 3 : base + 4, :]
            rows.append(total)
        smoothed.append(rows)
    forward_rows, inverse_rows, forward_lanes, inverse_lanes = frows, irows, flanes, ilanes
    tw_cos, tw_sin = twiddle[0:64, :], twiddle[64:128, :]
    for channel in range(4):
        state[channel * 64 : channel * 64 + 64, :] = smoothed[1][channel]
        factors[channel * 64 : channel * 64 + 64, :] = smoothed[0][channel]
    factors[256:512, :] = jnp.ones((256, 128), F32)

    def one_order(order, carry):
        signal = [state[c * 64 : c * 64 + 64, :] for c in range(4)]
        stage = dot(forward_rows[...], stack3(jnp.concatenate(signal, axis=1)))
        reals, imags = [], []
        for place in range(4):
            real = stage[0:64, place * 128 : place * 128 + 128]
            imag = stage[64:128, place * 128 : place * 128 + 128]
            reals.append(real * tw_cos + imag * tw_sin)
            imags.append(imag * tw_cos - real * tw_sin)
        left = jnp.concatenate([jnp.concatenate(reals, axis=0), jnp.concatenate(imags, axis=0)], axis=1)
        spectrum = dot(lanes3(left), repeat_high(forward_lanes))
        real, imag = spectrum[:, 0:128], spectrum[:, 128:256]
        at = pl.multiple_of(order * 256, 256)
        tap_real, tap_imag = hre[pl.ds(at, 256), :], him[pl.ds(at, 256), :]
        left = jnp.concatenate([real * tap_real - imag * tap_imag, real * tap_imag + imag * tap_real], axis=1)
        back = dot(lanes3(left), repeat_high(inverse_lanes))
        columns = []
        for place in range(4):
            real = back[place * 64 : place * 64 + 64, 0:128]
            imag = back[place * 64 : place * 64 + 64, 128:256]
            columns.append(
                jnp.concatenate([real * tw_cos - imag * tw_sin, real * tw_sin + imag * tw_cos], axis=0)
            )
        values = dot(inverse_rows[...], stack3(jnp.concatenate(columns, axis=1)))
        for channel in range(4):
            skip = scalars[pl.ds(channel * 16 + 12 + order, 1), :]
            conv = values[:, channel * 128 : channel * 128 + 128] + signal[channel] * skip
            factor = factors[pl.ds(at + channel * 64, 64), :]
            state[channel * 64 : channel * 64 + 64, :] = conv * factor
        return carry

    lax.fori_loop(0, 2, one_order, 0)
    for channel in range(4):
        result[pl.ds(channel, 64, stride=4), :] = state[channel * 64 : channel * 64 + 64, :]
    out[...] = result[...].astype(BF16).reshape(32, 8, 128)
    fetch.wait()


def norm_kernel(moved, gate, edges, gain, out, wide, ordered):
    wide[...] = moved[...].astype(F32).reshape(256, 128)
    for half in range(2):
        for channel in range(4):
            ordered[pl.ds(half * 128 + channel, 32, stride=4), :] = wide[
                pl.ds(half * 4 + channel, 32, stride=8), :
            ]
    for half in range(2):
        edge_row = 0 if half == 0 else 127
        factor = gate[half * 128 : half * 128 + 128, :]
        factor = factor + jnp.where(iota((128, 128), 0) == edge_row, edges[half : half + 1, :], 0.0)
        value = ordered[half * 128 : half * 128 + 128, :].T * factor
        scale = lax.rsqrt(jnp.mean(value * value, axis=1, keepdims=True) + NORM_EPS)
        out[half * 4 : half * 4 + 4] = (value * scale * gain[...]).astype(BF16).reshape(4, 32, 128)


def output_kernel(mixed, early, late, out):
    left = jnp.concatenate([mixed[c] for c in range(8)], axis=1)
    out[...] = (dot(left[:, 0:EARLY], early[...]) + dot(left[:, EARLY:1024], late[...])).astype(BF16)


VMEM = pl.BlockSpec(memory_space=pltpu.VMEM)
HBM = pl.BlockSpec(memory_space=pltpu.HBM)


def run(kernel, out_shape, inputs, scratch, name, unread=0):
    multi = isinstance(out_shape, (tuple, list))
    return pl.pallas_call(
        kernel,
        out_shape=out_shape,
        in_specs=[VMEM] * (len(inputs) - unread) + [HBM] * unread,
        out_specs=tuple(VMEM for _ in out_shape) if multi else VMEM,
        scratch_shapes=scratch,
        name=name,
        compiler_params=pltpu.CompilerParams(vmem_limit_bytes=24 * 1024 * 1024),
    )(*inputs)


def near(value):
    return pltpu.with_memory_space_constraint(value, pltpu.VMEM)


def far(*values):
    return tuple(pltpu.with_memory_space_constraint(value, pltpu.HBM) for value in values)


def local(
    tokens,
    norm_gain,
    first_gate,
    second_gate,
    value_weight,
    short_weight,
    short_bias,
    embed_weight,
    embed_bias,
    inner_weight,
    inner_bias,
    filter_freq,
    filter_weight,
    filter_skip,
    output_gain,
    output_weight,
):
    small = (
        embed_weight,
        embed_bias.reshape(1, -1),
        inner_weight,
        inner_bias.reshape(1, -1),
        filter_freq.reshape(1, -1),
        filter_weight.transpose(0, 1, 3, 2),
        short_weight,
        short_bias,
        filter_skip,
        output_gain.reshape(1, -1),
    )
    sent, rows, *small = run(
        project_kernel,
        (
            pltpu.VMEM((576, 128), BF16),
            pltpu.VMEM((256, 2048), BF16),
            *(pltpu.VMEM(value.shape, value.dtype) for value in small),
        ),
        far(tokens, norm_gain.reshape(1, -1), first_gate, second_gate, value_weight, *small),
        [
            pltpu.VMEM((256, 2048), BF16),
            pltpu.VMEM((1, 2048), F32),
            pltpu.VMEM((2048, 128), BF16),
            pltpu.VMEM((2048, 128), BF16),
            pltpu.VMEM((2048, 128), BF16),
            pltpu.VMEM((576, 128), F32),
            pltpu.SemaphoreType.DMA((6,)),
            pltpu.SemaphoreType.DMA((len(small),)),
        ],
        "project",
        5 + len(small),
    )
    moved = lax.all_to_all(
        sent.reshape(32, 9, 2, 128), "row", split_axis=0, concat_axis=0, tiled=True
    ).reshape(576, 128)
    *prepared, gate, kept_early = run(
        filter_kernel,
        (
            pltpu.VMEM((512, 128), F32),
            pltpu.VMEM((512, 128), F32),
            pltpu.VMEM((128, 192), BF16),
            pltpu.VMEM((64, 384), BF16),
            pltpu.VMEM((512, 256), BF16),
            pltpu.VMEM((512, 256), BF16),
            pltpu.VMEM((128, 128), F32),
            pltpu.VMEM((64, 128), F32),
            pltpu.VMEM((256, 128), F32),
            pltpu.VMEM((EARLY, 2048), BF16),
        ),
        (*(near(value) for value in (rows, *small[:9])), *far(second_gate, output_weight)),
        [
            pltpu.VMEM((256, 128), F32),
            pltpu.VMEM((64, 256), BF16),
            pltpu.VMEM((64, 256), BF16),
            pltpu.VMEM((1024, 128), F32),
            pltpu.VMEM((32, 128), F32),
            pltpu.VMEM((2048, 128), BF16),
            pltpu.SemaphoreType.DMA((2,)),
        ],
        "filters",
        2,
    )
    mixed, edges, kept = run(
        conv_kernel,
        (pltpu.VMEM((32, 8, 128), BF16), pltpu.VMEM((2, 128), F32), pltpu.VMEM((1024 - EARLY, 2048), BF16)),
        (*(near(value) for value in (moved, *prepared, small[6])), *far(output_weight)),
        [
            pltpu.VMEM((576, 128), F32),
            pltpu.VMEM((256, 128), F32),
            pltpu.VMEM((256, 128), F32),
            pltpu.VMEM((512, 128), F32),
            pltpu.SemaphoreType.DMA,
        ],
        "convolve",
        1,
    )
    result = lax.all_to_all(mixed, "row", split_axis=0, concat_axis=0, tiled=True)
    normed = run(
        norm_kernel,
        pltpu.VMEM((8, 32, 128), BF16),
        tuple(near(value) for value in (result, gate, edges, small[9])),
        [pltpu.VMEM((256, 128), F32), pltpu.VMEM((256, 128), F32)],
        "groupnorm",
    )
    gathered = lax.all_to_all(normed, "col", split_axis=0, concat_axis=0, tiled=True)
    return run(
        output_kernel,
        jax.ShapeDtypeStruct((32, 2048), BF16),
        (near(gathered), near(kept_early), near(kept)),
        [],
        "output",
    )


def solution(mesh):
    in_specs = (
        P("row", None),
        P(),
        P(None, "col"),
        P(None, "col"),
        P(None, "col"),
        P(None, None, "col"),
        P(None, "col"),
        P(),
        P(),
        P(),
        P(),
        P(),
        P(None, None, None, ("col", "row")),
        P(None, ("col", "row")),
        P("col"),
        P(),
    )
    out_specs = P(("row", "col"), None)
    return jax.shard_map(local, mesh=mesh, in_specs=in_specs, out_specs=out_specs, check_vma=False)
```

```python
import functools
import math

import jax
import jax.numpy as jnp
from jax import lax
from jax.experimental import pallas as pl
from jax.experimental.pallas import tpu as pltpu
from jax.sharding import PartitionSpec as P

CHANNELS = 1024
FREQ_BANDS = 16
EARLY = 192
NORM_EPS = 1e-06
DECAY_SLOW = math.log(0.01) / 1.5
DECAY_FAST = math.log(0.01) / 0.3

F32 = jnp.float32
BF16 = jnp.bfloat16

LONG_COEFFS = (
    6.283185160089469,
    -41.34165503141532,
    81.60100407320796,
    -76.54978229245017,
    39.5367060575916,
)
SHORT_COEFFS = (6.283164044302229, -41.33714237106961, 81.3407688866883, -70.99343326314641)


def cos_turns(turns, coeffs=LONG_COEFFS):
    r = 0.25 - jnp.abs(turns - jnp.round(turns))
    s = r * r
    acc = s * coeffs[-1] + coeffs[-2]
    for coeff in coeffs[-3::-1]:
        acc = acc * s + coeff
    return acc * r


def sin_turns(turns):
    return cos_turns(turns - 0.25)


def split(value):
    high = value.astype(BF16)
    low = (value - high.astype(F32)).astype(BF16)
    return high, low


def iota(shape, dim):
    return lax.broadcasted_iota(jnp.int32, shape, dim)


def to_turns(index, period):
    return (index & (period - 1)).astype(F32) * (1.0 / period)


def row_dft_table():
    shape = (128, 192)
    k1, n1 = iota(shape, 0) & 63, iota(shape, 1) & 63
    turns = to_turns((2 * k1 + 1) * n1, 256)
    value = cos_turns(turns + jnp.where(iota(shape, 0) < 64, 0.0, 0.25))
    high = value.astype(BF16).astype(F32)
    return jnp.where(iota(shape, 1) < 128, high, value - high).astype(BF16)


def row_inverse_table(scale):
    shape = (64, 384)
    n1, k1 = iota(shape, 0), iota(shape, 1) & 63
    turns = to_turns((2 * k1 + 1) * n1, 256)
    value = cos_turns(turns + jnp.where((iota(shape, 1) & 64) == 0, 0.0, 0.25)) * scale
    high = value.astype(BF16).astype(F32)
    return jnp.where(iota(shape, 1) < 256, high, value - high).astype(BF16)


def twiddles():
    shape = (64, 128)
    turns = to_turns((2 * iota(shape, 0) + 1) * iota(shape, 1), 32768)
    return cos_turns(turns), sin_turns(turns)


def lane_dft():
    shape = (128, 128)
    turns = to_turns(iota(shape, 0) * iota(shape, 1), 128)
    return split(cos_turns(turns)), split(sin_turns(turns))


def dot(left, right):
    return jnp.dot(left, right, preferred_element_type=F32)


def stack3(value):
    high, low = split(value)
    return jnp.concatenate([high, low, high], axis=0)


def lanes3(value):
    high, low = split(value)
    return jnp.concatenate([high, low, high], axis=1)


def project_kernel(*refs):
    extra = (len(refs) - 15) // 2
    tokens, gain, w0, w1, w2 = refs[0:5]
    small = refs[5 : 5 + extra]
    out, normed = refs[5 + extra : 7 + extra]
    carried = refs[7 + extra : 7 + 2 * extra]
    near_tokens, near_gain, n0, n1, n2, scratch, arrived, carry = refs[7 + 2 * extra :]
    rows = 128
    copies = [pltpu.make_async_copy(gain, near_gain, arrived.at[0])]
    for part in range(2):
        where = pl.ds(part * rows, rows)
        copies.append(pltpu.make_async_copy(tokens.at[where], near_tokens.at[where], arrived.at[part + 1]))
    for index, (source, target) in enumerate(((w0, n0), (w2, n2), (w1, n1))):
        copies.append(pltpu.make_async_copy(source, target, arrived.at[index + 3]))
    carries = [
        pltpu.make_async_copy(source, target, carry.at[index])
        for index, (source, target) in enumerate(zip(small, carried))
    ]
    for copy in copies[:3]:
        copy.start()
    for copy in copies[3:]:
        copy.start(priority=1)
    copies[0].wait()
    for part in range(2):
        copies[part + 1].wait()
        wide = near_tokens[part * rows : part * rows + rows, :].astype(F32)
        scale = lax.rsqrt(jnp.mean(wide * wide, axis=1, keepdims=True) + NORM_EPS)
        normed[part * rows : part * rows + rows, :] = (wide * scale * near_gain[...]).astype(BF16)
    for copy in carries:
        copy.start()
    copies[3].wait()
    copies[4].wait()
    weights = jnp.concatenate([n0[...], n2[...]], axis=1)
    for half in range(2):
        gates = dot(normed[half * 128 : half * 128 + 128, :], weights)
        for branch in range(2):
            block = gates[:, branch * 128 : branch * 128 + 128].T
            for peer in range(32):
                start = peer * 18 + half * 9 + branch * 4
                scratch[start : start + 4, :] = block[peer * 4 : peer * 4 + 4, :]
    copies[5].wait()
    edges = dot(jnp.concatenate([normed[0:8, :], normed[248:256, :]], axis=0), n1[...])
    for peer in range(32):
        scratch[peer * 18 + 8 : peer * 18 + 9, :] = edges[0:1, :]
        scratch[peer * 18 + 17 : peer * 18 + 18, :] = edges[15:16, :]
    out[...] = scratch[...].astype(BF16)
    for copy in carries:
        copy.wait()


def lane_table(sign, cos, sin):
    def part(c, s):
        top = jnp.concatenate([c, -s if sign > 0 else s], axis=1)
        bottom = jnp.concatenate([s if sign > 0 else -s, c], axis=1)
        return jnp.concatenate([top, bottom], axis=0)

    high, low = part(cos[0], sin[0]), part(cos[1], sin[1])
    return jnp.concatenate([high, low], axis=0)


def filter_kernel(
    normed, ew, eb, iw, ib, freq, fw, sw, sb, skip, second_weight, weight,
    hre, him, frows, irows, flanes, ilanes, twiddle, scalars, gate, kept,
    build, lhs1, lhs2, taps, turned, w1, arrived,
):
    length = 8192
    fetch_second = pltpu.make_async_copy(second_weight, w1, arrived.at[1])
    fetch_second.start()
    fetch = pltpu.make_async_copy(weight.at[0:EARLY], kept, arrived.at[0])
    fetch.start()
    own = lax.axis_index("row") * 4
    first_channel = lax.axis_index("col") * 128 + own

    lines = []
    for branch in range(3):
        lines.append(sb[branch : branch + 1, :])
        lines.append(sw[branch].astype(F32))
    lines.append(jnp.zeros((4, 128), F32))
    lines = pltpu.roll(jnp.concatenate(lines, axis=0), (128 - own) % 128, 1)
    for channel in range(4):
        scalars[channel * 16 : channel * 16 + 16, :] = jnp.broadcast_to(
            lines[:, channel : channel + 1], (16, 128)
        )
        scalars[channel * 16 + 12 : channel * 16 + 14, :] = jnp.broadcast_to(
            skip[:, channel : channel + 1], (2, 128)
        )

    frows[...] = row_dft_table()
    irows[...] = row_inverse_table(1.0 / 8192)
    tw_cos, tw_sin = twiddles()
    twiddle[0:64, :] = tw_cos
    twiddle[64:128, :] = tw_sin
    cos, sin = lane_dft()
    flanes[...] = lane_table(1, cos, sin)
    ilanes[...] = lane_table(-1, cos, sin)

    def high_of(value):
        return value.astype(BF16).astype(F32)

    turns_of = freq[...] * (1.0 / (2.0 * math.pi))
    build[...] = jnp.zeros_like(build)
    embed = ew[...] * turns_of
    bias = eb[...] * turns_of - 0.25
    rows = jnp.concatenate([embed[1:33], embed[0:1], bias], axis=0)
    build[0:34, 0:64] = high_of(rows)
    build[48:82, 0:64] = high_of(rows)
    build[96:130, 0:64] = rows - high_of(rows)
    lhs1[...] = build[...].T[0:64, :].astype(BF16)
    inner = iw[...] * turns_of
    bias = ib[...] * turns_of - 0.25
    build[...] = jnp.zeros_like(build)
    build[0:64, 0:64] = high_of(inner)
    build[64:128, 0:64] = high_of(inner)
    build[128:192, 0:64] = inner - high_of(inner)
    build[192:193, 0:64] = high_of(bias)
    build[193:194, 0:64] = bias - high_of(bias)
    lhs2[...] = build[...].T[0:64, :].astype(BF16)
    left1 = lhs1[:, 0:144]
    left2 = lhs2[:, 0:208]
    parts = []
    for order in range(2):
        parts.append(fw[order, 0] + fw[order, 1])
        parts.append(fw[order, 0] - fw[order, 1])
    fhigh, flow = split(jnp.concatenate(parts, axis=0))
    left3 = jnp.concatenate([fhigh, flow], axis=1)

    band_step = (FREQ_BANDS - 1 - 0.0001) / (FREQ_BANDS - 1)
    band = 0.0001 + iota((16, 128), 0).astype(F32) * band_step
    lane = iota((16, 128), 1).astype(F32)
    coarse = band * (lane * (128.0 / length))
    fine = band * (lane * (1.0 / length))
    coarse_cos, coarse_sin = cos_turns(coarse), sin_turns(coarse)
    fine_cos, fine_sin = cos_turns(fine), sin_turns(fine)
    row = iota((16, 128), 0)
    extra = jnp.where(row == 0, lane * (1.0 / (length - 1)), jnp.where(row == 1, 1.0, 0.0))
    extra_step = jnp.where(row == 0, 128.0 / (length - 1), 0.0)

    rate_step = (DECAY_SLOW - DECAY_FAST) / (CHANNELS - 1)
    channel_row = (iota((8, 128), 0) & 3) + first_channel
    rate = -DECAY_SLOW + channel_row.astype(F32) * rate_step
    ramp = iota((8, 128), 1).astype(F32) * (1.0 / (length - 1))

    chunk = 4096
    blocks = chunk // 128
    ones16 = jnp.ones((16, chunk), BF16)
    turned[0:16, :] = coarse_cos
    turned[16:32, :] = coarse_sin

    def one_chunk(step, carry):
        first = step * blocks
        column = pltpu.roll(turned[...], (128 - first) % 128, 1)
        start = first.astype(F32)
        feature = []
        for block in range(blocks):
            ca = jnp.broadcast_to(column[0:16, block : block + 1], (16, 128))
            sa = jnp.broadcast_to(column[16:32, block : block + 1], (16, 128))
            feature.append(
                jnp.concatenate(
                    [
                        ca * fine_cos - sa * fine_sin,
                        -(sa * fine_cos + ca * fine_sin),
                        extra + extra_step * (start + float(block)),
                    ],
                    axis=0,
                )
            )
        hidden = cos_turns(dot(left1, stack3(jnp.concatenate(feature, axis=1))), SHORT_COEFFS)
        hidden = cos_turns(
            dot(left2, jnp.concatenate([stack3(hidden), ones16], axis=0)), SHORT_COEFFS
        )
        high = hidden.astype(BF16)
        value = dot(left3, jnp.concatenate([high, high], axis=0))
        for block in range(blocks):
            here = ramp + (start + float(block)) * (128.0 / (length - 1))
            window = jnp.exp(here * -rate)
            piece = value[:, block * 128 : block * 128 + 128] * jnp.concatenate([window, window], axis=0)
            at = pl.multiple_of((first + block) * 16, 16)
            taps[pl.ds(at, 16), :] = piece
        return carry

    lax.fori_loop(0, length // chunk, one_chunk, 0)
    piece = taps[0:16, :]
    swapped = jnp.concatenate([piece[4:8], piece[0:4], piece[12:16], piece[8:12]], axis=0)
    taps[0:16, :] = jnp.where(iota((16, 128), 1) == 0, 0.5 * (piece + swapped), piece)

    fetch_second.wait()
    source = dot(normed[...], w1[...]).astype(BF16).astype(F32)
    zero = jnp.zeros((1, 128), F32)
    before = jnp.concatenate([zero, source[0:255]], axis=0)
    after = jnp.concatenate([source[1:256], zero], axis=0)
    second = sw[1].astype(F32)
    total = sb[1:2, :] + before * second[0:1]
    total = total + source * second[1:2]
    gate[...] = total + after * second[2:3]

    spread = jnp.concatenate([taps[pl.ds(r, 64, stride=16), :] for r in range(16)], axis=1)
    stage = dot(frows[...], stack3(spread))
    (cos_high, cos_low), (sin_high, sin_low) = cos, sin
    real_table = jnp.concatenate([cos_high, sin_high, cos_low, sin_low], axis=0)
    imag_table = jnp.concatenate([-sin_high, cos_high, -sin_low, cos_low], axis=0)
    for kind, table, out in ((0, real_table, hre), (1, imag_table, him)):
        reals, imags = [], []
        for order in range(2):
            for channel in range(4):
                at = (order * 8 + kind * 4 + channel) * 128
                real, imag = stage[0:64, at : at + 128], stage[64:128, at : at + 128]
                reals.append(real * tw_cos + imag * tw_sin)
                imags.append(imag * tw_cos - real * tw_sin)
        left = jnp.concatenate([jnp.concatenate(reals, axis=0), jnp.concatenate(imags, axis=0)], axis=1)
        left = left.astype(BF16)
        out[...] = dot(jnp.concatenate([left, left], axis=1), table)
    fetch.wait()


def shifted(value, amount):
    size = 128
    lane, row = iota(value.shape, 1), iota(value.shape, 0)
    rolled = pltpu.roll(value, amount % size, 1)
    carried = pltpu.roll(rolled, amount % 64, 0)
    edge_lane = 0 if amount == 1 else size - 1
    edge_row = 0 if amount == 1 else 63
    carried = jnp.where(row == edge_row, 0.0, carried)
    return jnp.where(lane == edge_lane, carried, rolled)


def repeat_high(table):
    return jnp.concatenate([table[0:256, :], table[0:256, :], table[256:512, :]], axis=0)


def conv_kernel(
    moved, hre, him, frows, irows, flanes, ilanes, twiddle, scalars, sw, weight,
    out, edges, kept, wide, result, state, factors, arrived,
):
    fetch = pltpu.make_async_copy(weight.at[EARLY:1024], kept, arrived)
    fetch.start()
    wide[...] = moved[...].astype(F32)
    own = lax.axis_index("row")
    before = wide[pl.ds(jnp.maximum(own - 1, 0) * 18 + 17, 1), :]
    after = wide[pl.ds(jnp.minimum(own + 1, 31) * 18 + 8, 1), :]
    second = sw[1].astype(F32)
    edges[0:1, :] = jnp.where(own > 0, before, 0.0) * second[0:1]
    edges[1:2, :] = jnp.where(own < 31, after, 0.0) * second[2:3]
    smoothed = []
    for branch in range(2):
        rows = []
        for channel in range(4):
            value = wide[pl.ds(branch * 4 + channel, 64, stride=9), :]
            base = channel * 16 + branch * 8
            total = scalars[base : base + 1, :] + shifted(value, 1) * scalars[base + 1 : base + 2, :]
            total = total + value * scalars[base + 2 : base + 3, :]
            total = total + shifted(value, -1) * scalars[base + 3 : base + 4, :]
            rows.append(total)
        smoothed.append(rows)
    forward_rows, inverse_rows, forward_lanes, inverse_lanes = frows, irows, flanes, ilanes
    tw_cos, tw_sin = twiddle[0:64, :], twiddle[64:128, :]
    for channel in range(4):
        state[channel * 64 : channel * 64 + 64, :] = smoothed[1][channel]
        factors[channel * 64 : channel * 64 + 64, :] = smoothed[0][channel]
    factors[256:512, :] = jnp.ones((256, 128), F32)

    def one_order(order, carry):
        signal = [state[c * 64 : c * 64 + 64, :] for c in range(4)]
        stage = dot(forward_rows[...], stack3(jnp.concatenate(signal, axis=1)))
        reals, imags = [], []
        for place in range(4):
            real = stage[0:64, place * 128 : place * 128 + 128]
            imag = stage[64:128, place * 128 : place * 128 + 128]
            reals.append(real * tw_cos + imag * tw_sin)
            imags.append(imag * tw_cos - real * tw_sin)
        left = jnp.concatenate([jnp.concatenate(reals, axis=0), jnp.concatenate(imags, axis=0)], axis=1)
        high = left.astype(BF16)
        spectrum = dot(jnp.concatenate([high, high], axis=1), forward_lanes[...])
        real, imag = spectrum[:, 0:128], spectrum[:, 128:256]
        at = pl.multiple_of(order * 256, 256)
        tap_real, tap_imag = hre[pl.ds(at, 256), :], him[pl.ds(at, 256), :]
        left = jnp.concatenate([real * tap_real - imag * tap_imag, real * tap_imag + imag * tap_real], axis=1)
        high = left.astype(BF16)
        back = dot(jnp.concatenate([high, high], axis=1), inverse_lanes[...])
        columns = []
        for place in range(4):
            real = back[place * 64 : place * 64 + 64, 0:128]
            imag = back[place * 64 : place * 64 + 64, 128:256]
            columns.append(
                jnp.concatenate([real * tw_cos - imag * tw_sin, real * tw_sin + imag * tw_cos], axis=0)
            )
        values = dot(inverse_rows[...], stack3(jnp.concatenate(columns, axis=1)))
        for channel in range(4):
            skip = scalars[pl.ds(channel * 16 + 12 + order, 1), :]
            conv = values[:, channel * 128 : channel * 128 + 128] + signal[channel] * skip
            factor = factors[pl.ds(at + channel * 64, 64), :]
            state[channel * 64 : channel * 64 + 64, :] = conv * factor
        return carry

    lax.fori_loop(0, 2, one_order, 0)
    for channel in range(4):
        result[pl.ds(channel, 64, stride=4), :] = state[channel * 64 : channel * 64 + 64, :]
    out[...] = result[...].astype(BF16).reshape(32, 8, 128)
    fetch.wait()


def norm_kernel(moved, gate, edges, gain, out, wide, ordered):
    wide[...] = moved[...].astype(F32).reshape(256, 128)
    for half in range(2):
        for channel in range(4):
            ordered[pl.ds(half * 128 + channel, 32, stride=4), :] = wide[
                pl.ds(half * 4 + channel, 32, stride=8), :
            ]
    for half in range(2):
        edge_row = 0 if half == 0 else 127
        factor = gate[half * 128 : half * 128 + 128, :]
        factor = factor + jnp.where(iota((128, 128), 0) == edge_row, edges[half : half + 1, :], 0.0)
        value = ordered[half * 128 : half * 128 + 128, :].T * factor
        scale = lax.rsqrt(jnp.mean(value * value, axis=1, keepdims=True) + NORM_EPS)
        out[half * 4 : half * 4 + 4] = (value * scale * gain[...]).astype(BF16).reshape(4, 32, 128)


def output_kernel(mixed, early, late, out):
    left = jnp.concatenate([mixed[c] for c in range(8)], axis=1)
    out[...] = (dot(left[:, 0:EARLY], early[...]) + dot(left[:, EARLY:1024], late[...])).astype(BF16)


VMEM = pl.BlockSpec(memory_space=pltpu.VMEM)
HBM = pl.BlockSpec(memory_space=pltpu.HBM)


def run(kernel, out_shape, inputs, scratch, name, unread=0):
    multi = isinstance(out_shape, (tuple, list))
    return pl.pallas_call(
        kernel,
        out_shape=out_shape,
        in_specs=[VMEM] * (len(inputs) - unread) + [HBM] * unread,
        out_specs=tuple(VMEM for _ in out_shape) if multi else VMEM,
        scratch_shapes=scratch,
        name=name,
        compiler_params=pltpu.CompilerParams(vmem_limit_bytes=24 * 1024 * 1024),
    )(*inputs)


def near(value):
    return pltpu.with_memory_space_constraint(value, pltpu.VMEM)


def far(*values):
    return tuple(pltpu.with_memory_space_constraint(value, pltpu.HBM) for value in values)


def local(
    tokens,
    norm_gain,
    first_gate,
    second_gate,
    value_weight,
    short_weight,
    short_bias,
    embed_weight,
    embed_bias,
    inner_weight,
    inner_bias,
    filter_freq,
    filter_weight,
    filter_skip,
    output_gain,
    output_weight,
):
    small = (
        embed_weight,
        embed_bias.reshape(1, -1),
        inner_weight,
        inner_bias.reshape(1, -1),
        filter_freq.reshape(1, -1),
        filter_weight.transpose(0, 1, 3, 2),
        short_weight,
        short_bias,
        filter_skip,
        output_gain.reshape(1, -1),
    )
    sent, rows, *small = run(
        project_kernel,
        (
            pltpu.VMEM((576, 128), BF16),
            pltpu.VMEM((256, 2048), BF16),
            *(pltpu.VMEM(value.shape, value.dtype) for value in small),
        ),
        far(tokens, norm_gain.reshape(1, -1), first_gate, second_gate, value_weight, *small),
        [
            pltpu.VMEM((256, 2048), BF16),
            pltpu.VMEM((1, 2048), F32),
            pltpu.VMEM((2048, 128), BF16),
            pltpu.VMEM((2048, 128), BF16),
            pltpu.VMEM((2048, 128), BF16),
            pltpu.VMEM((576, 128), F32),
            pltpu.SemaphoreType.DMA((6,)),
            pltpu.SemaphoreType.DMA((len(small),)),
        ],
        "project",
        5 + len(small),
    )
    moved = lax.all_to_all(
        sent.reshape(32, 9, 2, 128), "row", split_axis=0, concat_axis=0, tiled=True
    ).reshape(576, 128)
    *prepared, gate, kept_early = run(
        filter_kernel,
        (
            pltpu.VMEM((512, 128), F32),
            pltpu.VMEM((512, 128), F32),
            pltpu.VMEM((128, 192), BF16),
            pltpu.VMEM((64, 384), BF16),
            pltpu.VMEM((512, 256), BF16),
            pltpu.VMEM((512, 256), BF16),
            pltpu.VMEM((128, 128), F32),
            pltpu.VMEM((64, 128), F32),
            pltpu.VMEM((256, 128), F32),
            pltpu.VMEM((EARLY, 2048), BF16),
        ),
        (*(near(value) for value in (rows, *small[:9])), *far(second_gate, output_weight)),
        [
            pltpu.VMEM((256, 128), F32),
            pltpu.VMEM((64, 256), BF16),
            pltpu.VMEM((64, 256), BF16),
            pltpu.VMEM((1024, 128), F32),
            pltpu.VMEM((32, 128), F32),
            pltpu.VMEM((2048, 128), BF16),
            pltpu.SemaphoreType.DMA((2,)),
        ],
        "filters",
        2,
    )
    mixed, edges, kept = run(
        conv_kernel,
        (pltpu.VMEM((32, 8, 128), BF16), pltpu.VMEM((2, 128), F32), pltpu.VMEM((1024 - EARLY, 2048), BF16)),
        (*(near(value) for value in (moved, *prepared, small[6])), *far(output_weight)),
        [
            pltpu.VMEM((576, 128), F32),
            pltpu.VMEM((256, 128), F32),
            pltpu.VMEM((256, 128), F32),
            pltpu.VMEM((512, 128), F32),
            pltpu.SemaphoreType.DMA,
        ],
        "convolve",
        1,
    )
    result = lax.all_to_all(mixed, "row", split_axis=0, concat_axis=0, tiled=True)
    normed = run(
        norm_kernel,
        pltpu.VMEM((8, 32, 128), BF16),
        tuple(near(value) for value in (result, gate, edges, small[9])),
        [pltpu.VMEM((256, 128), F32), pltpu.VMEM((256, 128), F32)],
        "groupnorm",
    )
    gathered = lax.all_to_all(normed, "col", split_axis=0, concat_axis=0, tiled=True)
    return run(
        output_kernel,
        jax.ShapeDtypeStruct((32, 2048), BF16),
        (near(gathered), near(kept_early), near(kept)),
        [],
        "output",
    )


def solution(mesh):
    in_specs = (
        P("row", None),
        P(),
        P(None, "col"),
        P(None, "col"),
        P(None, "col"),
        P(None, None, "col"),
        P(None, "col"),
        P(),
        P(),
        P(),
        P(),
        P(),
        P(None, None, None, ("col", "row")),
        P(None, ("col", "row")),
        P("col"),
        P(),
    )
    out_specs = P(("row", "col"), None)
    return jax.shard_map(local, mesh=mesh, in_specs=in_specs, out_specs=out_specs, check_vma=False)
```

```python
import functools
import math

import jax
import jax.numpy as jnp
from jax import lax
from jax.experimental import pallas as pl
from jax.experimental.pallas import tpu as pltpu
from jax.sharding import PartitionSpec as P

CHANNELS = 1024
FREQ_BANDS = 16
EARLY = 192
NORM_EPS = 1e-06
DECAY_SLOW = math.log(0.01) / 1.5
DECAY_FAST = math.log(0.01) / 0.3

F32 = jnp.float32
BF16 = jnp.bfloat16

LONG_COEFFS = (
    6.283185160089469,
    -41.34165503141532,
    81.60100407320796,
    -76.54978229245017,
    39.5367060575916,
)
SHORT_COEFFS = (6.283164044302229, -41.33714237106961, 81.3407688866883, -70.99343326314641)


def cos_turns(turns, coeffs=LONG_COEFFS):
    r = 0.25 - jnp.abs(turns - jnp.round(turns))
    s = r * r
    acc = s * coeffs[-1] + coeffs[-2]
    for coeff in coeffs[-3::-1]:
        acc = acc * s + coeff
    return acc * r


def sin_turns(turns):
    return cos_turns(turns - 0.25)


def split(value):
    high = value.astype(BF16)
    low = (value - high.astype(F32)).astype(BF16)
    return high, low


def iota(shape, dim):
    return lax.broadcasted_iota(jnp.int32, shape, dim)


def to_turns(index, period):
    return (index & (period - 1)).astype(F32) * (1.0 / period)


def row_dft_table():
    shape = (128, 192)
    k1, n1 = iota(shape, 0) & 63, iota(shape, 1) & 63
    turns = to_turns((2 * k1 + 1) * n1, 256)
    value = cos_turns(turns + jnp.where(iota(shape, 0) < 64, 0.0, 0.25))
    high = value.astype(BF16).astype(F32)
    return jnp.where(iota(shape, 1) < 128, high, value - high).astype(BF16)


def row_inverse_table(scale):
    shape = (64, 384)
    n1, k1 = iota(shape, 0), iota(shape, 1) & 63
    turns = to_turns((2 * k1 + 1) * n1, 256)
    value = cos_turns(turns + jnp.where((iota(shape, 1) & 64) == 0, 0.0, 0.25)) * scale
    high = value.astype(BF16).astype(F32)
    return jnp.where(iota(shape, 1) < 256, high, value - high).astype(BF16)


def twiddles():
    shape = (64, 128)
    turns = to_turns((2 * iota(shape, 0) + 1) * iota(shape, 1), 32768)
    return cos_turns(turns), sin_turns(turns)


def lane_dft():
    shape = (128, 128)
    turns = to_turns(iota(shape, 0) * iota(shape, 1), 128)
    return split(cos_turns(turns)), split(sin_turns(turns))


def dot(left, right):
    return jnp.dot(left, right, preferred_element_type=F32)


def stack3(value):
    high, low = split(value)
    return jnp.concatenate([high, low, high], axis=0)


def lanes3(value):
    high, low = split(value)
    return jnp.concatenate([high, low, high], axis=1)


def project_kernel(*refs):
    extra = (len(refs) - 15) // 2
    tokens, gain, w0, w1, w2 = refs[0:5]
    small = refs[5 : 5 + extra]
    out, normed = refs[5 + extra : 7 + extra]
    carried = refs[7 + extra : 7 + 2 * extra]
    near_tokens, near_gain, n0, n1, n2, scratch, arrived, carry = refs[7 + 2 * extra :]
    rows = 128
    copies = [pltpu.make_async_copy(gain, near_gain, arrived.at[0])]
    for part in range(2):
        where = pl.ds(part * rows, rows)
        copies.append(pltpu.make_async_copy(tokens.at[where], near_tokens.at[where], arrived.at[part + 1]))
    for index, (source, target) in enumerate(((w0, n0), (w2, n2), (w1, n1))):
        copies.append(pltpu.make_async_copy(source, target, arrived.at[index + 3]))
    carries = [
        pltpu.make_async_copy(source, target, carry.at[index])
        for index, (source, target) in enumerate(zip(small, carried))
    ]
    for copy in copies[:3]:
        copy.start()
    for copy in copies[3:]:
        copy.start(priority=1)
    copies[0].wait()
    for part in range(2):
        copies[part + 1].wait()
        wide = near_tokens[part * rows : part * rows + rows, :].astype(F32)
        scale = lax.rsqrt(jnp.mean(wide * wide, axis=1, keepdims=True) + NORM_EPS)
        normed[part * rows : part * rows + rows, :] = (wide * scale * near_gain[...]).astype(BF16)
    for copy in carries:
        copy.start()
    copies[3].wait()
    copies[4].wait()
    weights = jnp.concatenate([n0[...], n2[...]], axis=1)
    for half in range(2):
        gates = dot(normed[half * 128 : half * 128 + 128, :], weights)
        for branch in range(2):
            block = gates[:, branch * 128 : branch * 128 + 128].T
            for peer in range(32):
                start = peer * 18 + half * 9 + branch * 4
                scratch[start : start + 4, :] = block[peer * 4 : peer * 4 + 4, :]
    copies[5].wait()
    edges = dot(jnp.concatenate([normed[0:8, :], normed[248:256, :]], axis=0), n1[...])
    for peer in range(32):
        scratch[peer * 18 + 8 : peer * 18 + 9, :] = edges[0:1, :]
        scratch[peer * 18 + 17 : peer * 18 + 18, :] = edges[15:16, :]
    out[...] = scratch[...].astype(BF16)
    for copy in carries:
        copy.wait()


def lane_table(sign, cos, sin):
    def part(c, s):
        top = jnp.concatenate([c, -s if sign > 0 else s], axis=1)
        bottom = jnp.concatenate([s if sign > 0 else -s, c], axis=1)
        return jnp.concatenate([top, bottom], axis=0)

    high, low = part(cos[0], sin[0]), part(cos[1], sin[1])
    return jnp.concatenate([high, low], axis=0)


def filter_kernel(
    normed, ew, eb, iw, ib, freq, fw, sw, sb, skip, second_weight, weight,
    hre, him, frows, irows, flanes, ilanes, twiddle, scalars, gate, kept,
    build, lhs1, lhs2, taps, turned, w1, arrived,
):
    length = 8192
    fetch_second = pltpu.make_async_copy(second_weight, w1, arrived.at[1])
    fetch_second.start(priority=1)
    fetch = pltpu.make_async_copy(weight.at[0:EARLY], kept, arrived.at[0])
    fetch.start(priority=1)
    own = lax.axis_index("row") * 4
    first_channel = lax.axis_index("col") * 128 + own

    lines = []
    for branch in range(3):
        lines.append(sb[branch : branch + 1, :])
        lines.append(sw[branch].astype(F32))
    lines.append(jnp.zeros((4, 128), F32))
    lines = pltpu.roll(jnp.concatenate(lines, axis=0), (128 - own) % 128, 1)
    for channel in range(4):
        scalars[channel * 16 : channel * 16 + 16, :] = jnp.broadcast_to(
            lines[:, channel : channel + 1], (16, 128)
        )
        scalars[channel * 16 + 12 : channel * 16 + 14, :] = jnp.broadcast_to(
            skip[:, channel : channel + 1], (2, 128)
        )

    frows[...] = row_dft_table()
    irows[...] = row_inverse_table(1.0 / 8192)
    tw_cos, tw_sin = twiddles()
    twiddle[0:64, :] = tw_cos
    twiddle[64:128, :] = tw_sin
    cos, sin = lane_dft()
    flanes[...] = lane_table(1, cos, sin)
    ilanes[...] = lane_table(-1, cos, sin)

    def high_of(value):
        return value.astype(BF16).astype(F32)

    turns_of = freq[...] * (1.0 / (2.0 * math.pi))
    build[...] = jnp.zeros_like(build)
    embed = ew[...] * turns_of
    bias = eb[...] * turns_of - 0.25
    rows = jnp.concatenate([embed[1:33], embed[0:1], bias], axis=0)
    build[0:34, 0:64] = high_of(rows)
    build[48:82, 0:64] = high_of(rows)
    build[96:130, 0:64] = rows - high_of(rows)
    lhs1[...] = build[...].T[0:64, :].astype(BF16)
    inner = iw[...] * turns_of
    bias = ib[...] * turns_of - 0.25
    build[...] = jnp.zeros_like(build)
    build[0:64, 0:64] = high_of(inner)
    build[64:128, 0:64] = high_of(inner)
    build[128:192, 0:64] = inner - high_of(inner)
    build[192:193, 0:64] = high_of(bias)
    build[193:194, 0:64] = bias - high_of(bias)
    lhs2[...] = build[...].T[0:64, :].astype(BF16)
    left1 = lhs1[:, 0:144]
    left2 = lhs2[:, 0:208]
    parts = []
    for order in range(2):
        parts.append(fw[order, 0] + fw[order, 1])
        parts.append(fw[order, 0] - fw[order, 1])
    fhigh, flow = split(jnp.concatenate(parts, axis=0))
    left3 = jnp.concatenate([fhigh, flow], axis=1)

    band_step = (FREQ_BANDS - 1 - 0.0001) / (FREQ_BANDS - 1)
    band = 0.0001 + iota((16, 128), 0).astype(F32) * band_step
    lane = iota((16, 128), 1).astype(F32)
    coarse = band * (lane * (128.0 / length))
    fine = band * (lane * (1.0 / length))
    coarse_cos, coarse_sin = cos_turns(coarse), sin_turns(coarse)
    fine_cos, fine_sin = cos_turns(fine), sin_turns(fine)
    row = iota((16, 128), 0)
    extra = jnp.where(row == 0, lane * (1.0 / (length - 1)), jnp.where(row == 1, 1.0, 0.0))
    extra_step = jnp.where(row == 0, 128.0 / (length - 1), 0.0)

    rate_step = (DECAY_SLOW - DECAY_FAST) / (CHANNELS - 1)
    channel_row = (iota((8, 128), 0) & 3) + first_channel
    rate = -DECAY_SLOW + channel_row.astype(F32) * rate_step
    ramp = iota((8, 128), 1).astype(F32) * (1.0 / (length - 1))

    chunk = 4096
    blocks = chunk // 128
    ones16 = jnp.ones((16, chunk), BF16)
    turned[0:16, :] = coarse_cos
    turned[16:32, :] = coarse_sin

    def one_chunk(step, carry):
        first = step * blocks
        column = pltpu.roll(turned[...], (128 - first) % 128, 1)
        start = first.astype(F32)
        feature = []
        for block in range(blocks):
            ca = jnp.broadcast_to(column[0:16, block : block + 1], (16, 128))
            sa = jnp.broadcast_to(column[16:32, block : block + 1], (16, 128))
            feature.append(
                jnp.concatenate(
                    [
                        ca * fine_cos - sa * fine_sin,
                        -(sa * fine_cos + ca * fine_sin),
                        extra + extra_step * (start + float(block)),
                    ],
                    axis=0,
                )
            )
        hidden = cos_turns(dot(left1, stack3(jnp.concatenate(feature, axis=1))), SHORT_COEFFS)
        hidden = cos_turns(
            dot(left2, jnp.concatenate([stack3(hidden), ones16], axis=0)), SHORT_COEFFS
        )
        high = hidden.astype(BF16)
        value = dot(left3, jnp.concatenate([high, high], axis=0))
        for block in range(blocks):
            here = ramp + (start + float(block)) * (128.0 / (length - 1))
            window = jnp.exp(here * -rate)
            piece = value[:, block * 128 : block * 128 + 128] * jnp.concatenate([window, window], axis=0)
            at = pl.multiple_of((first + block) * 16, 16)
            taps[pl.ds(at, 16), :] = piece
        return carry

    lax.fori_loop(0, length // chunk, one_chunk, 0)
    piece = taps[0:16, :]
    swapped = jnp.concatenate([piece[4:8], piece[0:4], piece[12:16], piece[8:12]], axis=0)
    taps[0:16, :] = jnp.where(iota((16, 128), 1) == 0, 0.5 * (piece + swapped), piece)

    fetch_second.wait()
    source = dot(normed[...], w1[...]).astype(BF16).astype(F32)
    zero = jnp.zeros((1, 128), F32)
    before = jnp.concatenate([zero, source[0:255]], axis=0)
    after = jnp.concatenate([source[1:256], zero], axis=0)
    second = sw[1].astype(F32)
    total = sb[1:2, :] + before * second[0:1]
    total = total + source * second[1:2]
    gate[...] = total + after * second[2:3]

    spread = jnp.concatenate([taps[pl.ds(r, 64, stride=16), :] for r in range(16)], axis=1)
    stage = dot(frows[...], stack3(spread))
    (cos_high, cos_low), (sin_high, sin_low) = cos, sin
    real_table = jnp.concatenate([cos_high, sin_high, cos_low, sin_low], axis=0)
    imag_table = jnp.concatenate([-sin_high, cos_high, -sin_low, cos_low], axis=0)
    for kind, table, out in ((0, real_table, hre), (1, imag_table, him)):
        reals, imags = [], []
        for order in range(2):
            for channel in range(4):
                at = (order * 8 + kind * 4 + channel) * 128
                real, imag = stage[0:64, at : at + 128], stage[64:128, at : at + 128]
                reals.append(real * tw_cos + imag * tw_sin)
                imags.append(imag * tw_cos - real * tw_sin)
        left = jnp.concatenate([jnp.concatenate(reals, axis=0), jnp.concatenate(imags, axis=0)], axis=1)
        left = left.astype(BF16)
        out[...] = dot(jnp.concatenate([left, left], axis=1), table)
    fetch.wait()


def shifted(value, amount):
    size = 128
    lane, row = iota(value.shape, 1), iota(value.shape, 0)
    rolled = pltpu.roll(value, amount % size, 1)
    carried = pltpu.roll(rolled, amount % 64, 0)
    edge_lane = 0 if amount == 1 else size - 1
    edge_row = 0 if amount == 1 else 63
    carried = jnp.where(row == edge_row, 0.0, carried)
    return jnp.where(lane == edge_lane, carried, rolled)


def repeat_high(table):
    return jnp.concatenate([table[0:256, :], table[0:256, :], table[256:512, :]], axis=0)


def conv_kernel(
    moved, hre, him, frows, irows, flanes, ilanes, twiddle, scalars, sw, weight,
    out, edges, kept, wide, result, state, factors, arrived,
):
    fetch = pltpu.make_async_copy(weight.at[EARLY:1024], kept, arrived)
    fetch.start(priority=1)
    wide[...] = moved[...].astype(F32)
    own = lax.axis_index("row")
    before = wide[pl.ds(jnp.maximum(own - 1, 0) * 18 + 17, 1), :]
    after = wide[pl.ds(jnp.minimum(own + 1, 31) * 18 + 8, 1), :]
    second = sw[1].astype(F32)
    edges[0:1, :] = jnp.where(own > 0, before, 0.0) * second[0:1]
    edges[1:2, :] = jnp.where(own < 31, after, 0.0) * second[2:3]
    smoothed = []
    for branch in range(2):
        rows = []
        for channel in range(4):
            value = wide[pl.ds(branch * 4 + channel, 64, stride=9), :]
            base = channel * 16 + branch * 8
            total = scalars[base : base + 1, :] + shifted(value, 1) * scalars[base + 1 : base + 2, :]
            total = total + value * scalars[base + 2 : base + 3, :]
            total = total + shifted(value, -1) * scalars[base + 3 : base + 4, :]
            rows.append(total)
        smoothed.append(rows)
    forward_rows, inverse_rows, forward_lanes, inverse_lanes = frows, irows, flanes, ilanes
    tw_cos, tw_sin = twiddle[0:64, :], twiddle[64:128, :]
    for channel in range(4):
        state[channel * 64 : channel * 64 + 64, :] = smoothed[1][channel]
        factors[channel * 64 : channel * 64 + 64, :] = smoothed[0][channel]
    factors[256:512, :] = jnp.ones((256, 128), F32)

    def one_order(order, carry):
        signal = [state[c * 64 : c * 64 + 64, :] for c in range(4)]
        stage = dot(forward_rows[...], stack3(jnp.concatenate(signal, axis=1)))
        reals, imags = [], []
        for place in range(4):
            real = stage[0:64, place * 128 : place * 128 + 128]
            imag = stage[64:128, place * 128 : place * 128 + 128]
            reals.append(real * tw_cos + imag * tw_sin)
            imags.append(imag * tw_cos - real * tw_sin)
        left = jnp.concatenate([jnp.concatenate(reals, axis=0), jnp.concatenate(imags, axis=0)], axis=1)
        high = left.astype(BF16)
        spectrum = dot(jnp.concatenate([high, high], axis=1), forward_lanes[...])
        real, imag = spectrum[:, 0:128], spectrum[:, 128:256]
        at = pl.multiple_of(order * 256, 256)
        tap_real, tap_imag = hre[pl.ds(at, 256), :], him[pl.ds(at, 256), :]
        left = jnp.concatenate([real * tap_real - imag * tap_imag, real * tap_imag + imag * tap_real], axis=1)
        high = left.astype(BF16)
        back = dot(jnp.concatenate([high, high], axis=1), inverse_lanes[...])
        columns = []
        for place in range(4):
            real = back[place * 64 : place * 64 + 64, 0:128]
            imag = back[place * 64 : place * 64 + 64, 128:256]
            columns.append(
                jnp.concatenate([real * tw_cos - imag * tw_sin, real * tw_sin + imag * tw_cos], axis=0)
            )
        values = dot(inverse_rows[...], stack3(jnp.concatenate(columns, axis=1)))
        for channel in range(4):
            skip = scalars[pl.ds(channel * 16 + 12 + order, 1), :]
            conv = values[:, channel * 128 : channel * 128 + 128] + signal[channel] * skip
            factor = factors[pl.ds(at + channel * 64, 64), :]
            state[channel * 64 : channel * 64 + 64, :] = conv * factor
        return carry

    lax.fori_loop(0, 2, one_order, 0)
    for channel in range(4):
        result[pl.ds(channel, 64, stride=4), :] = state[channel * 64 : channel * 64 + 64, :]
    out[...] = result[...].astype(BF16).reshape(32, 8, 128)
    fetch.wait()


def norm_kernel(moved, gate, edges, gain, out, wide, ordered):
    wide[...] = moved[...].astype(F32).reshape(256, 128)
    for half in range(2):
        for channel in range(4):
            ordered[pl.ds(half * 128 + channel, 32, stride=4), :] = wide[
                pl.ds(half * 4 + channel, 32, stride=8), :
            ]
    for half in range(2):
        edge_row = 0 if half == 0 else 127
        factor = gate[half * 128 : half * 128 + 128, :]
        factor = factor + jnp.where(iota((128, 128), 0) == edge_row, edges[half : half + 1, :], 0.0)
        value = ordered[half * 128 : half * 128 + 128, :].T * factor
        scale = lax.rsqrt(jnp.mean(value * value, axis=1, keepdims=True) + NORM_EPS)
        out[half * 4 : half * 4 + 4] = (value * scale * gain[...]).astype(BF16).reshape(4, 32, 128)


def output_kernel(mixed, early, late, out):
    left = jnp.concatenate([mixed[c] for c in range(8)], axis=1)
    out[...] = (dot(left[:, 0:EARLY], early[...]) + dot(left[:, EARLY:1024], late[...])).astype(BF16)


VMEM = pl.BlockSpec(memory_space=pltpu.VMEM)
HBM = pl.BlockSpec(memory_space=pltpu.HBM)


def run(kernel, out_shape, inputs, scratch, name, unread=0):
    multi = isinstance(out_shape, (tuple, list))
    return pl.pallas_call(
        kernel,
        out_shape=out_shape,
        in_specs=[VMEM] * (len(inputs) - unread) + [HBM] * unread,
        out_specs=tuple(VMEM for _ in out_shape) if multi else VMEM,
        scratch_shapes=scratch,
        name=name,
        compiler_params=pltpu.CompilerParams(vmem_limit_bytes=24 * 1024 * 1024),
    )(*inputs)


def near(value):
    return pltpu.with_memory_space_constraint(value, pltpu.VMEM)


def far(*values):
    return tuple(pltpu.with_memory_space_constraint(value, pltpu.HBM) for value in values)


def local(
    tokens,
    norm_gain,
    first_gate,
    second_gate,
    value_weight,
    short_weight,
    short_bias,
    embed_weight,
    embed_bias,
    inner_weight,
    inner_bias,
    filter_freq,
    filter_weight,
    filter_skip,
    output_gain,
    output_weight,
):
    small = (
        embed_weight,
        embed_bias.reshape(1, -1),
        inner_weight,
        inner_bias.reshape(1, -1),
        filter_freq.reshape(1, -1),
        filter_weight.transpose(0, 1, 3, 2),
        short_weight,
        short_bias,
        filter_skip,
        output_gain.reshape(1, -1),
    )
    sent, rows, *small = run(
        project_kernel,
        (
            pltpu.VMEM((576, 128), BF16),
            pltpu.VMEM((256, 2048), BF16),
            *(pltpu.VMEM(value.shape, value.dtype) for value in small),
        ),
        far(tokens, norm_gain.reshape(1, -1), first_gate, second_gate, value_weight, *small),
        [
            pltpu.VMEM((256, 2048), BF16),
            pltpu.VMEM((1, 2048), F32),
            pltpu.VMEM((2048, 128), BF16),
            pltpu.VMEM((2048, 128), BF16),
            pltpu.VMEM((2048, 128), BF16),
            pltpu.VMEM((576, 128), F32),
            pltpu.SemaphoreType.DMA((6,)),
            pltpu.SemaphoreType.DMA((len(small),)),
        ],
        "project",
        5 + len(small),
    )
    moved = lax.all_to_all(
        sent.reshape(32, 9, 2, 128), "row", split_axis=0, concat_axis=0, tiled=True
    ).reshape(576, 128)
    *prepared, gate, kept_early = run(
        filter_kernel,
        (
            pltpu.VMEM((512, 128), F32),
            pltpu.VMEM((512, 128), F32),
            pltpu.VMEM((128, 192), BF16),
            pltpu.VMEM((64, 384), BF16),
            pltpu.VMEM((512, 256), BF16),
            pltpu.VMEM((512, 256), BF16),
            pltpu.VMEM((128, 128), F32),
            pltpu.VMEM((64, 128), F32),
            pltpu.VMEM((256, 128), F32),
            pltpu.VMEM((EARLY, 2048), BF16),
        ),
        (*(near(value) for value in (rows, *small[:9])), *far(second_gate, output_weight)),
        [
            pltpu.VMEM((256, 128), F32),
            pltpu.VMEM((64, 256), BF16),
            pltpu.VMEM((64, 256), BF16),
            pltpu.VMEM((1024, 128), F32),
            pltpu.VMEM((32, 128), F32),
            pltpu.VMEM((2048, 128), BF16),
            pltpu.SemaphoreType.DMA((2,)),
        ],
        "filters",
        2,
    )
    mixed, edges, kept = run(
        conv_kernel,
        (pltpu.VMEM((32, 8, 128), BF16), pltpu.VMEM((2, 128), F32), pltpu.VMEM((1024 - EARLY, 2048), BF16)),
        (*(near(value) for value in (moved, *prepared, small[6])), *far(output_weight)),
        [
            pltpu.VMEM((576, 128), F32),
            pltpu.VMEM((256, 128), F32),
            pltpu.VMEM((256, 128), F32),
            pltpu.VMEM((512, 128), F32),
            pltpu.SemaphoreType.DMA,
        ],
        "convolve",
        1,
    )
    result = lax.all_to_all(mixed, "row", split_axis=0, concat_axis=0, tiled=True)
    normed = run(
        norm_kernel,
        pltpu.VMEM((8, 32, 128), BF16),
        tuple(near(value) for value in (result, gate, edges, small[9])),
        [pltpu.VMEM((256, 128), F32), pltpu.VMEM((256, 128), F32)],
        "groupnorm",
    )
    gathered = lax.all_to_all(normed, "col", split_axis=0, concat_axis=0, tiled=True)
    return run(
        output_kernel,
        jax.ShapeDtypeStruct((32, 2048), BF16),
        (near(gathered), near(kept_early), near(kept)),
        [],
        "output",
    )


def solution(mesh):
    in_specs = (
        P("row", None),
        P(),
        P(None, "col"),
        P(None, "col"),
        P(None, "col"),
        P(None, None, "col"),
        P(None, "col"),
        P(),
        P(),
        P(),
        P(),
        P(),
        P(None, None, None, ("col", "row")),
        P(None, ("col", "row")),
        P("col"),
        P(),
    )
    out_specs = P(("row", "col"), None)
    return jax.shard_map(local, mesh=mesh, in_specs=in_specs, out_specs=out_specs, check_vma=False)
```

```python
import functools
import math

import jax
import jax.numpy as jnp
from jax import lax
from jax.experimental import pallas as pl
from jax.experimental.pallas import tpu as pltpu
from jax.sharding import PartitionSpec as P

CHANNELS = 1024
FREQ_BANDS = 16
EARLY = 224
NORM_EPS = 1e-06
DECAY_SLOW = math.log(0.01) / 1.5
DECAY_FAST = math.log(0.01) / 0.3

F32 = jnp.float32
BF16 = jnp.bfloat16

LONG_COEFFS = (
    6.283185160089469,
    -41.34165503141532,
    81.60100407320796,
    -76.54978229245017,
    39.5367060575916,
)
SHORT_COEFFS = (6.283164044302229, -41.33714237106961, 81.3407688866883, -70.99343326314641)


def cos_turns(turns, coeffs=LONG_COEFFS):
    r = 0.25 - jnp.abs(turns - jnp.round(turns))
    s = r * r
    acc = s * coeffs[-1] + coeffs[-2]
    for coeff in coeffs[-3::-1]:
        acc = acc * s + coeff
    return acc * r


def sin_turns(turns):
    return cos_turns(turns - 0.25)


def split(value):
    high = value.astype(BF16)
    low = (value - high.astype(F32)).astype(BF16)
    return high, low


def iota(shape, dim):
    return lax.broadcasted_iota(jnp.int32, shape, dim)


def to_turns(index, period):
    return (index & (period - 1)).astype(F32) * (1.0 / period)


def row_dft_table():
    shape = (128, 192)
    k1, n1 = iota(shape, 0) & 63, iota(shape, 1) & 63
    turns = to_turns((2 * k1 + 1) * n1, 256)
    value = cos_turns(turns + jnp.where(iota(shape, 0) < 64, 0.0, 0.25))
    high = value.astype(BF16).astype(F32)
    return jnp.where(iota(shape, 1) < 128, high, value - high).astype(BF16)


def row_inverse_table(scale):
    shape = (64, 384)
    n1, k1 = iota(shape, 0), iota(shape, 1) & 63
    turns = to_turns((2 * k1 + 1) * n1, 256)
    value = cos_turns(turns + jnp.where((iota(shape, 1) & 64) == 0, 0.0, 0.25)) * scale
    high = value.astype(BF16).astype(F32)
    return jnp.where(iota(shape, 1) < 256, high, value - high).astype(BF16)


def twiddles():
    shape = (64, 128)
    turns = to_turns((2 * iota(shape, 0) + 1) * iota(shape, 1), 32768)
    return cos_turns(turns), sin_turns(turns)


def lane_dft():
    shape = (128, 128)
    turns = to_turns(iota(shape, 0) * iota(shape, 1), 128)
    return split(cos_turns(turns)), split(sin_turns(turns))


def dot(left, right):
    return jnp.dot(left, right, preferred_element_type=F32)


def stack3(value):
    high, low = split(value)
    return jnp.concatenate([high, low, high], axis=0)


def lanes3(value):
    high, low = split(value)
    return jnp.concatenate([high, low, high], axis=1)


def project_kernel(*refs):
    extra = (len(refs) - 15) // 2
    tokens, gain, w0, w1, w2 = refs[0:5]
    small = refs[5 : 5 + extra]
    out, normed = refs[5 + extra : 7 + extra]
    carried = refs[7 + extra : 7 + 2 * extra]
    near_tokens, near_gain, n0, n1, n2, scratch, arrived, carry = refs[7 + 2 * extra :]
    rows = 128
    copies = [pltpu.make_async_copy(gain, near_gain, arrived.at[0])]
    for part in range(2):
        where = pl.ds(part * rows, rows)
        copies.append(pltpu.make_async_copy(tokens.at[where], near_tokens.at[where], arrived.at[part + 1]))
    for index, (source, target) in enumerate(((w0, n0), (w2, n2), (w1, n1))):
        copies.append(pltpu.make_async_copy(source, target, arrived.at[index + 3]))
    carries = [
        pltpu.make_async_copy(source, target, carry.at[index])
        for index, (source, target) in enumerate(zip(small, carried))
    ]
    for copy in copies[:3]:
        copy.start()
    for copy in copies[3:]:
        copy.start(priority=1)
    copies[0].wait()
    for part in range(2):
        copies[part + 1].wait()
        wide = near_tokens[part * rows : part * rows + rows, :].astype(F32)
        scale = lax.rsqrt(jnp.mean(wide * wide, axis=1, keepdims=True) + NORM_EPS)
        normed[part * rows : part * rows + rows, :] = (wide * scale * near_gain[...]).astype(BF16)
    for copy in carries:
        copy.start()
    copies[3].wait()
    copies[4].wait()
    weights = jnp.concatenate([n0[...], n2[...]], axis=1)
    for half in range(2):
        gates = dot(normed[half * 128 : half * 128 + 128, :], weights)
        for branch in range(2):
            block = gates[:, branch * 128 : branch * 128 + 128].T
            for peer in range(32):
                start = peer * 18 + half * 9 + branch * 4
                scratch[start : start + 4, :] = block[peer * 4 : peer * 4 + 4, :]
    copies[5].wait()
    edges = dot(jnp.concatenate([normed[0:8, :], normed[248:256, :]], axis=0), n1[...])
    for peer in range(32):
        scratch[peer * 18 + 8 : peer * 18 + 9, :] = edges[0:1, :]
        scratch[peer * 18 + 17 : peer * 18 + 18, :] = edges[15:16, :]
    out[...] = scratch[...].astype(BF16)
    for copy in carries:
        copy.wait()


def lane_table(sign, cos, sin):
    def part(c, s):
        top = jnp.concatenate([c, -s if sign > 0 else s], axis=1)
        bottom = jnp.concatenate([s if sign > 0 else -s, c], axis=1)
        return jnp.concatenate([top, bottom], axis=0)

    high, low = part(cos[0], sin[0]), part(cos[1], sin[1])
    return jnp.concatenate([high, low], axis=0)


def filter_kernel(
    normed, ew, eb, iw, ib, freq, fw, sw, sb, skip, second_weight, weight,
    hre, him, frows, irows, flanes, ilanes, twiddle, scalars, gate, kept,
    build, lhs1, lhs2, taps, turned, w1, arrived,
):
    length = 8192
    fetch_second = pltpu.make_async_copy(second_weight, w1, arrived.at[1])
    fetch_second.start()
    fetch = pltpu.make_async_copy(weight.at[0:EARLY], kept, arrived.at[0])
    fetch.start()
    own = lax.axis_index("row") * 4
    first_channel = lax.axis_index("col") * 128 + own

    lines = []
    for branch in range(3):
        lines.append(sb[branch : branch + 1, :])
        lines.append(sw[branch].astype(F32))
    lines.append(jnp.zeros((4, 128), F32))
    lines = pltpu.roll(jnp.concatenate(lines, axis=0), (128 - own) % 128, 1)
    for channel in range(4):
        scalars[channel * 16 : channel * 16 + 16, :] = jnp.broadcast_to(
            lines[:, channel : channel + 1], (16, 128)
        )
        scalars[channel * 16 + 12 : channel * 16 + 14, :] = jnp.broadcast_to(
            skip[:, channel : channel + 1], (2, 128)
        )

    frows[...] = row_dft_table()
    irows[...] = row_inverse_table(1.0 / 8192)
    tw_cos, tw_sin = twiddles()
    twiddle[0:64, :] = tw_cos
    twiddle[64:128, :] = tw_sin
    cos, sin = lane_dft()
    flanes[...] = lane_table(1, cos, sin)
    ilanes[...] = lane_table(-1, cos, sin)

    def high_of(value):
        return value.astype(BF16).astype(F32)

    turns_of = freq[...] * (1.0 / (2.0 * math.pi))
    build[...] = jnp.zeros_like(build)
    embed = ew[...] * turns_of
    bias = eb[...] * turns_of - 0.25
    rows = jnp.concatenate([embed[1:33], embed[0:1], bias], axis=0)
    build[0:34, 0:64] = high_of(rows)
    build[48:82, 0:64] = high_of(rows)
    build[96:130, 0:64] = rows - high_of(rows)
    lhs1[...] = build[...].T[0:64, :].astype(BF16)
    inner = iw[...] * turns_of
    bias = ib[...] * turns_of - 0.25
    build[...] = jnp.zeros_like(build)
    build[0:64, 0:64] = high_of(inner)
    build[64:128, 0:64] = high_of(inner)
    build[128:192, 0:64] = inner - high_of(inner)
    build[192:193, 0:64] = high_of(bias)
    build[193:194, 0:64] = bias - high_of(bias)
    lhs2[...] = build[...].T[0:64, :].astype(BF16)
    left1 = lhs1[:, 0:144]
    left2 = lhs2[:, 0:208]
    parts = []
    for order in range(2):
        parts.append(fw[order, 0] + fw[order, 1])
        parts.append(fw[order, 0] - fw[order, 1])
    fhigh, flow = split(jnp.concatenate(parts, axis=0))
    left3 = jnp.concatenate([fhigh, flow], axis=1)

    band_step = (FREQ_BANDS - 1 - 0.0001) / (FREQ_BANDS - 1)
    band = 0.0001 + iota((16, 128), 0).astype(F32) * band_step
    lane = iota((16, 128), 1).astype(F32)
    coarse = band * (lane * (128.0 / length))
    fine = band * (lane * (1.0 / length))
    coarse_cos, coarse_sin = cos_turns(coarse), sin_turns(coarse)
    fine_cos, fine_sin = cos_turns(fine), sin_turns(fine)
    row = iota((16, 128), 0)
    extra = jnp.where(row == 0, lane * (1.0 / (length - 1)), jnp.where(row == 1, 1.0, 0.0))
    extra_step = jnp.where(row == 0, 128.0 / (length - 1), 0.0)

    rate_step = (DECAY_SLOW - DECAY_FAST) / (CHANNELS - 1)
    channel_row = (iota((8, 128), 0) & 3) + first_channel
    rate = -DECAY_SLOW + channel_row.astype(F32) * rate_step
    ramp = iota((8, 128), 1).astype(F32) * (1.0 / (length - 1))

    chunk = 4096
    blocks = chunk // 128
    ones16 = jnp.ones((16, chunk), BF16)
    turned[0:16, :] = coarse_cos
    turned[16:32, :] = coarse_sin

    def one_chunk(step, carry):
        first = step * blocks
        column = pltpu.roll(turned[...], (128 - first) % 128, 1)
        start = first.astype(F32)
        feature = []
        for block in range(blocks):
            ca = jnp.broadcast_to(column[0:16, block : block + 1], (16, 128))
            sa = jnp.broadcast_to(column[16:32, block : block + 1], (16, 128))
            feature.append(
                jnp.concatenate(
                    [
                        ca * fine_cos - sa * fine_sin,
                        -(sa * fine_cos + ca * fine_sin),
                        extra + extra_step * (start + float(block)),
                    ],
                    axis=0,
                )
            )
        hidden = cos_turns(dot(left1, stack3(jnp.concatenate(feature, axis=1))), SHORT_COEFFS)
        hidden = cos_turns(
            dot(left2, jnp.concatenate([stack3(hidden), ones16], axis=0)), SHORT_COEFFS
        )
        high = hidden.astype(BF16)
        value = dot(left3, jnp.concatenate([high, high], axis=0))
        for block in range(blocks):
            here = ramp + (start + float(block)) * (128.0 / (length - 1))
            window = jnp.exp(here * -rate)
            piece = value[:, block * 128 : block * 128 + 128] * jnp.concatenate([window, window], axis=0)
            at = pl.multiple_of((first + block) * 16, 16)
            taps[pl.ds(at, 16), :] = piece
        return carry

    lax.fori_loop(0, length // chunk, one_chunk, 0)
    piece = taps[0:16, :]
    swapped = jnp.concatenate([piece[4:8], piece[0:4], piece[12:16], piece[8:12]], axis=0)
    taps[0:16, :] = jnp.where(iota((16, 128), 1) == 0, 0.5 * (piece + swapped), piece)

    fetch_second.wait()
    source = dot(normed[...], w1[...]).astype(BF16).astype(F32)
    zero = jnp.zeros((1, 128), F32)
    before = jnp.concatenate([zero, source[0:255]], axis=0)
    after = jnp.concatenate([source[1:256], zero], axis=0)
    second = sw[1].astype(F32)
    total = sb[1:2, :] + before * second[0:1]
    total = total + source * second[1:2]
    gate[...] = total + after * second[2:3]

    spread = jnp.concatenate([taps[pl.ds(r, 64, stride=16), :] for r in range(16)], axis=1)
    stage = dot(frows[...], stack3(spread))
    (cos_high, cos_low), (sin_high, sin_low) = cos, sin
    real_table = jnp.concatenate([cos_high, sin_high, cos_low, sin_low], axis=0)
    imag_table = jnp.concatenate([-sin_high, cos_high, -sin_low, cos_low], axis=0)
    for kind, table, out in ((0, real_table, hre), (1, imag_table, him)):
        reals, imags = [], []
        for order in range(2):
            for channel in range(4):
                at = (order * 8 + kind * 4 + channel) * 128
                real, imag = stage[0:64, at : at + 128], stage[64:128, at : at + 128]
                reals.append(real * tw_cos + imag * tw_sin)
                imags.append(imag * tw_cos - real * tw_sin)
        left = jnp.concatenate([jnp.concatenate(reals, axis=0), jnp.concatenate(imags, axis=0)], axis=1)
        left = left.astype(BF16)
        out[...] = dot(jnp.concatenate([left, left], axis=1), table)
    fetch.wait()


def shifted(value, amount):
    size = 128
    lane, row = iota(value.shape, 1), iota(value.shape, 0)
    rolled = pltpu.roll(value, amount % size, 1)
    carried = pltpu.roll(rolled, amount % 64, 0)
    edge_lane = 0 if amount == 1 else size - 1
    edge_row = 0 if amount == 1 else 63
    carried = jnp.where(row == edge_row, 0.0, carried)
    return jnp.where(lane == edge_lane, carried, rolled)


def repeat_high(table):
    return jnp.concatenate([table[0:256, :], table[0:256, :], table[256:512, :]], axis=0)


def conv_kernel(
    moved, hre, him, frows, irows, flanes, ilanes, twiddle, scalars, sw, weight,
    out, edges, kept, wide, result, state, factors, arrived,
):
    fetch = pltpu.make_async_copy(weight.at[EARLY:1024], kept, arrived)
    fetch.start()
    wide[...] = moved[...].astype(F32)
    own = lax.axis_index("row")
    before = wide[pl.ds(jnp.maximum(own - 1, 0) * 18 + 17, 1), :]
    after = wide[pl.ds(jnp.minimum(own + 1, 31) * 18 + 8, 1), :]
    second = sw[1].astype(F32)
    edges[0:1, :] = jnp.where(own > 0, before, 0.0) * second[0:1]
    edges[1:2, :] = jnp.where(own < 31, after, 0.0) * second[2:3]
    smoothed = []
    for branch in range(2):
        rows = []
        for channel in range(4):
            value = wide[pl.ds(branch * 4 + channel, 64, stride=9), :]
            base = channel * 16 + branch * 8
            total = scalars[base : base + 1, :] + shifted(value, 1) * scalars[base + 1 : base + 2, :]
            total = total + value * scalars[base + 2 : base + 3, :]
            total = total + shifted(value, -1) * scalars[base + 3 : base + 4, :]
            rows.append(total)
        smoothed.append(rows)
    forward_rows, inverse_rows, forward_lanes, inverse_lanes = frows, irows, flanes, ilanes
    tw_cos, tw_sin = twiddle[0:64, :], twiddle[64:128, :]
    for channel in range(4):
        state[channel * 64 : channel * 64 + 64, :] = smoothed[1][channel]
        factors[channel * 64 : channel * 64 + 64, :] = smoothed[0][channel]
    factors[256:512, :] = jnp.ones((256, 128), F32)

    def one_order(order, carry):
        signal = [state[c * 64 : c * 64 + 64, :] for c in range(4)]
        stage = dot(forward_rows[...], stack3(jnp.concatenate(signal, axis=1)))
        reals, imags = [], []
        for place in range(4):
            real = stage[0:64, place * 128 : place * 128 + 128]
            imag = stage[64:128, place * 128 : place * 128 + 128]
            reals.append(real * tw_cos + imag * tw_sin)
            imags.append(imag * tw_cos - real * tw_sin)
        left = jnp.concatenate([jnp.concatenate(reals, axis=0), jnp.concatenate(imags, axis=0)], axis=1)
        high = left.astype(BF16)
        spectrum = dot(jnp.concatenate([high, high], axis=1), forward_lanes[...])
        real, imag = spectrum[:, 0:128], spectrum[:, 128:256]
        at = pl.multiple_of(order * 256, 256)
        tap_real, tap_imag = hre[pl.ds(at, 256), :], him[pl.ds(at, 256), :]
        left = jnp.concatenate([real * tap_real - imag * tap_imag, real * tap_imag + imag * tap_real], axis=1)
        high = left.astype(BF16)
        back = dot(jnp.concatenate([high, high], axis=1), inverse_lanes[...])
        columns = []
        for place in range(4):
            real = back[place * 64 : place * 64 + 64, 0:128]
            imag = back[place * 64 : place * 64 + 64, 128:256]
            columns.append(
                jnp.concatenate([real * tw_cos - imag * tw_sin, real * tw_sin + imag * tw_cos], axis=0)
            )
        values = dot(inverse_rows[...], stack3(jnp.concatenate(columns, axis=1)))
        for channel in range(4):
            skip = scalars[pl.ds(channel * 16 + 12 + order, 1), :]
            conv = values[:, channel * 128 : channel * 128 + 128] + signal[channel] * skip
            factor = factors[pl.ds(at + channel * 64, 64), :]
            state[channel * 64 : channel * 64 + 64, :] = conv * factor
        return carry

    lax.fori_loop(0, 2, one_order, 0)
    for channel in range(4):
        result[pl.ds(channel, 64, stride=4), :] = state[channel * 64 : channel * 64 + 64, :]
    out[...] = result[...].astype(BF16).reshape(32, 8, 128)
    fetch.wait()


def norm_kernel(moved, gate, edges, gain, out, wide, ordered):
    wide[...] = moved[...].astype(F32).reshape(256, 128)
    for half in range(2):
        for channel in range(4):
            ordered[pl.ds(half * 128 + channel, 32, stride=4), :] = wide[
                pl.ds(half * 4 + channel, 32, stride=8), :
            ]
    for half in range(2):
        edge_row = 0 if half == 0 else 127
        factor = gate[half * 128 : half * 128 + 128, :]
        factor = factor + jnp.where(iota((128, 128), 0) == edge_row, edges[half : half + 1, :], 0.0)
        value = ordered[half * 128 : half * 128 + 128, :].T * factor
        scale = lax.rsqrt(jnp.mean(value * value, axis=1, keepdims=True) + NORM_EPS)
        out[half * 4 : half * 4 + 4] = (value * scale * gain[...]).astype(BF16).reshape(4, 32, 128)


def output_kernel(mixed, early, late, out):
    left = jnp.concatenate([mixed[c] for c in range(8)], axis=1)
    out[...] = (dot(left[:, 0:EARLY], early[...]) + dot(left[:, EARLY:1024], late[...])).astype(BF16)


VMEM = pl.BlockSpec(memory_space=pltpu.VMEM)
HBM = pl.BlockSpec(memory_space=pltpu.HBM)


def run(kernel, out_shape, inputs, scratch, name, unread=0):
    multi = isinstance(out_shape, (tuple, list))
    return pl.pallas_call(
        kernel,
        out_shape=out_shape,
        in_specs=[VMEM] * (len(inputs) - unread) + [HBM] * unread,
        out_specs=tuple(VMEM for _ in out_shape) if multi else VMEM,
        scratch_shapes=scratch,
        name=name,
        compiler_params=pltpu.CompilerParams(vmem_limit_bytes=24 * 1024 * 1024),
    )(*inputs)


def near(value):
    return pltpu.with_memory_space_constraint(value, pltpu.VMEM)


def far(*values):
    return tuple(pltpu.with_memory_space_constraint(value, pltpu.HBM) for value in values)


def local(
    tokens,
    norm_gain,
    first_gate,
    second_gate,
    value_weight,
    short_weight,
    short_bias,
    embed_weight,
    embed_bias,
    inner_weight,
    inner_bias,
    filter_freq,
    filter_weight,
    filter_skip,
    output_gain,
    output_weight,
):
    small = (
        embed_weight,
        embed_bias.reshape(1, -1),
        inner_weight,
        inner_bias.reshape(1, -1),
        filter_freq.reshape(1, -1),
        filter_weight.transpose(0, 1, 3, 2),
        short_weight,
        short_bias,
        filter_skip,
        output_gain.reshape(1, -1),
    )
    sent, rows, *small = run(
        project_kernel,
        (
            pltpu.VMEM((576, 128), BF16),
            pltpu.VMEM((256, 2048), BF16),
            *(pltpu.VMEM(value.shape, value.dtype) for value in small),
        ),
        far(tokens, norm_gain.reshape(1, -1), first_gate, second_gate, value_weight, *small),
        [
            pltpu.VMEM((256, 2048), BF16),
            pltpu.VMEM((1, 2048), F32),
            pltpu.VMEM((2048, 128), BF16),
            pltpu.VMEM((2048, 128), BF16),
            pltpu.VMEM((2048, 128), BF16),
            pltpu.VMEM((576, 128), F32),
            pltpu.SemaphoreType.DMA((6,)),
            pltpu.SemaphoreType.DMA((len(small),)),
        ],
        "project",
        5 + len(small),
    )
    moved = lax.all_to_all(
        sent.reshape(32, 9, 2, 128), "row", split_axis=0, concat_axis=0, tiled=True
    ).reshape(576, 128)
    *prepared, gate, kept_early = run(
        filter_kernel,
        (
            pltpu.VMEM((512, 128), F32),
            pltpu.VMEM((512, 128), F32),
            pltpu.VMEM((128, 192), BF16),
            pltpu.VMEM((64, 384), BF16),
            pltpu.VMEM((512, 256), BF16),
            pltpu.VMEM((512, 256), BF16),
            pltpu.VMEM((128, 128), F32),
            pltpu.VMEM((64, 128), F32),
            pltpu.VMEM((256, 128), F32),
            pltpu.VMEM((EARLY, 2048), BF16),
        ),
        (*(near(value) for value in (rows, *small[:9])), *far(second_gate, output_weight)),
        [
            pltpu.VMEM((256, 128), F32),
            pltpu.VMEM((64, 256), BF16),
            pltpu.VMEM((64, 256), BF16),
            pltpu.VMEM((1024, 128), F32),
            pltpu.VMEM((32, 128), F32),
            pltpu.VMEM((2048, 128), BF16),
            pltpu.SemaphoreType.DMA((2,)),
        ],
        "filters",
        2,
    )
    mixed, edges, kept = run(
        conv_kernel,
        (pltpu.VMEM((32, 8, 128), BF16), pltpu.VMEM((2, 128), F32), pltpu.VMEM((1024 - EARLY, 2048), BF16)),
        (*(near(value) for value in (moved, *prepared, small[6])), *far(output_weight)),
        [
            pltpu.VMEM((576, 128), F32),
            pltpu.VMEM((256, 128), F32),
            pltpu.VMEM((256, 128), F32),
            pltpu.VMEM((512, 128), F32),
            pltpu.SemaphoreType.DMA,
        ],
        "convolve",
        1,
    )
    result = lax.all_to_all(mixed, "row", split_axis=0, concat_axis=0, tiled=True)
    normed = run(
        norm_kernel,
        pltpu.VMEM((8, 32, 128), BF16),
        tuple(near(value) for value in (result, gate, edges, small[9])),
        [pltpu.VMEM((256, 128), F32), pltpu.VMEM((256, 128), F32)],
        "groupnorm",
    )
    gathered = lax.all_to_all(normed, "col", split_axis=0, concat_axis=0, tiled=True)
    return run(
        output_kernel,
        jax.ShapeDtypeStruct((32, 2048), BF16),
        (near(gathered), near(kept_early), near(kept)),
        [],
        "output",
    )


def solution(mesh):
    in_specs = (
        P("row", None),
        P(),
        P(None, "col"),
        P(None, "col"),
        P(None, "col"),
        P(None, None, "col"),
        P(None, "col"),
        P(),
        P(),
        P(),
        P(),
        P(),
        P(None, None, None, ("col", "row")),
        P(None, ("col", "row")),
        P("col"),
        P(),
    )
    out_specs = P(("row", "col"), None)
    return jax.shard_map(local, mesh=mesh, in_specs=in_specs, out_specs=out_specs, check_vma=False)
```
